128 devices in a mesh: sp: 16 (over z, x), tp: 8 (over y, core).
Axes of the slice: x: 4, y: 4, z: 4, core: 2. Of those that a mesh axis runs over, the one named last changes fastest.
Arguments:
- tokens: bfloat16 [12288, 4096], P('sp', 'tp'), may hold values from -12 to 12
- query_weight: bfloat16 [4096, 2048], P(None, 'tp'), may hold values from -0.09375 to 0.09375
- key_weight: bfloat16 [4096, 2048], P(None, 'tp'), may hold values from -0.09375 to 0.09375
- value_weight: bfloat16 [4096, 2048], P(None, 'tp'), may hold values from -0.09375 to 0.09375
- position_bias: float32 [16, 320], P('tp'), may hold values from -104 to 154
- out_grad: bfloat16 [12288, 2048], P('sp', 'tp'), may hold values from -6 to 6
Outputs:
- input_grad: bfloat16 [12288, 4096], P('sp', 'tp')
- query_weight_grad: float32 [4096, 2048], P('sp', 'tp')
- key_weight_grad: float32 [4096, 2048], P('sp', 'tp')
- value_weight_grad: float32 [4096, 2048], P('sp', 'tp')
- bias_grad: float32 [16, 320], P('tp')
The draws below stay inside these ranges and needn't reach their ends.
All inputs are finite; a program needn't handle non-finite values.
Results may differ from the reference program's by a relative error of at most 0.014.
Values may be sent and summed in bfloat16 or wider, within the bound.
A program may use at most 128 MiB of HBM per device.

```python
import jax
import jax.numpy as jnp
import numpy as np
from jax import lax

WIDTH = 4096
HEADS = 16
HEAD_DIM = 128
SEGMENT = 64
PREVIOUS = 4
CLIP = 256
TOKENS = 12288
ATT_WIDTH = 2048
BIAS_LEN = 320
N_TP = 8


def draw_tokens(key, part):
    base = jax.random.normal(jax.random.fold_in(key, 11), (TOKENS, WIDTH), jnp.float32)
    base = jnp.clip(base, -6.0, 6.0)
    return base.astype(jnp.bfloat16)


def draw_position_bias(key, part):
    base = jax.random.normal(jax.random.fold_in(key, 21), (HEADS, BIAS_LEN), jnp.float32)
    base = jnp.clip(base, -4.0, 4.0)
    return base.astype(jnp.float32)


def shard_levels(rng, shape, split, smallest, top_value):
    level = 1.0
    for dim, blocks in split:
        heights = jax.random.uniform(jax.random.fold_in(jax.random.fold_in(rng, 6), dim), (blocks,), jnp.float32, smallest / len(split), top_value / len(split))
        level = level * jnp.repeat(jnp.exp(heights), shape[dim] // blocks).reshape((-1,) + (1,) * (len(shape) - 1 - dim))
    return level


def bell_draw(stream_key, extent, scale, most, shards=(), kind=jnp.bfloat16):
    values = scale * jax.random.normal(stream_key, extent, jnp.float32)
    if shards:
        values = values * shard_levels(stream_key, extent, shards, -0.22, 0.18)
    return jnp.clip(values, -most, most).astype(kind)


def setup_inputs(seed: int = 0) -> dict:
    arg_keys = jax.random.split(jax.random.key(seed), 7)
    tokens = draw_tokens(jax.random.fold_in(arg_keys[6], 71), 0)
    query_weight = bell_draw(arg_keys[1], (WIDTH, ATT_WIDTH), WIDTH ** -0.5, 0.09375, ((1, 8),))
    key_weight = bell_draw(arg_keys[2], (WIDTH, ATT_WIDTH), WIDTH ** -0.5, 0.09375, ((1, 8),))
    value_weight = bell_draw(arg_keys[3], (WIDTH, ATT_WIDTH), WIDTH ** -0.5, 0.09375, ((1, 8),))
    position_bias = draw_position_bias(jax.random.fold_in(arg_keys[6], 71), 0)
    out_grad = bell_draw(arg_keys[5], (TOKENS, ATT_WIDTH), 1.0, 6.0, ((0, 16), (1, 8)))
    return {"tokens": tokens, "query_weight": query_weight, "key_weight": key_weight, "value_weight": value_weight, "position_bias": position_bias, "out_grad": out_grad}


def bias_index(segment, reach, clip):
    query_pos = np.arange(segment)[:, None]
    band_pos = np.arange(reach + segment)[None, :]
    return (np.minimum(reach + query_pos - band_pos, clip) + segment - 1).astype(np.int32)


def fold_band(parts, count, head):
    shaped = parts.reshape(count, PREVIOUS + 1, SEGMENT, head)
    total = jnp.zeros((count + PREVIOUS, SEGMENT, head), jnp.float32)
    for band in range(PREVIOUS + 1):
        total = total.at[band:band + count].add(shaped[:, band])
    return total.reshape((count + PREVIOUS) * SEGMENT, head)


def head_grads(operands):
    query, keys, values, upstream, table = operands
    length, head = query.shape
    reach = PREVIOUS * SEGMENT
    count = length // SEGMENT
    factor = head ** -0.5
    padding = jnp.zeros((reach, head), keys.dtype)
    key_seg = jnp.concatenate([padding, keys]).reshape(count + PREVIOUS, SEGMENT, head)
    value_seg = jnp.concatenate([padding, values]).reshape(count + PREVIOUS, SEGMENT, head)
    key_band = jnp.stack([key_seg[band:band + count] for band in range(PREVIOUS + 1)], axis=1).reshape(count, reach + SEGMENT, head)
    value_band = jnp.stack([value_seg[band:band + count] for band in range(PREVIOUS + 1)], axis=1).reshape(count, reach + SEGMENT, head)
    query_seg = query.reshape(count, SEGMENT, head)
    grad_seg = upstream.reshape(count, SEGMENT, head)
    flat_index = bias_index(SEGMENT, reach, CLIP)
    bias = table[flat_index]
    scores = jnp.einsum('cqd,ckd->cqk', query_seg.astype(jnp.float32), key_band.astype(jnp.float32)) * factor + bias[None]
    key_pos = jnp.arange(count)[:, None] * SEGMENT - reach + jnp.arange(reach + SEGMENT)[None, :]
    valid = (key_pos >= 0)[:, None, :]
    masked = jnp.where(valid, scores, -jnp.inf)
    top = jnp.max(masked, axis=-1, keepdims=True)
    logsum = top + jnp.log(jnp.sum(jnp.exp(masked - top), axis=-1, keepdims=True))
    weights = jnp.exp(masked - logsum)
    weights_low = weights.astype(jnp.bfloat16)
    prob_grad = jnp.einsum('cqd,ckd->cqk', grad_seg.astype(jnp.float32), value_band.astype(jnp.float32))
    delta = jnp.sum(weights * prob_grad, axis=-1, keepdims=True)
    score_grad = weights * (prob_grad - delta)
    score_low = score_grad.astype(jnp.bfloat16)
    query_grad = (jnp.einsum('cqk,ckd->cqd', score_low.astype(jnp.float32), key_band.astype(jnp.float32)) * factor).reshape(length, head).astype(jnp.bfloat16)
    key_parts = jnp.einsum('cqk,cqd->ckd', score_low.astype(jnp.float32), query_seg.astype(jnp.float32)) * factor
    value_parts = jnp.einsum('cqk,cqd->ckd', weights_low.astype(jnp.float32), grad_seg.astype(jnp.float32))
    key_grad = fold_band(key_parts, count, head)[reach:].astype(jnp.bfloat16)
    value_grad = fold_band(value_parts, count, head)[reach:].astype(jnp.bfloat16)
    summed = jnp.sum(score_grad, axis=0).reshape(-1)
    table_grad = jnp.zeros((table.shape[0],), jnp.float32).at[flat_index.reshape(-1)].add(summed)
    return query_grad, key_grad, value_grad, table_grad


def reference(tokens, query_weight, key_weight, value_weight, position_bias, out_grad):
    query = jnp.dot(tokens, query_weight, preferred_element_type=jnp.float32).astype(jnp.bfloat16)
    keys = jnp.dot(tokens, key_weight, preferred_element_type=jnp.float32).astype(jnp.bfloat16)
    values = jnp.dot(tokens, value_weight, preferred_element_type=jnp.float32).astype(jnp.bfloat16)

    def by_head(array):
        return array.reshape(TOKENS, HEADS, HEAD_DIM).transpose(1, 0, 2)

    def by_token(array):
        return array.transpose(1, 0, 2).reshape(TOKENS, HEADS * HEAD_DIM)

    head_query, head_key, head_value, bias_grad = lax.map(head_grads, (by_head(query), by_head(keys), by_head(values), by_head(out_grad), position_bias))
    query_grad = by_token(head_query)
    key_grad = by_token(head_key)
    value_grad = by_token(head_value)
    tokens_t = tokens.T
    query_weight_grad = jnp.dot(tokens_t, query_grad, preferred_element_type=jnp.float32)
    key_weight_grad = jnp.dot(tokens_t, key_grad, preferred_element_type=jnp.float32)
    value_weight_grad = jnp.dot(tokens_t, value_grad, preferred_element_type=jnp.float32)
    group = HEADS * HEAD_DIM // N_TP
    total = jnp.zeros((TOKENS, WIDTH), jnp.float32)
    for number in range(N_TP):
        lower = number * group
        upper = lower + group
        term = jnp.dot(query_grad[:, lower:upper], query_weight[:, lower:upper].T, preferred_element_type=jnp.float32)
        term = term + jnp.dot(key_grad[:, lower:upper], key_weight[:, lower:upper].T, preferred_element_type=jnp.float32)
        term = term + jnp.dot(value_grad[:, lower:upper], value_weight[:, lower:upper].T, preferred_element_type=jnp.float32)
        rounded = lax.optimization_barrier(term.astype(jnp.bfloat16))
        total = total + rounded.astype(jnp.float32)
    input_grad = total.astype(jnp.bfloat16)
    return (input_grad, query_weight_grad, key_weight_grad, value_weight_grad, bias_grad)
```

```python
import functools

import jax
import jax.numpy as jnp
from jax import lax
from jax.experimental import pallas as pl
from jax.experimental.pallas import tpu as pltpu
from jax.sharding import PartitionSpec as P

MESH = pl.DeviceIdType.MESH
BF16, F32 = jnp.bfloat16, jnp.float32
SEGMENT, REACH, CLIP, HEAD = 64, 256, 256, 128
TILE = 128
SPAN = REACH + TILE
LENGTH, WIDTH, FEATURES = 768, 4096, 512
CHUNKS = LENGTH // TILE
HEADS = 2
COLS = HEADS * HEAD
FACTOR = HEAD ** (-0.5)
RING = 4
TABLE = 320
ROUND = 512


def dot(left, right, left_dim=1, right_dim=0):
    return lax.dot_general(left, right, (((left_dim,), (right_dim,)), ((), ())), preferred_element_type=F32)


class Ring:
    def __init__(self, me, up, down, block, via, direct, joined, sems):
        self.near = (lax.rem(me + 1, RING), lax.rem(me + RING - 1, RING))
        self.far = lax.rem(me + 2, RING)
        self.me, self.devices, self.block = me, (up, down), block
        self.landing, self.sems = (via, direct, joined), sems

    def copy(self, kind, d):
        source = (self.block(self.far, d), self.block(self.near[d], 1 - d), self.block(self.near[d], d))[kind]
        send, recv = self.sems
        return pltpu.make_async_remote_copy(
            src_ref=source,
            dst_ref=self.landing[kind](d),
            send_sem=send(kind, d),
            recv_sem=recv(kind, d),
            device_id=self.devices[d],
            device_id_type=MESH,
        )

    def start_far(self):
        for d in range(2):
            self.copy(0, d).start()

    def start_near(self, d):
        self.copy(1, d).start()

    def join(self):
        for d in range(2):
            self.copy(0, d).wait_recv()
            ref = self.block(self.near[d], d)
            ref[...] = (ref[...].astype(F32) + self.landing[0](d)[...].astype(F32)).astype(BF16)
            self.copy(2, d).start()

    def half(self, d):
        self.copy(2, d).wait_recv()
        self.copy(1, 1 - d).wait_recv()
        total = self.block(self.me, d)[...].astype(F32) + self.landing[2](d)[...].astype(F32)
        return total + self.landing[1](1 - d)[...].astype(F32)

    def wait_sends(self):
        for kind in range(3):
            for d in range(2):
                self.copy(kind, d).wait_send()


def kernel(
    tokens, wq, wk, wv, table, out_grad,
    input_out, wq_out, wk_out, wv_out, bias_out,
    whole, weight, query, kv, upstream, dkv, grads, grads_t, back_send, back_recv,
    part_a, part_b, far_ab, near_ab, join_ab, second_ab, far2_ab, near2_ab, join2_ab,
    term_own, term_send, term_recv, far_y, near_y, join_y,
    input_stage, weight_stage, bias, dsum, bias_x, bias_z,
    load_sem, gather_send, gather_recv, hop_send, hop_recv, core_send, core_recv,
    halo_send, halo_recv, back_sems, term_ss, term_rs, ring_ss, ring_rs, y_ss, y_rs, bx_s, bx_r, bz_s, bz_r, store_sem,
):
    sp, tp = lax.axis_index("sp"), lax.axis_index("tp")
    z, x = sp // RING, lax.rem(sp, RING)
    y, core = tp // 2, lax.rem(tp, 2)

    def at(value, by):
        return lax.rem(value + by, RING)

    def at_x(by):
        return (z * RING + at(x, by), tp)

    def at_z(by):
        return (at(z, by) * RING + x, tp)

    def at_y(by):
        return (sp, at(y, by) * 2 + core)

    def at_sp(by):
        return (lax.rem(sp + by, 16), tp)

    partner = (sp, y * 2 + 1 - core)

    barrier = pltpu.get_barrier_semaphore()
    peers = [partner, at_sp(1), at_sp(15)]
    for by in (1, 3):
        peers.append(at_y(by))
    for by in (1, 2, 3):
        peers += [at_x(by), at_z(by)]
    for peer in peers:
        pl.semaphore_signal(barrier, inc=1, device_id=peer, device_id_type=MESH)

    def feature_cols(y_index, core_index):
        return pl.ds(pl.multiple_of((y_index * 2 + core_index) * FEATURES, FEATURES), FEATURES)

    my_cols = feature_cols(y, core)
    loads = [pltpu.make_async_copy(tokens, whole.at[:, my_cols], load_sem.at[0])]
    for number, ref in enumerate((wq, wk, wv)):
        loads.append(pltpu.make_async_copy(ref, weight.at[:, number * COLS : (number + 1) * COLS], load_sem.at[1 + number]))
    loads.append(pltpu.make_async_copy(out_grad, upstream, load_sem.at[4]))
    for load in loads:
        load.start()

    lane = lax.broadcasted_iota(jnp.int32, (8, ROUND), 1)
    row = lax.broadcasted_iota(jnp.int32, (SPAN, TILE), 0)
    column = lax.broadcasted_iota(jnp.int32, (SPAN, TILE), 1)
    low = jnp.where(column >= SEGMENT, SEGMENT, 0)
    seen = (row >= low) & (row < low + REACH + SEGMENT)
    for h in range(HEADS):
        entries = jnp.broadcast_to(table[h : h + 1, :], (8, TABLE))
        padded = jnp.concatenate([entries, jnp.zeros((8, ROUND - TABLE), F32)], axis=1)
        turned = pltpu.roll(padded, ROUND - TABLE + 1, 1)
        last = jnp.broadcast_to(table[h : h + 1, TABLE - 1 : TABLE], (8, ROUND))
        turned = jnp.where(lane < TILE, last, turned)
        skewed = pltpu.roll(jnp.broadcast_to(turned[0:1, :], (SPAN, ROUND)), 0, 1, stride=1, stride_axis=0)
        bias[h] = jnp.where(seen, skewed[:, :TILE], -jnp.inf)
        dsum[h] = jnp.zeros((SPAN, TILE), F32)
    dkv[...] = jnp.zeros(dkv.shape, F32)

    loads[0].wait()
    pl.semaphore_wait(barrier, len(peers))

    def rows_of(step):
        return pl.multiple_of(lax.rem(step + 4, CHUNKS) * TILE, TILE)

    def chunk_copy(rows, cols, target, send, recv):
        view = whole.at[rows, cols]
        return pltpu.make_async_remote_copy(
            src_ref=view, dst_ref=view, send_sem=send, recv_sem=recv, device_id=target, device_id_type=MESH
        )

    up, down = at_y(1), at_y(3)

    def gather_copy(step, d):
        return chunk_copy(pl.ds(rows_of(step), TILE), my_cols, (up, down)[d], gather_send.at[step, d], gather_recv.at[step, d])

    def gather_landed(step, d):
        cols = feature_cols(at(y, (3, 1)[d]), core)
        return chunk_copy(pl.ds(rows_of(step), TILE), cols, (up, down)[d], gather_send.at[step, d], gather_recv.at[step, d])

    def hop_copy(step, d):
        cols = feature_cols(at(y, (3, 1)[d]), core)
        rows = pl.ds(pl.multiple_of(rows_of(step) + d * SEGMENT, SEGMENT), SEGMENT)
        return chunk_copy(rows, cols, (up, down)[d], hop_send.at[step, d], hop_recv.at[step, d])

    def hop_landed(step, d):
        cols = feature_cols(at(y, 2), core)
        rows = pl.ds(pl.multiple_of(rows_of(step) + d * SEGMENT, SEGMENT), SEGMENT)
        return chunk_copy(rows, cols, (up, down)[d], hop_send.at[step, d], hop_recv.at[step, d])

    def core_copy(step, which):
        cols = feature_cols(at(y, (0, 3, 1, 2)[which]), core)
        return chunk_copy(pl.ds(rows_of(step), TILE), cols, partner, core_send.at[step, which], core_recv.at[step, which])

    def core_landed(step, which):
        cols = feature_cols(at(y, (0, 3, 1, 2)[which]), 1 - core)
        return chunk_copy(pl.ds(rows_of(step), TILE), cols, partner, core_send.at[step, which], core_recv.at[step, which])

    def halo_copy(step):
        return pltpu.make_async_remote_copy(
            src_ref=kv.at[pl.ds(pl.multiple_of(LENGTH + step * TILE, TILE), TILE), :],
            dst_ref=kv.at[pl.ds(pl.multiple_of(step * TILE, TILE), TILE), :],
            send_sem=halo_send.at[step],
            recv_sem=halo_recv.at[step],
            device_id=at_sp(1),
            device_id_type=MESH,
        )

    back_copy = pltpu.make_async_remote_copy(
        src_ref=back_send,
        dst_ref=back_recv,
        send_sem=back_sems.at[0],
        recv_sem=back_sems.at[1],
        device_id=at_sp(15),
        device_id_type=MESH,
    )

    edge = jnp.where(sp == 0, REACH, 0)

    def attend(tile):
        start = pl.multiple_of(tile * TILE, TILE)
        keys_at, here = pl.ds(start, SPAN), pl.ds(start, TILE)
        for h in range(HEADS):
            cols = slice(h * HEAD, (h + 1) * HEAD)
            value_cols = slice(COLS + h * HEAD, COLS + (h + 1) * HEAD)
            keys, values = kv[keys_at, cols], kv[keys_at, value_cols]
            asked, given = query[here, cols], upstream[here, cols]
            scores = dot(keys, asked, 1, 1) * FACTOR + bias[h]
            scores = jnp.where(row + start < edge, -jnp.inf, scores)
            top = jnp.max(scores, axis=0, keepdims=True)
            raised = jnp.exp(scores - top)
            weights = raised * (1.0 / jnp.sum(raised, axis=0, keepdims=True))
            prob_grad = dot(values, given, 1, 1)
            delta = jnp.sum(weights * prob_grad, axis=0, keepdims=True)
            score_grad = weights * (prob_grad - delta)
            weights_low, score_low = weights.astype(BF16), score_grad.astype(BF16)
            dsum[h] = dsum[h] + score_grad
            dkv[keys_at, value_cols] = dkv[keys_at, value_cols] + dot(weights_low, given)
            dkv[keys_at, cols] = dkv[keys_at, cols] + dot(score_low, asked)
            query_grad = dot(score_low, keys, 0, 0) * FACTOR
            grads[here, cols] = query_grad.astype(BF16)
            grads_t[cols, here] = query_grad.T.astype(BF16)

    for step in range(2):
        for d in range(2):
            gather_copy(step, d).start()
        core_copy(step, 0).start()
    for load in loads[1:]:
        load.wait()

    def gather_step(s, carry):
        @pl.when(s < CHUNKS)
        def _():
            for d in range(2):
                gather_landed(s, d).wait_recv()
                hop_copy(s, d).start()
            for d in range(2):
                core_copy(s, 1 + d).start()

        @pl.when(s < CHUNKS - 2)
        def _():
            for d in range(2):
                gather_copy(s + 2, d).start()
            core_copy(s + 2, 0).start()

        @pl.when((s >= 1) & (s <= CHUNKS))
        def _():
            for d in range(2):
                hop_landed(s - 1, d).wait_recv()
            core_copy(s - 1, 3).start()

        @pl.when(s == 4)
        def _():
            for step in range(2):
                halo_copy(step).wait_recv()

        @pl.when(s >= 4)
        def _():
            attend(s - 4)

        @pl.when(s == 5)
        def _():
            back_send[...] = dkv[0:REACH, :].astype(BF16)
            back_copy.start()

        @pl.when((s >= 1) & (s <= CHUNKS))
        def _():
            for which in range(4):
                core_landed(s - 1, which).wait_recv()
            start = rows_of(s - 1)
            projected = dot(whole[pl.ds(start, TILE), :], weight[...]).astype(BF16)
            query[pl.ds(start, TILE), :] = projected[:, :COLS]
            kv[pl.ds(pl.multiple_of(start + REACH, TILE), TILE), :] = projected[:, COLS:]

        @pl.when((s >= 1) & (s <= 2))
        def _():
            halo_copy(s - 1).start()

        return carry

    lax.fori_loop(0, CHUNKS + 4, gather_step, 0)

    back_copy.wait_recv()
    dkv[LENGTH:, :] = dkv[LENGTH:, :] + back_recv[...].astype(F32)

    def finish_chunk(chunk, carry):
        start = pl.multiple_of(chunk * TILE, TILE)
        total = dkv[pl.ds(pl.multiple_of(start + REACH, TILE), TILE), :]
        total = jnp.concatenate([total[:, :COLS] * FACTOR, total[:, COLS:]], axis=1)
        grads[pl.ds(start, TILE), COLS:] = total.astype(BF16)
        grads_t[COLS:, pl.ds(start, TILE)] = total.T.astype(BF16)
        return carry

    lax.fori_loop(0, CHUNKS, finish_chunk, 0)

    def first_ring(p, side):
        me = (x, z)[side]
        part = (part_a, part_b)[side]
        at_side = (at_x, at_z)[side]
        return Ring(
            me, at_side(1), at_side(3),
            lambda k, half: part.at[p, k, pl.ds(2 * half, 2)],
            lambda d: far_ab.at[p, side, d],
            lambda d: near_ab.at[p, side, d],
            lambda d: join_ab.at[p, side, d],
            (lambda kind, d: ring_ss.at[p, side, 0, kind, d], lambda kind, d: ring_rs.at[p, side, 0, kind, d]),
        )

    def second_ring(p, side):
        me = (z, x)[side]
        at_side = (at_z, at_x)[side]
        return Ring(
            me, at_side(1), at_side(3),
            lambda k, half: second_ab.at[p, side, k, half * SEGMENT : (half + 1) * SEGMENT],
            lambda d: far2_ab.at[p, side, d],
            lambda d: near2_ab.at[p, side, d],
            lambda d: join2_ab.at[p, side, d],
            (lambda kind, d: ring_ss.at[p, side, 1, kind, d], lambda kind, d: ring_rs.at[p, side, 1, kind, d]),
        )

    y_ring = Ring(
        y, up, down,
        lambda k, half: term_own.at[k, half * (LENGTH // 2) : (half + 1) * (LENGTH // 2)],
        lambda d: far_y.at[d],
        lambda d: near_y.at[d],
        lambda d: join_y.at[d],
        (lambda kind, d: y_ss.at[kind, d], lambda kind, d: y_rs.at[kind, d]),
    )

    def term(y_index, core_index):
        start = pl.multiple_of((y_index * 2 + core_index) * FEATURES, FEATURES)
        return dot(grads[...], weight[pl.ds(start, FEATURES), :], 1, 1)

    def term_copy(k):
        return pltpu.make_async_remote_copy(
            src_ref=term_send.at[k],
            dst_ref=term_recv.at[k],
            send_sem=term_ss.at[k],
            recv_sem=term_rs.at[k],
            device_id=partner,
            device_id_type=MESH,
        )

    def reduce_step(k, carry):
        @pl.when(k < 3)
        def _():
            def weight_rows(z_index, inner):
                left = grads_t[pl.ds(pl.multiple_of(k * COLS, COLS), COLS), :]
                features = pl.ds(pl.multiple_of(z_index * RING * COLS, RING * COLS), RING * COLS)
                made = dot(left, whole[:, features]).astype(BF16)
                for x_index in range(RING):
                    cut = slice(x_index * COLS, (x_index + 1) * COLS)
                    part_a[k, x_index, z_index] = made[:HEAD, cut]
                    part_b[k, z_index, x_index] = made[HEAD:, cut]
                return inner

            lax.fori_loop(0, RING, weight_rows, 0)
            rings = [first_ring(k, side) for side in range(2)]
            for ring in rings:
                ring.start_far()
            for ring in rings:
                for d in range(2):
                    ring.start_near(d)

        ahead = jnp.where(k == 0, 2, jnp.where(k == 1, 1, jnp.where(k == 2, 3, 0)))
        y_index = at(y, ahead)
        term_send[k] = term(y_index, 1 - core).astype(BF16)
        term_copy(k).start()
        made = term(y_index, core)
        term_copy(k).wait_recv()
        term_own[y_index] = (made + term_recv[k].astype(F32)).astype(BF16)

        @pl.when(k == 0)
        def _():
            y_ring.start_far()

        for d in range(2):
            @pl.when(k == 1 + d)
            def _():
                y_ring.start_near(d)

        @pl.when((k >= 1) & (k < 3))
        def _():
            for side in range(2):
                first_ring(k - 1, side).join()

        return carry

    lax.fori_loop(0, RING, reduce_step, 0)

    bias_x[x] = jnp.zeros((8, ROUND), F32)
    for h in range(HEADS):
        wide = jnp.concatenate([dsum[h], jnp.zeros((SPAN, ROUND - TILE), F32)], axis=1)
        rows = SPAN
        while rows > 24:
            rows //= 2
            wide = wide[:rows] + pltpu.roll(wide[rows:], ROUND - rows, 1)
        wide = wide[0:8] + pltpu.roll(wide[8:16], ROUND - 8, 1) + pltpu.roll(wide[16:24], ROUND - 16, 1)
        sums = wide[0:1]
        for r in range(1, 8):
            sums = sums + pltpu.roll(wide[r : r + 1], ROUND - r, 1)
        first = lax.broadcasted_iota(jnp.int32, (1, ROUND), 1)
        clipped = jnp.sum(jnp.where(first < TILE, sums, 0.0), axis=1, keepdims=True)
        placed = pltpu.roll(sums, TABLE - 1, 1)
        bias_x[x, h : h + 1, :] = jnp.where(first == TABLE - 1, clipped, placed)

    def bias_copy(buffer, me, target, send, recv, slot):
        view = buffer.at[me]
        return pltpu.make_async_remote_copy(
            src_ref=view, dst_ref=view, send_sem=send.at[slot], recv_sem=recv.at[slot], device_id=target, device_id_type=MESH
        )

    for by in (1, 2, 3):
        bias_copy(bias_x, x, at_x(by), bx_s, bx_r, by - 1).start()

    y_ring.join()
    for side in range(2):
        first_ring(2, side).join()

    for by in (1, 2, 3):
        bias_copy(bias_x, at(x, 4 - by), at_x(by), bx_s, bx_r, by - 1).wait_recv()
    bias_z[z] = (bias_x[0] + bias_x[1]) + (bias_x[2] + bias_x[3])
    for by in (1, 2, 3):
        bias_copy(bias_z, z, at_z(by), bz_s, bz_r, by - 1).start()

    def second_start(p):
        for side in range(2):
            ring = first_ring(p, side)
            for half in range(2):
                second_ab[p, side, 2 * half : 2 * half + 2] = ring.half(half).astype(BF16)
        rings = [second_ring(p, side) for side in range(2)]
        for ring in rings:
            ring.start_far()
        for ring in rings:
            for d in range(2):
                ring.start_near(d)

    def second_join(p):
        for side in range(2):
            second_ring(p, side).join()

    def second_finish(p):
        for side in range(2):
            ring = second_ring(p, side)
            total = jnp.concatenate([ring.half(0), ring.half(1)], axis=0)
            weight_stage[p, :, side * HEAD : (side + 1) * HEAD] = total.T
        pltpu.make_async_copy(weight_stage.at[p], (wq_out, wk_out, wv_out)[p], store_sem.at[p]).start()

    second_start(0)
    second_start(1)
    second_join(0)
    second_finish(0)
    second_start(2)
    second_join(1)
    second_finish(1)
    for d in range(2):
        input_stage[d * (LENGTH // 2) : (d + 1) * (LENGTH // 2), :] = y_ring.half(d).astype(BF16)
    input_store = pltpu.make_async_copy(input_stage, input_out, store_sem.at[3])
    input_store.start()
    second_join(2)
    for by in (1, 2, 3):
        bias_copy(bias_z, at(z, 4 - by), at_z(by), bz_s, bz_r, by - 1).wait_recv()
    bias_out[...] = ((bias_z[0] + bias_z[1]) + (bias_z[2] + bias_z[3]))[:HEADS, :TABLE]
    second_finish(2)

    for step in range(CHUNKS):
        for d in range(2):
            gather_copy(step, d).wait_send()
            hop_copy(step, d).wait_send()
        for which in range(4):
            core_copy(step, which).wait_send()
    for step in range(2):
        halo_copy(step).wait_send()
    back_copy.wait_send()
    for k in range(RING):
        term_copy(k).wait_send()
    y_ring.wait_sends()
    for p in range(3):
        for side in range(2):
            first_ring(p, side).wait_sends()
            second_ring(p, side).wait_sends()
    for by in (1, 2, 3):
        bias_copy(bias_x, x, at_x(by), bx_s, bx_r, by - 1).wait_send()
        bias_copy(bias_z, z, at_z(by), bz_s, bz_r, by - 1).wait_send()
    for p in range(3):
        pltpu.make_async_copy(weight_stage.at[p], (wq_out, wk_out, wv_out)[p], store_sem.at[p]).wait()
    input_store.wait()


def shards(tokens, query_weight, key_weight, value_weight, position_bias, out_grad):
    anywhere = pl.BlockSpec(memory_space=pl.ANY)
    near = pl.BlockSpec(memory_space=pltpu.VMEM)
    dma = pltpu.SemaphoreType.DMA
    vmem = pltpu.VMEM
    grad = jax.ShapeDtypeStruct((COLS, COLS), F32)
    return pl.pallas_call(
        kernel,
        name="segment_attention_grads",
        out_shape=(
            jax.ShapeDtypeStruct((LENGTH, FEATURES), BF16), grad, grad, grad,
            jax.ShapeDtypeStruct((HEADS, TABLE), F32),
        ),
        in_specs=[anywhere, anywhere, anywhere, anywhere, near, anywhere],
        out_specs=(anywhere, anywhere, anywhere, anywhere, near),
        scratch_shapes=[
            vmem((LENGTH, WIDTH), BF16),
            vmem((WIDTH, 3 * COLS), BF16),
            vmem((LENGTH, COLS), BF16),
            vmem((REACH + LENGTH, 2 * COLS), BF16),
            vmem((LENGTH, COLS), BF16),
            vmem((REACH + LENGTH, 2 * COLS), F32),
            vmem((LENGTH, 3 * COLS), BF16),
            vmem((3 * COLS, LENGTH), BF16),
            vmem((REACH, 2 * COLS), BF16),
            vmem((REACH, 2 * COLS), BF16),
            vmem((3, RING, RING, HEAD, COLS), BF16),
            vmem((3, RING, RING, HEAD, COLS), BF16),
            vmem((3, 2, 2, 2, HEAD, COLS), BF16),
            vmem((3, 2, 2, 2, HEAD, COLS), BF16),
            vmem((3, 2, 2, 2, HEAD, COLS), BF16),
            vmem((3, 2, RING, HEAD, COLS), BF16),
            vmem((3, 2, 2, SEGMENT, COLS), BF16),
            vmem((3, 2, 2, SEGMENT, COLS), BF16),
            vmem((3, 2, 2, SEGMENT, COLS), BF16),
            vmem((RING, LENGTH, FEATURES), BF16),
            vmem((RING, LENGTH, FEATURES), BF16),
            vmem((RING, LENGTH, FEATURES), BF16),
            vmem((2, LENGTH // 2, FEATURES), BF16),
            vmem((2, LENGTH // 2, FEATURES), BF16),
            vmem((2, LENGTH // 2, FEATURES), BF16),
            vmem((LENGTH, FEATURES), BF16),
            vmem((3, COLS, COLS), F32),
            vmem((HEADS, SPAN, TILE), F32),
            vmem((HEADS, SPAN, TILE), F32),
            vmem((RING, 8, ROUND), F32),
            vmem((RING, 8, ROUND), F32),
            dma((5,)),
            dma((CHUNKS, 2)), dma((CHUNKS, 2)),
            dma((CHUNKS, 2)), dma((CHUNKS, 2)),
            dma((CHUNKS, 4)), dma((CHUNKS, 4)),
            dma((2,)), dma((2,)),
            dma((2,)),
            dma((RING,)), dma((RING,)),
            dma((3, 2, 2, 3, 2)), dma((3, 2, 2, 3, 2)),
            dma((3, 2)), dma((3, 2)),
            dma((3,)), dma((3,)), dma((3,)), dma((3,)),
            dma((4,)),
        ],
        compiler_params=pltpu.CompilerParams(
            collective_id=0, has_side_effects=True, vmem_limit_bytes=67_000_000
        ),
    )(tokens, query_weight, key_weight, value_weight, position_bias, out_grad)


def solution(mesh):
    return jax.shard_map(
        shards,
        mesh=mesh,
        in_specs=(P("sp", "tp"), P(None, "tp"), P(None, "tp"), P(None, "tp"), P("tp", None), P("sp", "tp")),
        out_specs=(P("sp", "tp"), P("sp", "tp"), P("sp", "tp"), P("sp", "tp"), P("tp", None)),
        check_vma=False,
    )
```

```python
import functools

import jax
import jax.numpy as jnp
from jax import lax
from jax.experimental import pallas as pl
from jax.experimental.pallas import tpu as pltpu
from jax.sharding import PartitionSpec as P

MESH = pl.DeviceIdType.MESH
BF16, F32 = jnp.bfloat16, jnp.float32
SEGMENT, REACH, CLIP, HEAD = 64, 256, 256, 128
TILE = 128
SPAN = REACH + TILE
LENGTH, WIDTH, FEATURES = 768, 4096, 512
CHUNKS = LENGTH // TILE
HEADS = 2
COLS = HEADS * HEAD
FACTOR = HEAD ** (-0.5)
RING = 4
TABLE = 320
ROUND = 512


def dot(left, right, left_dim=1, right_dim=0):
    return lax.dot_general(left, right, (((left_dim,), (right_dim,)), ((), ())), preferred_element_type=F32)


class Ring:
    def __init__(self, me, up, down, block, via, direct, joined, sent, far_sem, rest_sem):
        self.near = (lax.rem(me + 1, RING), lax.rem(me + RING - 1, RING))
        self.far = lax.rem(me + 2, RING)
        self.me, self.devices, self.block = me, (up, down), block
        self.landing = (via, direct, joined)
        self.sent, self.arrived = sent, (far_sem, rest_sem, rest_sem)

    def start(self, kind, d):
        source = (self.block(self.far, d), self.block(self.near[d], 1 - d), self.block(self.near[d], d))[kind]
        pltpu.make_async_remote_copy(
            src_ref=source,
            dst_ref=self.landing[kind](d),
            send_sem=self.sent,
            recv_sem=self.arrived[kind],
            device_id=self.devices[d],
            device_id_type=MESH,
        ).start()

    def start_far(self):
        for d in range(2):
            self.start(0, d)

    def start_near(self, d):
        self.start(1, d)

    def join(self):
        for d in range(2):
            ref = self.block(self.near[d], d)
            ref[...] = (ref[...].astype(F32) + self.landing[0](d)[...].astype(F32)).astype(BF16)
            self.start(2, d)

    def half(self, d):
        total = self.block(self.me, d)[...].astype(F32) + self.landing[2](d)[...].astype(F32)
        return total + self.landing[1](1 - d)[...].astype(F32)


def await_bytes(view, sem):
    pltpu.make_async_copy(view, view, sem).wait()


def kernel(
    tokens, wq, wk, wv, table, out_grad,
    input_out, wq_out, wk_out, wv_out, bias_out,
    whole, weight, query, kv, upstream, dkv, grads, grads_t, back_send, back_recv,
    part_a, part_b, far_ab, near_join, second_ab, far2_ab, near_join2,
    term_own, term_send, term_recv, far_y, near_join_y,
    bias, dsum, bias_x, bias_z,
    load_sem, gather_recv, hop_recv, core_recv, halo_recv, term_rs, ring_rs, second_rs, y_rs, bias_rs, sent,
):
    sp, tp = lax.axis_index("sp"), lax.axis_index("tp")
    z, x = sp // RING, lax.rem(sp, RING)
    y, core = tp // 2, lax.rem(tp, 2)

    def at(value, by):
        return lax.rem(value + by, RING)

    def at_x(by):
        return (z * RING + at(x, by), tp)

    def at_z(by):
        return (at(z, by) * RING + x, tp)

    def at_y(by):
        return (sp, at(y, by) * 2 + core)

    def at_sp(by):
        return (lax.rem(sp + by, 16), tp)

    partner = (sp, y * 2 + 1 - core)

    barrier = pltpu.get_barrier_semaphore()
    peers = [partner, at_sp(1), at_sp(15)]
    for by in (1, 3):
        peers.append(at_y(by))
    for by in (1, 2, 3):
        peers += [at_x(by), at_z(by)]
    for peer in peers:
        pl.semaphore_signal(barrier, inc=1, device_id=peer, device_id_type=MESH)

    def feature_cols(y_index, core_index):
        return pl.ds(pl.multiple_of((y_index * 2 + core_index) * FEATURES, FEATURES), FEATURES)

    my_cols = feature_cols(y, core)
    own_load = pltpu.make_async_copy(tokens, whole.at[:, my_cols], load_sem.at[0])
    own_load.start()
    with jax.named_scope("entry"):
        own_load.wait()
        pl.semaphore_wait(barrier, len(peers))

    def rows_of(step):
        return pl.multiple_of(lax.rem(step + 4, CHUNKS) * TILE, TILE)

    def chunk_copy(rows, cols, target, send, recv):
        view = whole.at[rows, cols]
        return pltpu.make_async_remote_copy(
            src_ref=view, dst_ref=view, send_sem=send, recv_sem=recv, device_id=target, device_id_type=MESH
        )

    up, down = at_y(1), at_y(3)

    def gather_copy(step, d):
        return chunk_copy(pl.ds(rows_of(step), TILE), my_cols, (up, down)[d], sent.at[0], gather_recv.at[step])

    def hop_copy(step, d):
        cols = feature_cols(at(y, (3, 1)[d]), core)
        rows = pl.ds(pl.multiple_of(rows_of(step) + d * SEGMENT, SEGMENT), SEGMENT)
        return chunk_copy(rows, cols, (up, down)[d], sent.at[1], hop_recv.at[step])

    def core_copy(step, which):
        cols = feature_cols(at(y, (0, 3, 1, 2)[which]), core)
        return chunk_copy(pl.ds(rows_of(step), TILE), cols, partner, sent.at[2], core_recv.at[step])

    def halo_copy(step):
        return pltpu.make_async_remote_copy(
            src_ref=kv.at[pl.ds(pl.multiple_of(LENGTH + step * TILE, TILE), TILE), :],
            dst_ref=kv.at[pl.ds(pl.multiple_of(step * TILE, TILE), TILE), :],
            send_sem=sent.at[3],
            recv_sem=halo_recv.at[0],
            device_id=at_sp(1),
            device_id_type=MESH,
        )

    back_copy = pltpu.make_async_remote_copy(
        src_ref=back_send,
        dst_ref=back_recv,
        send_sem=sent.at[4],
        recv_sem=halo_recv.at[1],
        device_id=at_sp(15),
        device_id_type=MESH,
    )

    edge = jnp.where(sp == 0, REACH, 0)
    row = lax.broadcasted_iota(jnp.int32, (SPAN, TILE), 0)

    def attend(tile):
        start = pl.multiple_of(tile * TILE, TILE)
        keys_at, here = pl.ds(start, SPAN), pl.ds(start, TILE)
        heads = []
        for h in range(HEADS):
            cols = slice(h * HEAD, (h + 1) * HEAD)
            value_cols = slice(COLS + h * HEAD, COLS + (h + 1) * HEAD)
            keys, values = kv[keys_at, cols], kv[keys_at, value_cols]
            asked, given = query[here, cols], upstream[here, cols]
            heads.append((cols, value_cols, keys, asked, given, dot(keys, asked, 1, 1), dot(values, given, 1, 1)))
        lows = []
        for h in range(HEADS):
            scores = heads[h][5] * FACTOR + bias[h]
            scores = jnp.where(row + start < edge, -jnp.inf, scores)
            top = jnp.max(scores, axis=0, keepdims=True)
            raised = jnp.exp(scores - top)
            weights = raised * (1.0 / jnp.sum(raised, axis=0, keepdims=True))
            prob_grad = heads[h][6]
            delta = jnp.sum(weights * prob_grad, axis=0, keepdims=True)
            score_grad = weights * (prob_grad - delta)
            dsum[h] = dsum[h] + score_grad
            lows.append((weights.astype(BF16), score_grad.astype(BF16)))
        for h in range(HEADS):
            cols, value_cols, keys, asked, given = heads[h][:5]
            weights_low, score_low = lows[h]
            dkv[keys_at, value_cols] = dkv[keys_at, value_cols] + dot(weights_low, given)
            dkv[keys_at, cols] = dkv[keys_at, cols] + dot(score_low, asked)
            query_grad = dot(score_low, keys, 0, 0) * FACTOR
            grads[here, cols] = query_grad.astype(BF16)
            grads_t[cols, here] = query_grad.T.astype(BF16)

    for step in range(2):
        for d in range(2):
            gather_copy(step, d).start()
        core_copy(step, 0).start()

    loads = []
    for number, ref in enumerate((wq, wk, wv)):
        loads.append(pltpu.make_async_copy(ref, weight.at[:, number * COLS : (number + 1) * COLS], load_sem.at[1 + number]))
    loads.append(pltpu.make_async_copy(out_grad, upstream, load_sem.at[4]))
    for load in loads:
        load.start()

    lane = lax.broadcasted_iota(jnp.int32, (8, ROUND), 1)
    column = lax.broadcasted_iota(jnp.int32, (SPAN, TILE), 1)
    low = jnp.where(column >= SEGMENT, SEGMENT, 0)
    seen = (row >= low) & (row < low + REACH + SEGMENT)
    for h in range(HEADS):
        entries = jnp.broadcast_to(table[h : h + 1, :], (8, TABLE))
        padded = jnp.concatenate([entries, jnp.zeros((8, ROUND - TABLE), F32)], axis=1)
        turned = pltpu.roll(padded, ROUND - TABLE + 1, 1)
        last = jnp.broadcast_to(table[h : h + 1, TABLE - 1 : TABLE], (8, ROUND))
        turned = jnp.where(lane < TILE, last, turned)
        skewed = pltpu.roll(jnp.broadcast_to(turned[0:1, :], (SPAN, ROUND)), 0, 1, stride=1, stride_axis=0)
        bias[h] = jnp.where(seen, skewed[:, :TILE], -jnp.inf)
        dsum[h] = jnp.zeros((SPAN, TILE), F32)
    dkv[...] = jnp.zeros(dkv.shape, F32)

    for load in loads:
        load.wait()

    def gather_step(s, carry):
        @pl.when(s < CHUNKS)
        def _():
            with jax.named_scope("gather_wait"):
                await_bytes(whole.at[0 : 2 * TILE, 0:FEATURES], gather_recv.at[s])
                for d in range(2):
                    hop_copy(s, d).start()
                for d in range(2):
                    core_copy(s, 1 + d).start()

        @pl.when(s < CHUNKS - 2)
        def _():
            for d in range(2):
                gather_copy(s + 2, d).start()
            core_copy(s + 2, 0).start()

        @pl.when((s >= 1) & (s <= CHUNKS))
        def _():
            with jax.named_scope("hop_wait"):
                await_bytes(whole.at[0:TILE, 0:FEATURES], hop_recv.at[s - 1])
                core_copy(s - 1, 3).start()

        @pl.when(s == 4)
        def _():
            with jax.named_scope("halo_wait"):
                await_bytes(kv.at[0:REACH, :], halo_recv.at[0])

        @pl.when(s >= 4)
        def _():
            with jax.named_scope("attend"):
                attend(s - 4)

        @pl.when(s == 5)
        def _():
            back_send[...] = dkv[0:REACH, :].astype(BF16)
            back_copy.start()

        @pl.when((s >= 1) & (s <= CHUNKS))
        def _():
            with jax.named_scope("core_wait"):
                await_bytes(whole.at[0:TILE, 0 : 4 * FEATURES], core_recv.at[s - 1])

            with jax.named_scope("project"):
                start = rows_of(s - 1)
                projected = dot(whole[pl.ds(start, TILE), :], weight[...]).astype(BF16)
                query[pl.ds(start, TILE), :] = projected[:, :COLS]
                kv[pl.ds(pl.multiple_of(start + REACH, TILE), TILE), :] = projected[:, COLS:]

        @pl.when((s >= 1) & (s <= 2))
        def _():
            halo_copy(s - 1).start()

        return carry

    lax.fori_loop(0, CHUNKS + 4, gather_step, 0)

    def first_ring(p, side):
        me = (x, z)[side]
        part = (part_a, part_b)[side]
        at_side = (at_x, at_z)[side]
        return Ring(
            me, at_side(1), at_side(3),
            lambda k, half: part.at[p, k, pl.ds(2 * half, 2)],
            lambda d: far_ab.at[p, side, d],
            lambda d: near_join.at[p, 0, side, d],
            lambda d: near_join.at[p, 1, side, d],
            sent.at[5], ring_rs.at[p, 0], ring_rs.at[p, 1],
        )

    def second_ring(p, side):
        me = (z, x)[side]
        at_side = (at_z, at_x)[side]
        return Ring(
            me, at_side(1), at_side(3),
            lambda k, half: second_ab.at[p, side, k, half * SEGMENT : (half + 1) * SEGMENT],
            lambda d: far2_ab.at[p, side, d],
            lambda d: near_join2.at[p, 0, side, d],
            lambda d: near_join2.at[p, 1, side, d],
            sent.at[6], second_rs.at[p, 0], second_rs.at[p, 1],
        )

    y_ring = Ring(
        y, up, down,
        lambda k, half: term_own.at[k, half * (LENGTH // 2) : (half + 1) * (LENGTH // 2)],
        lambda d: far_y.at[d],
        lambda d: near_join_y.at[0, d],
        lambda d: near_join_y.at[1, d],
        sent.at[7], y_rs.at[0], y_rs.at[1],
    )

    def term(y_index, core_index):
        start = pl.multiple_of((y_index * 2 + core_index) * FEATURES, FEATURES)
        return dot(grads[...], weight[pl.ds(start, FEATURES), :], 1, 1)

    def term_copy(k):
        return pltpu.make_async_remote_copy(
            src_ref=term_send.at[k],
            dst_ref=term_recv.at[k],
            send_sem=sent.at[8],
            recv_sem=term_rs.at[k],
            device_id=partner,
            device_id_type=MESH,
        )

    def send_term(k):
        with jax.named_scope("term_send"):
            term_send[k] = term(at(y, ahead(k)), 1 - core).astype(BF16)
        term_copy(k).start()

    def ahead(k):
        return jnp.where(k == 0, 2, jnp.where(k == 1, 1, jnp.where(k == 2, 3, 0)))

    def bias_send(buffer, me, targets, which):
        view = buffer.at[me]
        for target in targets:
            pltpu.make_async_remote_copy(
                src_ref=view, dst_ref=view, send_sem=sent.at[9], recv_sem=bias_rs.at[which], device_id=target, device_id_type=MESH
            ).start()

    def bias_sums():
        bias_x[x] = jnp.zeros((8, ROUND), F32)
        for h in range(HEADS):
            wide = jnp.concatenate([dsum[h], jnp.zeros((SPAN, ROUND - TILE), F32)], axis=1)
            rows = SPAN
            while rows > 24:
                rows //= 2
                wide = wide[:rows] + pltpu.roll(wide[rows:], ROUND - rows, 1)
            wide = wide[0:8] + pltpu.roll(wide[8:16], ROUND - 8, 1) + pltpu.roll(wide[16:24], ROUND - 16, 1)
            sums = wide[0:1]
            for r in range(1, 8):
                sums = sums + pltpu.roll(wide[r : r + 1], ROUND - r, 1)
            first = lax.broadcasted_iota(jnp.int32, (1, ROUND), 1)
            clipped = jnp.sum(jnp.where(first < TILE, sums, 0.0), axis=1, keepdims=True)
            placed = pltpu.roll(sums, TABLE - 1, 1)
            bias_x[x, h : h + 1, :] = jnp.where(first == TABLE - 1, clipped, placed)

    def finish():
        with jax.named_scope("back_wait"):
            back_copy.wait_recv()
            dkv[LENGTH:, :] = dkv[LENGTH:, :] + back_recv[...].astype(F32)

        def finish_chunk(chunk, carry):
            start = pl.multiple_of(chunk * TILE, TILE)
            total = dkv[pl.ds(pl.multiple_of(start + REACH, TILE), TILE), :]
            total = jnp.concatenate([total[:, :COLS] * FACTOR, total[:, COLS:]], axis=1)
            grads[pl.ds(start, TILE), COLS:] = total.astype(BF16)
            grads_t[COLS:, pl.ds(start, TILE)] = total.T.astype(BF16)
            return carry

        with jax.named_scope("finish"):
            lax.fori_loop(0, CHUNKS, finish_chunk, 0)

    def weight_part(k):
        def rows(i, inner):
            z_index = at(z, 2 + i)
            left = grads_t[pl.ds(pl.multiple_of(k * COLS, COLS), COLS), :]
            features = pl.ds(pl.multiple_of(z_index * RING * COLS, RING * COLS), RING * COLS)
            made = dot(left, whole[:, features]).astype(BF16)
            for x_index in range(RING):
                cut = slice(x_index * COLS, (x_index + 1) * COLS)
                part_b[k, z_index, x_index] = made[HEAD:, cut]

                @pl.when((k > 0) | (x_index != at(x, 2)))
                def _():
                    part_a[k, x_index, z_index] = made[:HEAD, cut]

            @pl.when(i == 0)
            def _():
                first_ring(k, 1).start_far()

            return inner

        with jax.named_scope("weight_rows"):
            lax.fori_loop(0, RING, rows, 0)

        @pl.when(k > 0)
        def _():
            first_ring(k, 0).start_far()

        for side in range(2):
            for d in range(2):
                first_ring(k, side).start_near(d)

    def own_term(k):
        with jax.named_scope("term_own"):
            y_index = at(y, ahead(k))
            made = term(y_index, core)
            term_copy(k).wait_recv()
            term_own[y_index] = (made + term_recv[k].astype(F32)).astype(BF16)

    with jax.named_scope("weight_first"):
        far_x = at(x, 2)
        for z_index in range(RING):
            features = pl.ds(pl.multiple_of(z_index * RING * COLS + far_x * COLS, COLS), COLS)
            part_a[0, far_x, z_index] = dot(grads_t[0:HEAD, :], whole[:, features]).astype(BF16)
        first_ring(0, 0).start_far()

    def first_join(p):
        with jax.named_scope("join_first"):
            await_bytes(far_ab.at[p], ring_rs.at[p, 0])
            for side in range(2):
                first_ring(p, side).join()

    def reduce_step(k, carry):
        @pl.when(k < 3)
        def _():
            weight_part(k)

        @pl.when(k == 0)
        def _():
            finish()
            with jax.named_scope("bias_sums"):
                bias_sums()
            bias_send(bias_x, x, [at_x(by) for by in (1, 2, 3)], 0)

        @pl.when(k >= 1)
        def _():
            own_term(k - 1)

        @pl.when(k == 1)
        def _():
            y_ring.start_far()

        for d in range(2):
            @pl.when(k == 2 + d)
            def _():
                y_ring.start_near(d)

        @pl.when(k < RING)
        def _():
            send_term(k)

        @pl.when((k >= 1) & (k < 3))
        def _():
            first_join(k - 1)

        @pl.when(k == 3)
        def _():
            with jax.named_scope("bias_x"):
                await_bytes(bias_x.at[0:3], bias_rs.at[0])
                bias_z[z] = (bias_x[0] + bias_x[1]) + (bias_x[2] + bias_x[3])
                bias_send(bias_z, z, [at_z(by) for by in (1, 2, 3)], 1)

        return carry

    lax.fori_loop(0, RING + 1, reduce_step, 0)

    with jax.named_scope("join_y"):
        await_bytes(far_y, y_rs.at[0])
        y_ring.join()

    def second_start(p):
        with jax.named_scope(f"second_start_{p}"):
            await_bytes(near_join.at[p], ring_rs.at[p, 1])
            for side in range(2):
                ring = first_ring(p, side)
                for half in range(2):
                    second_ab[p, side, 2 * half : 2 * half + 2] = ring.half(half).astype(BF16)
            rings = [second_ring(p, side) for side in range(2)]
            for ring in rings:
                ring.start_far()
            for ring in rings:
                for d in range(2):
                    ring.start_near(d)

    def second_join(p):
        with jax.named_scope(f"second_join_{p}"):
            await_bytes(far2_ab.at[p], second_rs.at[p, 0])
            for side in range(2):
                second_ring(p, side).join()

    def second_finish(p):
        with jax.named_scope(f"second_finish_{p}"):
            await_bytes(near_join2.at[p], second_rs.at[p, 1])
            for side in range(2):
                ring = second_ring(p, side)
                total = jnp.concatenate([ring.half(0), ring.half(1)], axis=0)
                (wq_out, wk_out, wv_out)[p][:, side * HEAD : (side + 1) * HEAD] = total.T

    second_start(0)
    first_join(2)
    second_start(1)
    second_join(0)
    second_start(2)
    second_join(1)
    second_finish(0)
    with jax.named_scope("bias_z"):
        await_bytes(bias_z.at[0:3], bias_rs.at[1])
        bias_out[...] = ((bias_z[0] + bias_z[1]) + (bias_z[2] + bias_z[3]))[:HEADS, :TABLE]
    second_join(2)
    second_finish(1)
    with jax.named_scope("input_sum"):
        await_bytes(near_join_y, y_rs.at[1])
        for d in range(2):
            input_out[d * (LENGTH // 2) : (d + 1) * (LENGTH // 2), :] = y_ring.half(d).astype(BF16)
    second_finish(2)

    with jax.named_scope("drain"):
        await_bytes(whole.at[:, 0 : 2 * FEATURES], sent.at[0])
        await_bytes(whole.at[:, 0:FEATURES], sent.at[1])
        await_bytes(whole.at[:, 0 : 4 * FEATURES], sent.at[2])
        await_bytes(kv.at[0:REACH, :], sent.at[3])
        await_bytes(back_send, sent.at[4])
        await_bytes(far_ab, sent.at[5])
        await_bytes(near_join, sent.at[5])
        await_bytes(far2_ab, sent.at[6])
        await_bytes(near_join2, sent.at[6])
        await_bytes(far_y, sent.at[7])
        await_bytes(near_join_y, sent.at[7])
        await_bytes(term_recv, sent.at[8])
        await_bytes(bias_x.at[0:3], sent.at[9])
        await_bytes(bias_z.at[0:3], sent.at[9])


def shards(tokens, query_weight, key_weight, value_weight, position_bias, out_grad):
    anywhere = pl.BlockSpec(memory_space=pl.ANY)
    near = pl.BlockSpec(memory_space=pltpu.VMEM)
    dma = pltpu.SemaphoreType.DMA
    vmem = pltpu.VMEM
    grad = vmem((COLS, COLS), F32)
    return pl.pallas_call(
        kernel,
        name="segment_attention_grads",
        out_shape=(
            vmem((LENGTH, FEATURES), BF16), grad, grad, grad,
            vmem((HEADS, TABLE), F32),
        ),
        in_specs=[anywhere, anywhere, anywhere, anywhere, near, anywhere],
        out_specs=(near,) * 5,
        scratch_shapes=[
            vmem((LENGTH, WIDTH), BF16),
            vmem((WIDTH, 3 * COLS), BF16),
            vmem((LENGTH, COLS), BF16),
            vmem((REACH + LENGTH, 2 * COLS), BF16),
            vmem((LENGTH, COLS), BF16),
            vmem((REACH + LENGTH, 2 * COLS), F32),
            vmem((LENGTH, 3 * COLS), BF16),
            vmem((3 * COLS, LENGTH), BF16),
            vmem((REACH, 2 * COLS), BF16),
            vmem((REACH, 2 * COLS), BF16),
            vmem((3, RING, RING, HEAD, COLS), BF16),
            vmem((3, RING, RING, HEAD, COLS), BF16),
            vmem((3, 2, 2, 2, HEAD, COLS), BF16),
            vmem((3, 2, 2, 2, 2, HEAD, COLS), BF16),
            vmem((3, 2, RING, HEAD, COLS), BF16),
            vmem((3, 2, 2, SEGMENT, COLS), BF16),
            vmem((3, 2, 2, 2, SEGMENT, COLS), BF16),
            vmem((RING, LENGTH, FEATURES), BF16),
            vmem((RING, LENGTH, FEATURES), BF16),
            vmem((RING, LENGTH, FEATURES), BF16),
            vmem((2, LENGTH // 2, FEATURES), BF16),
            vmem((2, 2, LENGTH // 2, FEATURES), BF16),
            vmem((HEADS, SPAN, TILE), F32),
            vmem((HEADS, SPAN, TILE), F32),
            vmem((RING, 8, ROUND), F32),
            vmem((RING, 8, ROUND), F32),
            dma((5,)),
            dma((CHUNKS,)), dma((CHUNKS,)), dma((CHUNKS,)),
            dma((3,)),
            dma((RING,)),
            dma((3, 2)), dma((3, 2)), dma((2,)),
            dma((2,)),
            dma((10,)),
        ],
        compiler_params=pltpu.CompilerParams(
            collective_id=0, has_side_effects=True, vmem_limit_bytes=62_000_000
        ),
    )(tokens, query_weight, key_weight, value_weight, position_bias, out_grad)


def solution(mesh):
    return jax.shard_map(
        shards,
        mesh=mesh,
        in_specs=(P("sp", "tp"), P(None, "tp"), P(None, "tp"), P(None, "tp"), P("tp", None), P("sp", "tp")),
        out_specs=(P("sp", "tp"), P("sp", "tp"), P("sp", "tp"), P("sp", "tp"), P("tp", None)),
        check_vma=False,
    )
```

```python
import functools

import jax
import jax.numpy as jnp
from jax import lax
from jax.experimental import pallas as pl
from jax.experimental.pallas import tpu as pltpu
from jax.sharding import PartitionSpec as P

MESH = pl.DeviceIdType.MESH
BF16, F32 = jnp.bfloat16, jnp.float32
SEGMENT, REACH, CLIP, HEAD = 64, 256, 256, 128
TILE = 128
SPAN = REACH + TILE
LENGTH, WIDTH, FEATURES = 768, 4096, 512
CHUNKS = LENGTH // TILE
HEADS = 2
COLS = HEADS * HEAD
FACTOR = HEAD ** (-0.5)
RING = 4
TABLE = 320
ROUND = 512
AHEAD = (2, 1, 3, 0)


def dot(left, right, left_dim=1, right_dim=0):
    return lax.dot_general(left, right, (((left_dim,), (right_dim,)), ((), ())), preferred_element_type=F32)


class Ring:
    def __init__(self, me, up, down, block, via, direct, joined, sent, far_sem, rest_sem):
        self.near = (lax.rem(me + 1, RING), lax.rem(me + RING - 1, RING))
        self.far = lax.rem(me + 2, RING)
        self.me, self.devices, self.block = me, (up, down), block
        self.landing = (via, direct, joined)
        self.sent, self.arrived = sent, (far_sem, rest_sem, rest_sem)

    def start(self, kind, d):
        source = (self.block(self.far, d), self.block(self.near[d], 1 - d), self.block(self.near[d], d))[kind]
        pltpu.make_async_remote_copy(
            src_ref=source,
            dst_ref=self.landing[kind](d),
            send_sem=self.sent,
            recv_sem=self.arrived[kind],
            device_id=self.devices[d],
            device_id_type=MESH,
        ).start()

    def start_far(self):
        for d in range(2):
            self.start(0, d)

    def start_near(self, d):
        self.start(1, d)

    def join(self):
        for d in range(2):
            ref = self.block(self.near[d], d)
            ref[...] = (ref[...].astype(F32) + self.landing[0](d)[...].astype(F32)).astype(BF16)
            self.start(2, d)

    def half(self, d):
        total = self.block(self.me, d)[...].astype(F32) + self.landing[2](d)[...].astype(F32)
        return total + self.landing[1](1 - d)[...].astype(F32)


def await_bytes(view, sem):
    pltpu.make_async_copy(view, view, sem).wait()


def kernel(
    tokens, wq, wk, wv, position_bias, out_grad,
    input_out, wq_out, wk_out, wv_out, bias_out,
    table, whole, weight, projected, query, kv, upstream, dkv, grads, grads_t, back_send, back_recv,
    part_a, part_b, far_ab, near_join, second_ab, far2_ab, near_join2,
    term_own, term_send, term_recv, far_y, near_join_y,
    bias, dsum, bias_x, bias_z,
    load_sem, pass_recv, gather_recv, hop_recv, core_recv, last_recv, halo_recv, term_rs, ring_rs, second_rs, y_rs, bias_rs, sent,
):
    sp, tp = lax.axis_index("sp"), lax.axis_index("tp")
    z, x = sp // RING, lax.rem(sp, RING)
    y, core = tp // 2, lax.rem(tp, 2)

    def at(value, by):
        return lax.rem(value + by, RING)

    def at_x(by):
        return (z * RING + at(x, by), tp)

    def at_z(by):
        return (at(z, by) * RING + x, tp)

    def at_y(by):
        return (sp, at(y, by) * 2 + core)

    def at_sp(by):
        return (lax.rem(sp + by, 16), tp)

    partner = (sp, y * 2 + 1 - core)

    barrier = pltpu.get_barrier_semaphore()
    peers = [partner, at_sp(1), at_sp(15)]
    for by in (1, 3):
        peers.append(at_y(by))
    for by in (1, 2, 3):
        peers += [at_x(by), at_z(by)]
    for peer in peers:
        pl.semaphore_signal(barrier, inc=1, device_id=peer, device_id_type=MESH)

    def feature_cols(y_index, core_index):
        return pl.ds(pl.multiple_of((y_index * 2 + core_index) * FEATURES, FEATURES), FEATURES)

    my_cols = feature_cols(y, core)
    own_loads = []
    for number, (first, last) in enumerate(((4 * TILE, 5 * TILE), (5 * TILE, 6 * TILE), (0, 4 * TILE))):
        own = pltpu.make_async_copy(tokens.at[first:last, :], whole.at[first:last, my_cols], load_sem.at[number])
        own.start()
        own_loads.append(own)
    with jax.named_scope("entry"):
        pl.semaphore_wait(barrier, len(peers))

    def rows_of(step):
        return pl.multiple_of(lax.rem(step + 4, CHUNKS) * TILE, TILE)

    def chunk_copy(rows, cols, target, send, recv):
        view = whole.at[rows, cols]
        return pltpu.make_async_remote_copy(
            src_ref=view, dst_ref=view, send_sem=send, recv_sem=recv, device_id=target, device_id_type=MESH
        )

    up, down = at_y(1), at_y(3)

    def gather_start(step):
        for half in range(2):
            for d in range(2):
                first = pl.multiple_of(rows_of(step) + (half ^ d) * SEGMENT, SEGMENT)
                sem = (pass_recv, gather_recv)[half].at[step]
                chunk_copy(pl.ds(first, SEGMENT), my_cols, (up, down)[d], sent.at[0], sem).start()

    def hop_copy(step, d):
        cols = feature_cols(at(y, (3, 1)[d]), core)
        rows = pl.ds(pl.multiple_of(rows_of(step) + d * SEGMENT, SEGMENT), SEGMENT)
        return chunk_copy(rows, cols, (up, down)[d], sent.at[1], hop_recv.at[step])

    def core_copy(step, which):
        cols = feature_cols(at(y, (0, 3, 1, 2)[which]), core)
        sem = (last_recv if which == 3 else core_recv).at[step]
        return chunk_copy(pl.ds(rows_of(step), TILE), cols, partner, sent.at[2], sem)

    def halo_copy(step):
        return pltpu.make_async_remote_copy(
            src_ref=kv.at[pl.ds(pl.multiple_of(LENGTH + step * TILE, TILE), TILE), :],
            dst_ref=kv.at[pl.ds(pl.multiple_of(step * TILE, TILE), TILE), :],
            send_sem=sent.at[3],
            recv_sem=halo_recv.at[0],
            device_id=at_sp(1),
            device_id_type=MESH,
        )

    def back_start(half):
        rows = slice(half * TILE, (half + 1) * TILE)
        back_send[rows] = dkv[rows, :].astype(BF16)
        pltpu.make_async_remote_copy(
            src_ref=back_send.at[rows],
            dst_ref=back_recv.at[rows],
            send_sem=sent.at[4],
            recv_sem=halo_recv.at[1],
            device_id=at_sp(15),
            device_id_type=MESH,
        ).start()

    edge = jnp.where(sp == 0, REACH, 0)
    row = lax.broadcasted_iota(jnp.int32, (SPAN, TILE), 0)

    def attend(tile):
        start = tile * TILE if isinstance(tile, int) else pl.multiple_of(tile * TILE, TILE)
        keys_at, here = pl.ds(start, SPAN), pl.ds(start, TILE)
        heads = []
        for h in range(HEADS):
            cols = slice(h * HEAD, (h + 1) * HEAD)
            value_cols = slice(COLS + h * HEAD, COLS + (h + 1) * HEAD)
            keys, values = kv[keys_at, cols], kv[keys_at, value_cols]
            asked, given = query[here, cols], upstream[here, cols]
            heads.append((cols, value_cols, keys, asked, given, dot(keys, asked, 1, 1), dot(values, given, 1, 1)))
        lows = []
        for h in range(HEADS):
            scores = heads[h][5] * FACTOR + bias[h]
            if not isinstance(tile, int):
                scores = jnp.where(row + start < edge, -jnp.inf, scores)
            top = jnp.max(scores, axis=0, keepdims=True)
            raised = jnp.exp(scores - top)
            weights = raised * (1.0 / jnp.sum(raised, axis=0, keepdims=True))
            prob_grad = heads[h][6]
            delta = jnp.sum(weights * prob_grad, axis=0, keepdims=True)
            score_grad = weights * (prob_grad - delta)
            dsum[h] = dsum[h] + score_grad
            lows.append((weights.astype(BF16), score_grad.astype(BF16)))
        for h in range(HEADS):
            cols, value_cols, keys, asked, given = heads[h][:5]
            weights_low, score_low = lows[h]
            dkv[keys_at, value_cols] = dkv[keys_at, value_cols] + dot(weights_low, given)
            dkv[keys_at, cols] = dkv[keys_at, cols] + dot(score_low, asked)
            query_grad = dot(score_low, keys, 0, 0) * FACTOR
            grads[here, cols] = query_grad.astype(BF16)
            grads_t[cols, here] = query_grad.T.astype(BF16)

    for step in range(2):
        own_loads[step].wait()
        gather_start(step)
        core_copy(step, 0).start()
    own_loads[2].wait()

    table_load = pltpu.make_async_copy(position_bias, table, load_sem.at[7])
    table_load.start()
    loads = []
    for number, ref in enumerate((wq, wk, wv)):
        loads.append(pltpu.make_async_copy(ref, weight.at[:, number * COLS : (number + 1) * COLS], load_sem.at[3 + number]))
    loads.append(pltpu.make_async_copy(out_grad, upstream, load_sem.at[6]))
    for load in loads:
        load.start()

    lane = lax.broadcasted_iota(jnp.int32, (8, ROUND), 1)
    column = lax.broadcasted_iota(jnp.int32, (SPAN, TILE), 1)
    low = jnp.where(column >= SEGMENT, SEGMENT, 0)
    seen = (row >= low) & (row < low + REACH + SEGMENT)
    table_load.wait()
    for h in range(HEADS):
        entries = jnp.broadcast_to(table[h : h + 1, :], (8, TABLE))
        padded = jnp.concatenate([entries, jnp.zeros((8, ROUND - TABLE), F32)], axis=1)
        turned = pltpu.roll(padded, ROUND - TABLE + 1, 1)
        last = jnp.broadcast_to(table[h : h + 1, TABLE - 1 : TABLE], (8, ROUND))
        turned = jnp.where(lane < TILE, last, turned)
        skewed = pltpu.roll(jnp.broadcast_to(turned[0:1, :], (SPAN, ROUND)), 0, 1, stride=1, stride_axis=0)
        bias[h] = jnp.where(seen, skewed[:, :TILE], -jnp.inf)
        dsum[h] = jnp.zeros((SPAN, TILE), F32)
    dkv[...] = jnp.zeros(dkv.shape, F32)

    for load in loads:
        load.wait()

    def project_from(step, blocks):
        total = None
        for which in blocks:
            for on in (core, 1 - core):
                cols = feature_cols(at(y, (0, 3, 1, 2)[which]), on)
                part = dot(whole[pl.ds(rows_of(step), TILE), cols], weight[cols, :])
                total = part if total is None else total + part
        return total

    def hop_landed(step):
        with jax.named_scope("hop_wait"):
            await_bytes(whole.at[0:TILE, 0:FEATURES], hop_recv.at[step])
            core_copy(step, 3).start()

    def gather_step(s, carry):
        @pl.when(s < CHUNKS)
        def _():
            with jax.named_scope("pass_wait"):
                await_bytes(whole.at[0:TILE, 0:FEATURES], pass_recv.at[s])
                for d in range(2):
                    hop_copy(s, d).start()

        @pl.when(s < CHUNKS - 2)
        def _():
            gather_start(s + 2)
            core_copy(s + 2, 0).start()

        @pl.when(s == CHUNKS)
        def _():
            hop_landed(s - 1)

        @pl.when(s >= 1)
        def _():
            with jax.named_scope("core_wait"):
                await_bytes(whole.at[0:TILE, 0 : 3 * FEATURES], core_recv.at[s - 1])
            with jax.named_scope("project"):
                projected[...] = project_from(s - 1, (0, 1, 2))

        @pl.when(s < CHUNKS)
        def _():
            with jax.named_scope("gather_wait"):
                await_bytes(whole.at[0:TILE, 0:FEATURES], gather_recv.at[s])
                for d in range(2):
                    core_copy(s, 1 + d).start()

        @pl.when((s >= 1) & (s < CHUNKS))
        def _():
            hop_landed(s - 1)

        @pl.when(s == 4)
        def _():
            with jax.named_scope("halo_wait"):
                await_bytes(kv.at[0:REACH, :], halo_recv.at[0])

        @pl.when((s == 4) | (s == 6))
        def _():
            with jax.named_scope("attend"):
                attend(jnp.where(s == 4, 0, 2))

            @pl.when(s == 4)
            def _():
                back_start(0)

        @pl.when(s >= 1)
        def _():
            with jax.named_scope("last_wait"):
                await_bytes(whole.at[0:TILE, 0:FEATURES], last_recv.at[s - 1])
            with jax.named_scope("project_rest"):
                start = rows_of(s - 1)
                low = (projected[...] + project_from(s - 1, (3,))).astype(BF16)
                query[pl.ds(start, TILE), :] = low[:, :COLS]
                kv[pl.ds(pl.multiple_of(start + REACH, TILE), TILE), :] = low[:, COLS:]

        @pl.when((s >= 1) & (s <= 2))
        def _():
            halo_copy(s - 1).start()

        @pl.when(s == 4)
        def _():
            with jax.named_scope("attend"):
                attend(s - 3)
            back_start(1)

        return carry

    lax.fori_loop(0, CHUNKS + 1, gather_step, 0)
    with jax.named_scope("attend_last"):
        for tile in range(3, CHUNKS):
            attend(tile)

    def first_ring(p, side):
        me = (x, z)[side]
        part = (part_a, part_b)[side]
        at_side = (at_x, at_z)[side]
        return Ring(
            me, at_side(1), at_side(3),
            lambda k, half: part.at[p, k, pl.ds(2 * half, 2)],
            lambda d: far_ab.at[p, side, d],
            lambda d: near_join.at[p, 0, side, d],
            lambda d: near_join.at[p, 1, side, d],
            sent.at[5], ring_rs.at[p, 0], ring_rs.at[p, 1],
        )

    def second_ring(p, side):
        me = (z, x)[side]
        at_side = (at_z, at_x)[side]
        return Ring(
            me, at_side(1), at_side(3),
            lambda k, half: second_ab.at[p, side, k, half * SEGMENT : (half + 1) * SEGMENT],
            lambda d: far2_ab.at[p, side, d],
            lambda d: near_join2.at[p, 0, side, d],
            lambda d: near_join2.at[p, 1, side, d],
            sent.at[6], second_rs.at[p, 0], second_rs.at[p, 1],
        )

    y_ring = Ring(
        y, up, down,
        lambda k, half: term_own.at[k, half * (LENGTH // 2) : (half + 1) * (LENGTH // 2)],
        lambda d: far_y.at[d],
        lambda d: near_join_y.at[0, d],
        lambda d: near_join_y.at[1, d],
        sent.at[7], y_rs.at[0], y_rs.at[1],
    )

    halves = (slice(0, LENGTH // 2), slice(LENGTH // 2, LENGTH))

    def term(y_index, core_index, rows):
        start = pl.multiple_of((y_index * 2 + core_index) * FEATURES, FEATURES)
        return dot(grads[rows, :], weight[pl.ds(start, FEATURES), :], 1, 1)

    def send_term(k, rows, sem):
        with jax.named_scope("term_send"):
            term_send[k, rows] = term(at(y, AHEAD[k]), 1 - core, rows).astype(BF16)
        pltpu.make_async_remote_copy(
            src_ref=term_send.at[k, rows],
            dst_ref=term_recv.at[k, rows],
            send_sem=sent.at[8],
            recv_sem=term_rs.at[sem],
            device_id=partner,
            device_id_type=MESH,
        ).start()

    def own_term(k, rows, sem):
        with jax.named_scope("term_own"):
            y_index = at(y, AHEAD[k])
            made = term(y_index, core, rows)
            await_bytes(term_recv.at[k, rows], term_rs.at[sem])
            term_own[y_index, rows] = (made + term_recv[k, rows].astype(F32)).astype(BF16)

    def bias_send(buffer, me, targets, which):
        view = buffer.at[me]
        for target in targets:
            pltpu.make_async_remote_copy(
                src_ref=view, dst_ref=view, send_sem=sent.at[9], recv_sem=bias_rs.at[which], device_id=target, device_id_type=MESH
            ).start()

    def bias_sums():
        bias_x[x] = jnp.zeros((8, TILE), F32)
        for h in range(HEADS):
            wide = jnp.concatenate([dsum[h], jnp.zeros((SPAN, ROUND - TILE), F32)], axis=1)
            rows = SPAN
            while rows > 24:
                rows //= 2
                wide = wide[:rows] + pltpu.roll(wide[rows:], ROUND - rows, 1)
            wide = wide[0:8] + pltpu.roll(wide[8:16], ROUND - 8, 1) + pltpu.roll(wide[16:24], ROUND - 16, 1)
            sums = wide[0:1]
            for r in range(1, 8):
                sums = sums + pltpu.roll(wide[r : r + 1], ROUND - r, 1)
            first = lax.broadcasted_iota(jnp.int32, (1, ROUND), 1)
            clipped = jnp.sum(jnp.where(first < TILE, sums, 0.0), axis=1, keepdims=True)
            placed = pltpu.roll(sums, TABLE - 1, 1)
            sums = jnp.where(first == TABLE - 1, clipped, placed)
            for piece in range(3):
                bias_x[x, 3 * h + piece : 3 * h + piece + 1, :] = sums[:, piece * TILE : (piece + 1) * TILE]

    def finish():
        with jax.named_scope("back_wait"):
            await_bytes(back_recv, halo_recv.at[1])
            dkv[LENGTH:, :] = dkv[LENGTH:, :] + back_recv[...].astype(F32)

        def finish_chunk(chunk, carry):
            start = pl.multiple_of(chunk * TILE, TILE)
            total = dkv[pl.ds(pl.multiple_of(start + REACH, TILE), TILE), :]
            total = jnp.concatenate([total[:, :COLS] * FACTOR, total[:, COLS:]], axis=1)
            grads[pl.ds(start, TILE), COLS:] = total.astype(BF16)
            grads_t[COLS:, pl.ds(start, TILE)] = total.T.astype(BF16)
            return carry

        with jax.named_scope("finish"):
            lax.fori_loop(0, CHUNKS, finish_chunk, 0)

    def weight_row(k, z_index):
        features = pl.ds(pl.multiple_of(z_index * RING * COLS, RING * COLS), RING * COLS)
        made = dot(grads_t[k * COLS : (k + 1) * COLS, :], whole[:, features]).astype(BF16)
        for x_index in range(RING):
            cut = slice(x_index * COLS, (x_index + 1) * COLS)
            part_b[k, z_index, x_index] = made[HEAD:, cut]

            @pl.when(x_index != at(x, 2))
            def _():
                part_a[k, x_index, z_index] = made[:HEAD, cut]

    def weight_far(k):
        far_x = at(x, 2)
        with jax.named_scope("weight_far"):
            for z_index in range(RING):
                features = pl.ds(pl.multiple_of(z_index * RING * COLS + far_x * COLS, COLS), COLS)
                left = grads_t[k * COLS : k * COLS + HEAD, :]
                part_a[k, far_x, z_index] = dot(left, whole[:, features]).astype(BF16)
            first_ring(k, 0).start_far()
            weight_row(k, at(z, 2))
            first_ring(k, 1).start_far()

    def weight_rest(k):
        def rows(i, inner):
            weight_row(k, at(z, i))
            return inner

        with jax.named_scope("weight_rest"):
            lax.fori_loop(3, RING + 2, rows, 0)
        for side in range(2):
            for d in range(2):
                first_ring(k, side).start_near(d)

    def first_join(p):
        with jax.named_scope("join_first"):
            await_bytes(far_ab.at[p], ring_rs.at[p, 0])
            for side in range(2):
                first_ring(p, side).join()

    whole_rows = slice(0, LENGTH)
    weight_far(0)
    weight_rest(0)
    finish()
    for half in range(2):
        send_term(0, halves[half], half)
    weight_far(1)
    for half in range(2):
        own_term(0, halves[half], half)
        y_ring.start(0, half)
    send_term(1, whole_rows, 2)
    weight_rest(1)
    first_join(0)
    with jax.named_scope("bias_sums"):
        bias_sums()
    bias_send(bias_x, x, [at_x(by) for by in (1, 2, 3)], 0)
    own_term(1, whole_rows, 2)
    y_ring.start_near(0)
    weight_far(2)
    send_term(2, whole_rows, 3)
    send_term(3, whole_rows, 4)
    own_term(2, whole_rows, 3)
    y_ring.start_near(1)
    weight_rest(2)
    first_join(1)
    with jax.named_scope("join_y"):
        await_bytes(far_y, y_rs.at[0])
        y_ring.join()
    with jax.named_scope("bias_x"):
        await_bytes(bias_x.at[0:3], bias_rs.at[0])
        bias_z[z] = (bias_x[0] + bias_x[1]) + (bias_x[2] + bias_x[3])
    bias_send(bias_z, z, [at_z(by) for by in (1, 2, 3)], 1)
    own_term(3, whole_rows, 4)

    def second_start(p):
        with jax.named_scope(f"second_start_{p}"):
            await_bytes(near_join.at[p], ring_rs.at[p, 1])
            for side in range(2):
                ring = first_ring(p, side)
                for half in range(2):
                    second_ab[p, side, 2 * half : 2 * half + 2] = ring.half(half).astype(BF16)
            rings = [second_ring(p, side) for side in range(2)]
            for ring in rings:
                ring.start_far()
            for ring in rings:
                for d in range(2):
                    ring.start_near(d)

    def second_join(p):
        with jax.named_scope(f"second_join_{p}"):
            await_bytes(far2_ab.at[p], second_rs.at[p, 0])
            for side in range(2):
                second_ring(p, side).join()

    def second_finish(p):
        with jax.named_scope(f"second_finish_{p}"):
            await_bytes(near_join2.at[p], second_rs.at[p, 1])
            for side in range(2):
                ring = second_ring(p, side)
                total = jnp.concatenate([ring.half(0), ring.half(1)], axis=0)
                (wq_out, wk_out, wv_out)[p][:, side * HEAD : (side + 1) * HEAD] = total.T

    second_start(0)
    first_join(2)
    second_start(1)
    second_join(0)
    second_start(2)
    second_join(1)
    second_finish(0)
    with jax.named_scope("bias_z"):
        await_bytes(bias_z.at[0:3], bias_rs.at[1])
        sums = (bias_z[0] + bias_z[1]) + (bias_z[2] + bias_z[3])
        for h in range(HEADS):
            for piece in range(3):
                cut = slice(piece * TILE, min((piece + 1) * TILE, TABLE))
                bias_out[h : h + 1, cut] = sums[3 * h + piece : 3 * h + piece + 1, : cut.stop - cut.start]
    second_join(2)
    second_finish(1)
    with jax.named_scope("input_sum"):
        await_bytes(near_join_y, y_rs.at[1])
        for d in range(2):
            input_out[d * (LENGTH // 2) : (d + 1) * (LENGTH // 2), :] = y_ring.half(d).astype(BF16)
    second_finish(2)

    with jax.named_scope("drain"):
        await_bytes(whole.at[:, 0 : 2 * FEATURES], sent.at[0])
        await_bytes(whole.at[:, 0:FEATURES], sent.at[1])
        await_bytes(whole.at[:, 0 : 4 * FEATURES], sent.at[2])
        await_bytes(kv.at[0:REACH, :], sent.at[3])
        await_bytes(back_send, sent.at[4])
        await_bytes(far_ab, sent.at[5])
        await_bytes(near_join, sent.at[5])
        await_bytes(far2_ab, sent.at[6])
        await_bytes(near_join2, sent.at[6])
        await_bytes(far_y, sent.at[7])
        await_bytes(near_join_y, sent.at[7])
        await_bytes(term_recv, sent.at[8])
        await_bytes(bias_x.at[0:3], sent.at[9])
        await_bytes(bias_z.at[0:3], sent.at[9])


def store_results(*refs):
    sources, targets, sems = refs[:5], refs[5:10], refs[10]
    copies = [pltpu.make_async_copy(source, target, sems.at[n]) for n, (source, target) in enumerate(zip(sources, targets))]
    for copy in copies:
        copy.start()
    for copy in copies:
        copy.wait()


def shards(tokens, query_weight, key_weight, value_weight, position_bias, out_grad):
    anywhere = pl.BlockSpec(memory_space=pl.ANY)
    near = pl.BlockSpec(memory_space=pltpu.VMEM)
    dma = pltpu.SemaphoreType.DMA
    vmem = pltpu.VMEM
    grad = vmem((COLS, COLS), F32)
    results = pl.pallas_call(
        kernel,
        name="segment_attention_grads",
        out_shape=(
            vmem((LENGTH, FEATURES), BF16), grad, grad, grad,
            vmem((HEADS, TABLE), F32),
        ),
        in_specs=[anywhere] * 6,
        out_specs=(near,) * 5,
        scratch_shapes=[
            vmem((HEADS, TABLE), F32),
            vmem((LENGTH, WIDTH), BF16),
            vmem((WIDTH, 3 * COLS), BF16),
            vmem((TILE, 3 * COLS), F32),
            vmem((LENGTH, COLS), BF16),
            vmem((REACH + LENGTH, 2 * COLS), BF16),
            vmem((LENGTH, COLS), BF16),
            vmem((REACH + LENGTH, 2 * COLS), F32),
            vmem((LENGTH, 3 * COLS), BF16),
            vmem((3 * COLS, LENGTH), BF16),
            vmem((REACH, 2 * COLS), BF16),
            vmem((REACH, 2 * COLS), BF16),
            vmem((3, RING, RING, HEAD, COLS), BF16),
            vmem((3, RING, RING, HEAD, COLS), BF16),
            vmem((3, 2, 2, 2, HEAD, COLS), BF16),
            vmem((3, 2, 2, 2, 2, HEAD, COLS), BF16),
            vmem((3, 2, RING, HEAD, COLS), BF16),
            vmem((3, 2, 2, SEGMENT, COLS), BF16),
            vmem((3, 2, 2, 2, SEGMENT, COLS), BF16),
            vmem((RING, LENGTH, FEATURES), BF16),
            vmem((RING, LENGTH, FEATURES), BF16),
            vmem((RING, LENGTH, FEATURES), BF16),
            vmem((2, LENGTH // 2, FEATURES), BF16),
            vmem((2, 2, LENGTH // 2, FEATURES), BF16),
            vmem((HEADS, SPAN, TILE), F32),
            vmem((HEADS, SPAN, TILE), F32),
            vmem((RING, 8, TILE), F32),
            vmem((RING, 8, TILE), F32),
            dma((8,)),
            dma((CHUNKS,)), dma((CHUNKS,)), dma((CHUNKS,)), dma((CHUNKS,)), dma((CHUNKS,)),
            dma((3,)),
            dma((RING + 1,)),
            dma((3, 2)), dma((3, 2)), dma((2,)),
            dma((2,)),
            dma((10,)),
        ],
        compiler_params=pltpu.CompilerParams(
            collective_id=0, has_side_effects=True, vmem_limit_bytes=62_000_000
        ),
    )(tokens, query_weight, key_weight, value_weight, position_bias, out_grad)
    return pl.pallas_call(
        store_results,
        name="store_results",
        out_shape=tuple(jax.ShapeDtypeStruct(result.shape, result.dtype) for result in results),
        in_specs=[near] * 5,
        out_specs=(anywhere,) * 5,
        scratch_shapes=[dma((5,))],
        compiler_params=pltpu.CompilerParams(vmem_limit_bytes=1_000_000),
    )(*results)


def solution(mesh):
    return jax.shard_map(
        shards,
        mesh=mesh,
        in_specs=(P("sp", "tp"), P(None, "tp"), P(None, "tp"), P(None, "tp"), P("tp", None), P("sp", "tp")),
        out_specs=(P("sp", "tp"), P("sp", "tp"), P("sp", "tp"), P("sp", "tp"), P("tp", None)),
        check_vma=False,
    )
```

```python
import functools

import jax
import jax.numpy as jnp
from jax import lax
from jax.experimental import pallas as pl
from jax.experimental.pallas import tpu as pltpu
from jax.sharding import PartitionSpec as P

MESH = pl.DeviceIdType.MESH
BF16, F32 = jnp.bfloat16, jnp.float32
SEGMENT, REACH, CLIP, HEAD = 64, 256, 256, 128
TILE = 128
SPAN = REACH + TILE
LENGTH, WIDTH, FEATURES = 768, 4096, 512
CHUNKS = LENGTH // TILE
HEADS = 2
COLS = HEADS * HEAD
FACTOR = HEAD ** (-0.5)
RING = 4
TABLE = 320
ROUND = 512
AHEAD = (2, 1, 3, 0)
STRAIGHT = (2,)


def dot(left, right, left_dim=1, right_dim=0):
    return lax.dot_general(left, right, (((left_dim,), (right_dim,)), ((), ())), preferred_element_type=F32)


class Ring:
    def __init__(self, me, up, down, block, via, direct, joined, sent, far_sem, rest_sem):
        self.near = (lax.rem(me + 1, RING), lax.rem(me + RING - 1, RING))
        self.far = lax.rem(me + 2, RING)
        self.me, self.devices, self.block = me, (up, down), block
        self.landing = (via, direct, joined)
        self.sent, self.arrived = sent, (far_sem, rest_sem, rest_sem)

    def start(self, kind, d):
        source = (self.block(self.far, d), self.block(self.near[d], 1 - d), self.block(self.near[d], d))[kind]
        pltpu.make_async_remote_copy(
            src_ref=source,
            dst_ref=self.landing[kind](d),
            send_sem=self.sent,
            recv_sem=self.arrived[kind],
            device_id=self.devices[d],
            device_id_type=MESH,
        ).start()

    def start_straight(self, opposite):
        for d in range(2):
            pltpu.make_async_remote_copy(
                src_ref=self.block(self.far, d),
                dst_ref=self.landing[0](d),
                send_sem=self.sent,
                recv_sem=self.arrived[0],
                device_id=opposite,
                device_id_type=MESH,
            ).start()
        for kind in (1, 2):
            for d in range(2):
                self.start(kind, d)

    def start_far(self):
        for d in range(2):
            self.start(0, d)

    def start_near(self, d):
        self.start(1, d)

    def join(self):
        for d in range(2):
            ref = self.block(self.near[d], d)
            ref[...] = (ref[...].astype(F32) + self.landing[0](d)[...].astype(F32)).astype(BF16)
            self.start(2, d)

    def half(self, d):
        total = self.block(self.me, d)[...].astype(F32) + self.landing[2](d)[...].astype(F32)
        return total + self.landing[1](1 - d)[...].astype(F32)


def await_bytes(view, sem):
    pltpu.make_async_copy(view, view, sem).wait()


def kernel(
    tokens, wq, wk, wv, position_bias, out_grad,
    input_out, wq_out, wk_out, wv_out, bias_out,
    table, whole, weight, projected, query, kv, upstream, keys_t, dkv, grads, grads_t, back_send, back_recv,
    part_a, part_b, far_ab, near_join, second_ab, far2_ab, near_join2,
    term_own, term_send, term_recv, far_y, near_join_y,
    bias, dsum, bias_x, bias_z,
    load_sem, pass_recv, gather_recv, hop_recv, core_recv, last_recv, halo_recv, term_rs, ring_rs, second_rs, y_rs, bias_rs, sent,
):
    sp, tp = lax.axis_index("sp"), lax.axis_index("tp")
    z, x = sp // RING, lax.rem(sp, RING)
    y, core = tp // 2, lax.rem(tp, 2)

    def at(value, by):
        return lax.rem(value + by, RING)

    def at_x(by):
        return (z * RING + at(x, by), tp)

    def at_z(by):
        return (at(z, by) * RING + x, tp)

    def at_y(by):
        return (sp, at(y, by) * 2 + core)

    def at_sp(by):
        return (lax.rem(sp + by, 16), tp)

    partner = (sp, y * 2 + 1 - core)

    barrier = pltpu.get_barrier_semaphore()
    peers = [partner, at_sp(1), at_sp(15)]
    for by in (1, 3):
        peers.append(at_y(by))
    for by in (1, 2, 3):
        peers += [at_x(by), at_z(by)]
    for peer in peers:
        pl.semaphore_signal(barrier, inc=1, device_id=peer, device_id_type=MESH)

    def feature_cols(y_index, core_index):
        return pl.ds(pl.multiple_of((y_index * 2 + core_index) * FEATURES, FEATURES), FEATURES)

    my_cols = feature_cols(y, core)
    own_loads = []
    for number, (first, last) in enumerate(((4 * TILE, 5 * TILE), (5 * TILE, 6 * TILE), (0, 4 * TILE))):
        own = pltpu.make_async_copy(tokens.at[first:last, :], whole.at[first:last, my_cols], load_sem.at[number])
        own.start()
        own_loads.append(own)
    with jax.named_scope("entry"):
        pl.semaphore_wait(barrier, len(peers))

    def rows_of(step):
        return pl.multiple_of(lax.rem(step + 4, CHUNKS) * TILE, TILE)

    def chunk_copy(rows, cols, target, send, recv):
        view = whole.at[rows, cols]
        return pltpu.make_async_remote_copy(
            src_ref=view, dst_ref=view, send_sem=send, recv_sem=recv, device_id=target, device_id_type=MESH
        )

    up, down = at_y(1), at_y(3)

    def gather_start(step):
        for half in range(2):
            for d in range(2):
                first = pl.multiple_of(rows_of(step) + (half ^ d) * SEGMENT, SEGMENT)
                sem = (pass_recv, gather_recv)[half].at[step]
                chunk_copy(pl.ds(first, SEGMENT), my_cols, (up, down)[d], sent.at[0], sem).start()

    def hop_copy(step, d):
        cols = feature_cols(at(y, (3, 1)[d]), core)
        rows = pl.ds(pl.multiple_of(rows_of(step) + d * SEGMENT, SEGMENT), SEGMENT)
        return chunk_copy(rows, cols, (up, down)[d], sent.at[1], hop_recv.at[step])

    def core_copy(step, which):
        cols = feature_cols(at(y, (0, 3, 1, 2)[which]), core)
        sem = (last_recv if which == 3 else core_recv).at[step]
        return chunk_copy(pl.ds(rows_of(step), TILE), cols, partner, sent.at[2], sem)

    def halo_copy(step):
        return pltpu.make_async_remote_copy(
            src_ref=kv.at[pl.ds(pl.multiple_of(LENGTH + step * TILE, TILE), TILE), :],
            dst_ref=kv.at[pl.ds(pl.multiple_of(step * TILE, TILE), TILE), :],
            send_sem=sent.at[3],
            recv_sem=halo_recv.at[0],
            device_id=at_sp(1),
            device_id_type=MESH,
        )

    def back_start(half):
        rows = slice(half * TILE, (half + 1) * TILE)
        back_send[rows] = dkv[rows, :].astype(BF16)
        pltpu.make_async_remote_copy(
            src_ref=back_send.at[rows],
            dst_ref=back_recv.at[rows],
            send_sem=sent.at[4],
            recv_sem=halo_recv.at[1],
            device_id=at_sp(15),
            device_id_type=MESH,
        ).start()

    edge = jnp.where(sp == 0, REACH, 0)
    row = lax.broadcasted_iota(jnp.int32, (SPAN, TILE), 0)

    def attend(tile):
        start = tile * TILE if isinstance(tile, int) else pl.multiple_of(tile * TILE, TILE)
        keys_at, here = pl.ds(start, SPAN), pl.ds(start, TILE)
        heads = []
        for h in range(HEADS):
            cols = slice(h * HEAD, (h + 1) * HEAD)
            value_cols = slice(COLS + h * HEAD, COLS + (h + 1) * HEAD)
            keys, values = kv[keys_at, cols], kv[keys_at, value_cols]
            asked, given = query[here, cols], upstream[here, cols]
            heads.append((cols, value_cols, keys, asked, given, dot(keys, asked, 1, 1), dot(values, given, 1, 1)))
        lows = []
        for h in range(HEADS):
            scores = heads[h][5] * FACTOR + bias[h]
            if not isinstance(tile, int):
                scores = jnp.where(row + start < edge, -jnp.inf, scores)
            top = jnp.max(scores, axis=0, keepdims=True)
            raised = jnp.exp(scores - top)
            weights = raised * (1.0 / jnp.sum(raised, axis=0, keepdims=True))
            prob_grad = heads[h][6]
            delta = jnp.sum(weights * prob_grad, axis=0, keepdims=True)
            score_grad = weights * (prob_grad - delta)
            dsum[h] = dsum[h] + score_grad
            lows.append((weights.astype(BF16), score_grad.astype(BF16)))
        for h in range(HEADS):
            cols, value_cols, keys, asked, given = heads[h][:5]
            weights_low, score_low = lows[h]
            grads_t[cols, here] = (dot(keys_t[cols, keys_at], score_low) * FACTOR).astype(BF16)
            dkv[keys_at, value_cols] = dkv[keys_at, value_cols] + dot(weights_low, given)
            dkv[keys_at, cols] = dkv[keys_at, cols] + dot(score_low, asked)

    for step in range(2):
        own_loads[step].wait()
        gather_start(step)
        core_copy(step, 0).start()
    own_loads[2].wait()

    table_load = pltpu.make_async_copy(position_bias, table, load_sem.at[7])
    table_load.start()
    loads = []
    for number, ref in enumerate((wq, wk, wv)):
        loads.append(pltpu.make_async_copy(ref, weight.at[:, number * COLS : (number + 1) * COLS], load_sem.at[3 + number]))
    loads.append(pltpu.make_async_copy(out_grad, upstream, load_sem.at[6]))
    for load in loads:
        load.start()

    lane = lax.broadcasted_iota(jnp.int32, (8, ROUND), 1)
    column = lax.broadcasted_iota(jnp.int32, (SPAN, TILE), 1)
    low = jnp.where(column >= SEGMENT, SEGMENT, 0)
    seen = (row >= low) & (row < low + REACH + SEGMENT)
    table_load.wait()
    for h in range(HEADS):
        entries = jnp.broadcast_to(table[h : h + 1, :], (8, TABLE))
        padded = jnp.concatenate([entries, jnp.zeros((8, ROUND - TABLE), F32)], axis=1)
        turned = pltpu.roll(padded, ROUND - TABLE + 1, 1)
        last = jnp.broadcast_to(table[h : h + 1, TABLE - 1 : TABLE], (8, ROUND))
        turned = jnp.where(lane < TILE, last, turned)
        skewed = pltpu.roll(jnp.broadcast_to(turned[0:1, :], (SPAN, ROUND)), 0, 1, stride=1, stride_axis=0)
        bias[h] = jnp.where(seen, skewed[:, :TILE], -jnp.inf)
        dsum[h] = jnp.zeros((SPAN, TILE), F32)
    dkv[...] = jnp.zeros(dkv.shape, F32)

    for load in loads:
        load.wait()

    def project_from(step, blocks):
        total = None
        for which in blocks:
            for on in (core, 1 - core):
                cols = feature_cols(at(y, (0, 3, 1, 2)[which]), on)
                part = dot(whole[pl.ds(rows_of(step), TILE), cols], weight[cols, :])
                total = part if total is None else total + part
        return total

    def hop_landed(step):
        with jax.named_scope("hop_wait"):
            await_bytes(whole.at[0:TILE, 0:FEATURES], hop_recv.at[step])
            core_copy(step, 3).start()

    def project_most(step):
        with jax.named_scope("core_wait"):
            await_bytes(whole.at[0:TILE, 0 : 3 * FEATURES], core_recv.at[step])
        with jax.named_scope("project"):
            projected[lax.rem(step, 2)] = project_from(step, (0, 1, 2))

    def gather_step(s, carry):
        @pl.when(s < CHUNKS)
        def _():
            with jax.named_scope("pass_wait"):
                await_bytes(whole.at[0:TILE, 0:FEATURES], pass_recv.at[s])
                for d in range(2):
                    hop_copy(s, d).start()

        @pl.when(s < CHUNKS - 2)
        def _():
            gather_start(s + 2)
            core_copy(s + 2, 0).start()

        @pl.when((s >= 1) & (s < CHUNKS))
        def _():
            project_most(s - 1)

        @pl.when(s < CHUNKS)
        def _():
            with jax.named_scope("gather_wait"):
                await_bytes(whole.at[0:TILE, 0:FEATURES], gather_recv.at[s])
                for d in range(2):
                    core_copy(s, 1 + d).start()

        @pl.when(s >= 1)
        def _():
            hop_landed(s - 1)

        @pl.when(s == CHUNKS - 1)
        def _():
            project_most(s)

        @pl.when(s == 4)
        def _():
            with jax.named_scope("halo_wait"):
                await_bytes(kv.at[0:REACH, :], halo_recv.at[0])
                keys_t[:, 0:REACH] = kv[0:REACH, :COLS].T

        @pl.when((s == 4) | (s == 6))
        def _():
            with jax.named_scope("attend"):
                attend(jnp.where(s == 4, 0, 2))

            @pl.when(s == 4)
            def _():
                back_start(0)

        @pl.when(s >= 1)
        def _():
            with jax.named_scope("last_wait"):
                await_bytes(whole.at[0:TILE, 0:FEATURES], last_recv.at[s - 1])
            with jax.named_scope("project_rest"):
                start = rows_of(s - 1)
                low = (projected[lax.rem(s - 1, 2)] + project_from(s - 1, (3,))).astype(BF16)
                query[pl.ds(start, TILE), :] = low[:, :COLS]
                kv[pl.ds(pl.multiple_of(start + REACH, TILE), TILE), :] = low[:, COLS:]
                keys_t[:, pl.ds(pl.multiple_of(start + REACH, TILE), TILE)] = low[:, COLS : 2 * COLS].T

        @pl.when((s >= 1) & (s <= 2))
        def _():
            halo_copy(s - 1).start()

        @pl.when(s == 4)
        def _():
            with jax.named_scope("attend"):
                attend(s - 3)
            back_start(1)

        return carry

    lax.fori_loop(0, CHUNKS + 1, gather_step, 0)
    with jax.named_scope("attend_last"):
        for tile in range(3, CHUNKS):
            attend(tile)

    def first_ring(p, side):
        me = (x, z)[side]
        part = (part_a, part_b)[side]
        at_side = (at_x, at_z)[side]
        return Ring(
            me, at_side(1), at_side(3),
            lambda k, half: part.at[p, k, pl.ds(2 * half, 2)],
            lambda d: far_ab.at[p, side, d],
            lambda d: near_join.at[p, 0, side, d],
            lambda d: near_join.at[p, 1, side, d],
            sent.at[5], ring_rs.at[p, 0], ring_rs.at[p, 1],
        )

    def second_ring(p, side):
        me = (z, x)[side]
        at_side = (at_z, at_x)[side]
        return Ring(
            me, at_side(1), at_side(3),
            lambda k, half: second_ab.at[p, side, k, half * SEGMENT : (half + 1) * SEGMENT],
            lambda d: far2_ab.at[p, side, d],
            lambda d: near_join2.at[p, 0, side, d],
            lambda d: near_join2.at[p, 1, side, d],
            sent.at[6], second_rs.at[p, 0], second_rs.at[p, 1],
        )

    y_ring = Ring(
        y, up, down,
        lambda k, half: term_own.at[k, half * (LENGTH // 2) : (half + 1) * (LENGTH // 2)],
        lambda d: far_y.at[d],
        lambda d: near_join_y.at[0, d],
        lambda d: near_join_y.at[1, d],
        sent.at[7], y_rs.at[0], y_rs.at[1],
    )

    halves = (slice(0, LENGTH // 2), slice(LENGTH // 2, LENGTH))

    def term(y_index, core_index, rows):
        start = pl.multiple_of((y_index * 2 + core_index) * FEATURES, FEATURES)
        return dot(grads[rows, :], weight[pl.ds(start, FEATURES), :], 1, 1)

    def send_term(k, rows, sem):
        with jax.named_scope("term_send"):
            term_send[k, rows] = term(at(y, AHEAD[k]), 1 - core, rows).astype(BF16)
        pltpu.make_async_remote_copy(
            src_ref=term_send.at[k, rows],
            dst_ref=term_recv.at[k, rows],
            send_sem=sent.at[8],
            recv_sem=term_rs.at[sem],
            device_id=partner,
            device_id_type=MESH,
        ).start()

    def own_term(k, rows, sem):
        with jax.named_scope("term_own"):
            y_index = at(y, AHEAD[k])
            made = term(y_index, core, rows)
            await_bytes(term_recv.at[k, rows], term_rs.at[sem])
            term_own[y_index, rows] = (made + term_recv[k, rows].astype(F32)).astype(BF16)

    def bias_send(buffer, me, targets, which):
        view = buffer.at[me]
        for target in targets:
            pltpu.make_async_remote_copy(
                src_ref=view, dst_ref=view, send_sem=sent.at[9], recv_sem=bias_rs.at[which], device_id=target, device_id_type=MESH
            ).start()

    def bias_sums():
        bias_x[x] = jnp.zeros((8, TILE), F32)
        for h in range(HEADS):
            wide = jnp.concatenate([dsum[h], jnp.zeros((SPAN, ROUND - TILE), F32)], axis=1)
            rows = SPAN
            while rows > 24:
                rows //= 2
                wide = wide[:rows] + pltpu.roll(wide[rows:], ROUND - rows, 1)
            wide = wide[0:8] + pltpu.roll(wide[8:16], ROUND - 8, 1) + pltpu.roll(wide[16:24], ROUND - 16, 1)
            sums = wide[0:1]
            for r in range(1, 8):
                sums = sums + pltpu.roll(wide[r : r + 1], ROUND - r, 1)
            first = lax.broadcasted_iota(jnp.int32, (1, ROUND), 1)
            clipped = jnp.sum(jnp.where(first < TILE, sums, 0.0), axis=1, keepdims=True)
            placed = pltpu.roll(sums, TABLE - 1, 1)
            sums = jnp.where(first == TABLE - 1, clipped, placed)
            for piece in range(3):
                bias_x[x, 3 * h + piece : 3 * h + piece + 1, :] = sums[:, piece * TILE : (piece + 1) * TILE]

    def finish():
        with jax.named_scope("back_wait"):
            await_bytes(back_recv, halo_recv.at[1])
            dkv[LENGTH:, :] = dkv[LENGTH:, :] + back_recv[...].astype(F32)

        def finish_chunk(chunk, carry):
            start = pl.multiple_of(chunk * TILE, TILE)
            grads[pl.ds(start, TILE), :COLS] = grads_t[:COLS, pl.ds(start, TILE)].T
            total = dkv[pl.ds(pl.multiple_of(start + REACH, TILE), TILE), :]
            total = jnp.concatenate([total[:, :COLS] * FACTOR, total[:, COLS:]], axis=1)
            grads[pl.ds(start, TILE), COLS:] = total.astype(BF16)
            grads_t[COLS:, pl.ds(start, TILE)] = total.T.astype(BF16)
            return carry

        with jax.named_scope("finish"):
            lax.fori_loop(0, CHUNKS, finish_chunk, 0)

    def weight_row(k, z_index):
        features = pl.ds(pl.multiple_of(z_index * RING * COLS, RING * COLS), RING * COLS)
        made = dot(grads_t[k * COLS : (k + 1) * COLS, :], whole[:, features]).astype(BF16)
        for x_index in range(RING):
            cut = slice(x_index * COLS, (x_index + 1) * COLS)
            part_b[k, z_index, x_index] = made[HEAD:, cut]

            @pl.when(x_index != at(x, 2))
            def _():
                part_a[k, x_index, z_index] = made[:HEAD, cut]

    def weight_far(k):
        far_x = at(x, 2)
        with jax.named_scope("weight_far"):
            for z_index in range(RING):
                features = pl.ds(pl.multiple_of(z_index * RING * COLS + far_x * COLS, COLS), COLS)
                left = grads_t[k * COLS : k * COLS + HEAD, :]
                part_a[k, far_x, z_index] = dot(left, whole[:, features]).astype(BF16)
            first_ring(k, 0).start_far()
            weight_row(k, at(z, 2))
            first_ring(k, 1).start_far()

    def weight_rest(k):
        def rows(i, inner):
            weight_row(k, at(z, i))
            return inner

        with jax.named_scope("weight_rest"):
            lax.fori_loop(3, RING + 2, rows, 0)
        for side in range(2):
            for d in range(2):
                first_ring(k, side).start_near(d)

    def first_join(p):
        with jax.named_scope("join_first"):
            await_bytes(far_ab.at[p], ring_rs.at[p, 0])
            for side in range(2):
                first_ring(p, side).join()

    whole_rows = slice(0, LENGTH)
    weight_far(0)
    weight_rest(0)
    finish()
    for half in range(2):
        send_term(0, halves[half], half)
    weight_far(1)
    for half in range(2):
        own_term(0, halves[half], half)
        y_ring.start(0, half)
    weight_rest(1)
    first_join(0)
    send_term(1, whole_rows, 2)
    with jax.named_scope("bias_sums"):
        bias_sums()
    bias_send(bias_x, x, [at_x(by) for by in (1, 2, 3)], 0)
    weight_far(2)
    send_term(2, whole_rows, 3)
    send_term(3, whole_rows, 4)
    own_term(1, whole_rows, 2)
    y_ring.start_near(0)
    own_term(2, whole_rows, 3)
    y_ring.start_near(1)
    weight_rest(2)
    first_join(1)
    with jax.named_scope("join_y"):
        await_bytes(far_y, y_rs.at[0])
        y_ring.join()
    with jax.named_scope("bias_x"):
        await_bytes(bias_x.at[0:3], bias_rs.at[0])
        bias_z[z] = (bias_x[0] + bias_x[1]) + (bias_x[2] + bias_x[3])
    bias_send(bias_z, z, [at_z(by) for by in (1, 2, 3)], 1)
    own_term(3, whole_rows, 4)

    def second_start(p):
        with jax.named_scope(f"second_start_{p}"):
            await_bytes(near_join.at[p], ring_rs.at[p, 1])
            for side in range(2):
                ring = first_ring(p, side)
                for half in range(2):
                    second_ab[p, side, 2 * half : 2 * half + 2] = ring.half(half).astype(BF16)
            rings = [second_ring(p, side) for side in range(2)]
            if p in STRAIGHT:
                rings[0].start_straight(at_z(2))
                rings[1].start_straight(at_x(2))
                return
            for ring in rings:
                ring.start_far()
            for ring in rings:
                for d in range(2):
                    ring.start_near(d)

    def second_join(p):
        with jax.named_scope(f"second_join_{p}"):
            await_bytes(far2_ab.at[p], second_rs.at[p, 0])
            for side in range(2):
                second_ring(p, side).join()

    def second_finish(p):
        with jax.named_scope(f"second_finish_{p}"):
            await_bytes(near_join2.at[p], second_rs.at[p, 1])
            if p in STRAIGHT:
                await_bytes(far2_ab.at[p], second_rs.at[p, 0])
            for side in range(2):
                ring = second_ring(p, side)
                sums = [ring.half(half) for half in range(2)]
                if p in STRAIGHT:
                    sums = [sums[half] + far2_ab[p, side, half].astype(F32) for half in range(2)]
                total = jnp.concatenate(sums, axis=0)
                (wq_out, wk_out, wv_out)[p][:, side * HEAD : (side + 1) * HEAD] = total.T

    first_join(2)
    second_start(0)
    second_start(1)
    second_join(0)
    second_start(2)
    second_join(1)
    second_finish(0)
    with jax.named_scope("bias_z"):
        await_bytes(bias_z.at[0:3], bias_rs.at[1])
        sums = (bias_z[0] + bias_z[1]) + (bias_z[2] + bias_z[3])
        for h in range(HEADS):
            for piece in range(3):
                cut = slice(piece * TILE, min((piece + 1) * TILE, TABLE))
                bias_out[h : h + 1, cut] = sums[3 * h + piece : 3 * h + piece + 1, : cut.stop - cut.start]
    with jax.named_scope("input_sum"):
        await_bytes(near_join_y, y_rs.at[1])
        for d in range(2):
            input_out[d * (LENGTH // 2) : (d + 1) * (LENGTH // 2), :] = y_ring.half(d).astype(BF16)
    second_finish(1)
    second_finish(2)

    with jax.named_scope("drain"):
        await_bytes(whole.at[:, 0 : 2 * FEATURES], sent.at[0])
        await_bytes(whole.at[:, 0:FEATURES], sent.at[1])
        await_bytes(whole.at[:, 0 : 4 * FEATURES], sent.at[2])
        await_bytes(kv.at[0:REACH, :], sent.at[3])
        await_bytes(back_send, sent.at[4])
        await_bytes(far_ab, sent.at[5])
        await_bytes(near_join, sent.at[5])
        await_bytes(far2_ab, sent.at[6])
        await_bytes(near_join2, sent.at[6])
        await_bytes(far_y, sent.at[7])
        await_bytes(near_join_y, sent.at[7])
        await_bytes(term_recv, sent.at[8])
        await_bytes(bias_x.at[0:3], sent.at[9])
        await_bytes(bias_z.at[0:3], sent.at[9])


def store_results(*refs):
    sources, targets, sems = refs[:5], refs[5:10], refs[10]
    copies = [pltpu.make_async_copy(source, target, sems.at[n]) for n, (source, target) in enumerate(zip(sources, targets))]
    for copy in copies:
        copy.start()
    for copy in copies:
        copy.wait()


def shards(tokens, query_weight, key_weight, value_weight, position_bias, out_grad):
    anywhere = pl.BlockSpec(memory_space=pl.ANY)
    near = pl.BlockSpec(memory_space=pltpu.VMEM)
    dma = pltpu.SemaphoreType.DMA
    vmem = pltpu.VMEM
    grad = vmem((COLS, COLS), F32)
    results = pl.pallas_call(
        kernel,
        name="segment_attention_grads",
        out_shape=(
            vmem((LENGTH, FEATURES), BF16), grad, grad, grad,
            vmem((HEADS, TABLE), F32),
        ),
        in_specs=[anywhere] * 6,
        out_specs=(near,) * 5,
        scratch_shapes=[
            vmem((HEADS, TABLE), F32),
            vmem((LENGTH, WIDTH), BF16),
            vmem((WIDTH, 3 * COLS), BF16),
            vmem((2, TILE, 3 * COLS), F32),
            vmem((LENGTH, COLS), BF16),
            vmem((REACH + LENGTH, 2 * COLS), BF16),
            vmem((LENGTH, COLS), BF16),
            vmem((COLS, REACH + LENGTH), BF16),
            vmem((REACH + LENGTH, 2 * COLS), F32),
            vmem((LENGTH, 3 * COLS), BF16),
            vmem((3 * COLS, LENGTH), BF16),
            vmem((REACH, 2 * COLS), BF16),
            vmem((REACH, 2 * COLS), BF16),
            vmem((3, RING, RING, HEAD, COLS), BF16),
            vmem((3, RING, RING, HEAD, COLS), BF16),
            vmem((3, 2, 2, 2, HEAD, COLS), BF16),
            vmem((3, 2, 2, 2, 2, HEAD, COLS), BF16),
            vmem((3, 2, RING, HEAD, COLS), BF16),
            vmem((3, 2, 2, SEGMENT, COLS), BF16),
            vmem((3, 2, 2, 2, SEGMENT, COLS), BF16),
            vmem((RING, LENGTH, FEATURES), BF16),
            vmem((RING, LENGTH, FEATURES), BF16),
            vmem((RING, LENGTH, FEATURES), BF16),
            vmem((2, LENGTH // 2, FEATURES), BF16),
            vmem((2, 2, LENGTH // 2, FEATURES), BF16),
            vmem((HEADS, SPAN, TILE), F32),
            vmem((HEADS, SPAN, TILE), F32),
            vmem((RING, 8, TILE), F32),
            vmem((RING, 8, TILE), F32),
            dma((8,)),
            dma((CHUNKS,)), dma((CHUNKS,)), dma((CHUNKS,)), dma((CHUNKS,)), dma((CHUNKS,)),
            dma((3,)),
            dma((RING + 1,)),
            dma((3, 2)), dma((3, 2)), dma((2,)),
            dma((2,)),
            dma((10,)),
        ],
        compiler_params=pltpu.CompilerParams(
            collective_id=0, has_side_effects=True, vmem_limit_bytes=62_000_000
        ),
    )(tokens, query_weight, key_weight, value_weight, position_bias, out_grad)
    return pl.pallas_call(
        store_results,
        name="store_results",
        out_shape=tuple(jax.ShapeDtypeStruct(result.shape, result.dtype) for result in results),
        in_specs=[near] * 5,
        out_specs=(anywhere,) * 5,
        scratch_shapes=[dma((5,))],
        compiler_params=pltpu.CompilerParams(vmem_limit_bytes=1_000_000),
    )(*results)


def solution(mesh):
    return jax.shard_map(
        shards,
        mesh=mesh,
        in_specs=(P("sp", "tp"), P(None, "tp"), P(None, "tp"), P(None, "tp"), P("tp", None), P("sp", "tp")),
        out_specs=(P("sp", "tp"), P("sp", "tp"), P("sp", "tp"), P("sp", "tp"), P("tp", None)),
        check_vma=False,
    )
```

```python
import functools

import jax
import jax.numpy as jnp
from jax import lax
from jax.experimental import pallas as pl
from jax.experimental.pallas import tpu as pltpu
from jax.sharding import PartitionSpec as P

MESH = pl.DeviceIdType.MESH
BF16, F32 = jnp.bfloat16, jnp.float32
SEGMENT, REACH, CLIP, HEAD = 64, 256, 256, 128
TILE = 128
SPAN = REACH + TILE
LENGTH, WIDTH, FEATURES = 768, 4096, 512
CHUNKS = LENGTH // TILE
HEADS = 2
COLS = HEADS * HEAD
FACTOR = HEAD ** (-0.5)
RING = 4
LOG2_E = 1.4426950408889634
TABLE = 320
ROUND = 512
AHEAD = (2, 1, 3, 0)
STRAIGHT = (2,)


def dot(left, right, left_dim=1, right_dim=0):
    return lax.dot_general(left, right, (((left_dim,), (right_dim,)), ((), ())), preferred_element_type=F32)


class Ring:
    def __init__(self, me, up, down, block, via, direct, joined, sent, far_sem, rest_sem):
        self.near = (lax.rem(me + 1, RING), lax.rem(me + RING - 1, RING))
        self.far = lax.rem(me + 2, RING)
        self.me, self.devices, self.block = me, (up, down), block
        self.landing = (via, direct, joined)
        self.sent, self.arrived = sent, (far_sem, rest_sem, rest_sem)

    def start(self, kind, d):
        source = (self.block(self.far, d), self.block(self.near[d], 1 - d), self.block(self.near[d], d))[kind]
        pltpu.make_async_remote_copy(
            src_ref=source,
            dst_ref=self.landing[kind](d),
            send_sem=self.sent,
            recv_sem=self.arrived[kind],
            device_id=self.devices[d],
            device_id_type=MESH,
        ).start()

    def start_straight(self, opposite):
        for d in range(2):
            pltpu.make_async_remote_copy(
                src_ref=self.block(self.far, d),
                dst_ref=self.landing[0](d),
                send_sem=self.sent,
                recv_sem=self.arrived[0],
                device_id=opposite,
                device_id_type=MESH,
            ).start()
        for kind in (1, 2):
            for d in range(2):
                self.start(kind, d)

    def start_far(self):
        for d in range(2):
            self.start(0, d)

    def start_near(self, d):
        self.start(1, d)

    def join(self):
        for d in range(2):
            ref = self.block(self.near[d], d)
            ref[...] = (ref[...].astype(F32) + self.landing[0](d)[...].astype(F32)).astype(BF16)
            self.start(2, d)

    def half(self, d):
        total = self.block(self.me, d)[...].astype(F32) + self.landing[2](d)[...].astype(F32)
        return total + self.landing[1](1 - d)[...].astype(F32)


def await_bytes(view, sem):
    pltpu.make_async_copy(view, view, sem).wait()


def kernel(
    tokens, wq, wk, wv, position_bias, out_grad,
    input_out, wq_out, wk_out, wv_out, bias_out,
    table, whole, weight, projected, query, kv, upstream, keys_t, dkv, grads, grads_t, back_send, back_recv,
    part_a, part_b, far_ab, near_join, second_ab, far2_ab, near_join2,
    term_own, term_send, term_recv, far_y, near_join_y,
    bias, dsum, bias_x, bias_z,
    load_sem, pass_recv, gather_recv, hop_recv, core_recv, last_recv, halo_recv, term_rs, ring_rs, second_rs, y_rs, bias_rs, sent,
):
    sp, tp = lax.axis_index("sp"), lax.axis_index("tp")
    z, x = sp // RING, lax.rem(sp, RING)
    y, core = tp // 2, lax.rem(tp, 2)

    def at(value, by):
        return lax.rem(value + by, RING)

    def at_x(by):
        return (z * RING + at(x, by), tp)

    def at_z(by):
        return (at(z, by) * RING + x, tp)

    def at_y(by):
        return (sp, at(y, by) * 2 + core)

    def at_sp(by):
        return (lax.rem(sp + by, 16), tp)

    partner = (sp, y * 2 + 1 - core)

    barrier = pltpu.get_barrier_semaphore()
    peers = [partner, at_sp(1), at_sp(15)]
    for by in (1, 3):
        peers.append(at_y(by))
    for by in (1, 2, 3):
        peers += [at_x(by), at_z(by)]
    for peer in peers:
        pl.semaphore_signal(barrier, inc=1, device_id=peer, device_id_type=MESH)

    def feature_cols(y_index, core_index):
        return pl.ds(pl.multiple_of((y_index * 2 + core_index) * FEATURES, FEATURES), FEATURES)

    my_cols = feature_cols(y, core)
    own_loads = []
    for number, (first, last) in enumerate(((4 * TILE, 5 * TILE), (5 * TILE, 6 * TILE), (0, 4 * TILE))):
        own = pltpu.make_async_copy(tokens.at[first:last, :], whole.at[first:last, my_cols], load_sem.at[number])
        own.start()
        own_loads.append(own)
    with jax.named_scope("entry"):
        pl.semaphore_wait(barrier, len(peers))

    def rows_of(step):
        return pl.multiple_of(lax.rem(step + 4, CHUNKS) * TILE, TILE)

    def chunk_copy(rows, cols, target, send, recv):
        view = whole.at[rows, cols]
        return pltpu.make_async_remote_copy(
            src_ref=view, dst_ref=view, send_sem=send, recv_sem=recv, device_id=target, device_id_type=MESH
        )

    up, down = at_y(1), at_y(3)

    def gather_start(step):
        for half in range(2):
            for d in range(2):
                first = pl.multiple_of(rows_of(step) + (half ^ d) * SEGMENT, SEGMENT)
                sem = (pass_recv, gather_recv)[half].at[step]
                chunk_copy(pl.ds(first, SEGMENT), my_cols, (up, down)[d], sent.at[0], sem).start()

    def hop_copy(step, d):
        cols = feature_cols(at(y, (3, 1)[d]), core)
        rows = pl.ds(pl.multiple_of(rows_of(step) + d * SEGMENT, SEGMENT), SEGMENT)
        return chunk_copy(rows, cols, (up, down)[d], sent.at[1], hop_recv.at[step])

    def core_copy(step, which):
        cols = feature_cols(at(y, (0, 3, 1, 2)[which]), core)
        sem = (last_recv if which == 3 else core_recv).at[step]
        return chunk_copy(pl.ds(rows_of(step), TILE), cols, partner, sent.at[2], sem)

    def halo_copy(step):
        return pltpu.make_async_remote_copy(
            src_ref=kv.at[pl.ds(pl.multiple_of(LENGTH + step * TILE, TILE), TILE), :],
            dst_ref=kv.at[pl.ds(pl.multiple_of(step * TILE, TILE), TILE), :],
            send_sem=sent.at[3],
            recv_sem=halo_recv.at[0],
            device_id=at_sp(1),
            device_id_type=MESH,
        )

    def back_start(half):
        rows = slice(half * TILE, (half + 1) * TILE)
        back_send[rows] = dkv[rows, :].astype(BF16)
        pltpu.make_async_remote_copy(
            src_ref=back_send.at[rows],
            dst_ref=back_recv.at[rows],
            send_sem=sent.at[4],
            recv_sem=halo_recv.at[1],
            device_id=at_sp(15),
            device_id_type=MESH,
        ).start()

    edge = jnp.where(sp == 0, REACH, 0)
    row = lax.broadcasted_iota(jnp.int32, (SPAN, TILE), 0)

    def ranges(tile):
        start = tile * TILE if isinstance(tile, int) else pl.multiple_of(tile * TILE, TILE)
        return start, pl.ds(start, SPAN), pl.ds(start, TILE)

    head_cols = [slice(h * HEAD, (h + 1) * HEAD) for h in range(HEADS)]
    value_cols = [slice(COLS + h * HEAD, COLS + (h + 1) * HEAD) for h in range(HEADS)]

    def attend_products(tile):
        _, keys_at, here = ranges(tile)
        return [
            (dot(kv[keys_at, head_cols[h]], query[here, head_cols[h]], 1, 1), dot(kv[keys_at, value_cols[h]], upstream[here, head_cols[h]], 1, 1))
            for h in range(HEADS)
        ]

    def attend_weights(tile, products):
        start, _, _ = ranges(tile)
        lows = []
        for h in range(HEADS):
            raw, prob_grad = products[h]
            scores = raw * (FACTOR * LOG2_E) + bias[h]
            if not isinstance(tile, int):
                scores = jnp.where(row + start < edge, -jnp.inf, scores)
            raised = jnp.exp2(scores - jnp.max(scores, axis=0, keepdims=True))
            weights = raised * (1.0 / jnp.sum(raised, axis=0, keepdims=True))
            delta = jnp.sum(weights * prob_grad, axis=0, keepdims=True)
            score_grad = weights * (prob_grad - delta)
            dsum[h] = dsum[h] + score_grad
            lows.append((weights.astype(BF16), score_grad.astype(BF16)))
        return lows

    def attend_queries(tile, lows):
        _, keys_at, here = ranges(tile)
        for h in range(HEADS):
            grads_t[head_cols[h], here] = (dot(keys_t[head_cols[h], keys_at], lows[h][1]) * FACTOR).astype(BF16)

    def attend_keys(tile, lows):
        _, keys_at, here = ranges(tile)
        for h in range(HEADS):
            weights_low, score_low = lows[h]
            dkv[keys_at, value_cols[h]] = dkv[keys_at, value_cols[h]] + dot(weights_low, upstream[here, head_cols[h]])
            dkv[keys_at, head_cols[h]] = dkv[keys_at, head_cols[h]] + dot(score_low, query[here, head_cols[h]])

    def attend(tile):
        lows = attend_weights(tile, attend_products(tile))
        attend_queries(tile, lows)
        attend_keys(tile, lows)

    for step in range(2):
        own_loads[step].wait()
        gather_start(step)
        core_copy(step, 0).start()
    own_loads[2].wait()

    table_load = pltpu.make_async_copy(position_bias, table, load_sem.at[7])
    table_load.start()
    loads = []
    for number, ref in enumerate((wq, wk, wv)):
        loads.append(pltpu.make_async_copy(ref, weight.at[:, number * COLS : (number + 1) * COLS], load_sem.at[3 + number]))
    loads.append(pltpu.make_async_copy(out_grad, upstream, load_sem.at[6]))
    for load in loads:
        load.start()

    lane = lax.broadcasted_iota(jnp.int32, (8, ROUND), 1)
    column = lax.broadcasted_iota(jnp.int32, (SPAN, TILE), 1)
    low = jnp.where(column >= SEGMENT, SEGMENT, 0)
    seen = (row >= low) & (row < low + REACH + SEGMENT)
    table_load.wait()
    for h in range(HEADS):
        entries = jnp.broadcast_to(table[h : h + 1, :], (8, TABLE))
        padded = jnp.concatenate([entries, jnp.zeros((8, ROUND - TABLE), F32)], axis=1)
        turned = pltpu.roll(padded, ROUND - TABLE + 1, 1)
        last = jnp.broadcast_to(table[h : h + 1, TABLE - 1 : TABLE], (8, ROUND))
        turned = jnp.where(lane < TILE, last, turned)
        skewed = pltpu.roll(jnp.broadcast_to(turned[0:1, :], (SPAN, ROUND)), 0, 1, stride=1, stride_axis=0)
        bias[h] = jnp.where(seen, skewed[:, :TILE] * LOG2_E, -jnp.inf)
        dsum[h] = jnp.zeros((SPAN, TILE), F32)
    dkv[...] = jnp.zeros(dkv.shape, F32)

    for load in loads:
        load.wait()

    def project_from(step, blocks):
        total = None
        for which in blocks:
            for on in (core, 1 - core):
                cols = feature_cols(at(y, (0, 3, 1, 2)[which]), on)
                part = dot(whole[pl.ds(rows_of(step), TILE), cols], weight[cols, :])
                total = part if total is None else total + part
        return total

    def hop_landed(step):
        with jax.named_scope("hop_wait"):
            await_bytes(whole.at[0:TILE, 0:FEATURES], hop_recv.at[step])
            core_copy(step, 3).start()

    def project_most(step):
        with jax.named_scope("core_wait"):
            await_bytes(whole.at[0:TILE, 0 : 3 * FEATURES], core_recv.at[step])
        with jax.named_scope("project"):
            projected[lax.rem(step, 2)] = project_from(step, (0, 1, 2))

    def gather_step(s, carry):
        @pl.when(s < CHUNKS)
        def _():
            with jax.named_scope("pass_wait"):
                await_bytes(whole.at[0:TILE, 0:FEATURES], pass_recv.at[s])
                for d in range(2):
                    hop_copy(s, d).start()

        @pl.when(s < CHUNKS - 2)
        def _():
            gather_start(s + 2)
            core_copy(s + 2, 0).start()

        @pl.when((s >= 1) & (s < CHUNKS))
        def _():
            project_most(s - 1)

        @pl.when(s < CHUNKS)
        def _():
            with jax.named_scope("gather_wait"):
                await_bytes(whole.at[0:TILE, 0:FEATURES], gather_recv.at[s])
                for d in range(2):
                    core_copy(s, 1 + d).start()

        @pl.when(s >= 1)
        def _():
            hop_landed(s - 1)

        @pl.when(s == CHUNKS - 1)
        def _():
            project_most(s)

        @pl.when(s == 4)
        def _():
            with jax.named_scope("halo_wait"):
                await_bytes(kv.at[0:REACH, :], halo_recv.at[0])
                keys_t[:, 0:REACH] = kv[0:REACH, :COLS].T

        @pl.when((s == 4) | (s == 6))
        def _():
            with jax.named_scope("attend"):
                attend(jnp.where(s == 4, 0, 2))

            @pl.when(s == 4)
            def _():
                back_start(0)

        @pl.when(s >= 1)
        def _():
            with jax.named_scope("last_wait"):
                await_bytes(whole.at[0:TILE, 0:FEATURES], last_recv.at[s - 1])
            with jax.named_scope("project_rest"):
                start = rows_of(s - 1)
                low = (projected[lax.rem(s - 1, 2)] + project_from(s - 1, (3,))).astype(BF16)
                query[pl.ds(start, TILE), :] = low[:, :COLS]
                kv[pl.ds(pl.multiple_of(start + REACH, TILE), TILE), :] = low[:, COLS:]
                keys_t[:, pl.ds(pl.multiple_of(start + REACH, TILE), TILE)] = low[:, COLS : 2 * COLS].T

        @pl.when((s >= 1) & (s <= 2))
        def _():
            halo_copy(s - 1).start()

        @pl.when(s == 4)
        def _():
            with jax.named_scope("attend"):
                attend(s - 3)
            back_start(1)

        return carry

    lax.fori_loop(0, CHUNKS + 1, gather_step, 0)
    with jax.named_scope("attend_last"):
        products = {tile: attend_products(tile) for tile in (3, 4)}
        lows = {3: attend_weights(3, products[3])}
        products[5] = attend_products(5)
        attend_queries(3, lows[3])
        for tile in (4, 5):
            lows[tile] = attend_weights(tile, products[tile])
            attend_queries(tile, lows[tile])
            attend_keys(tile - 1, lows[tile - 1])
        attend_keys(5, lows[5])

    def first_ring(p, side):
        me = (x, z)[side]
        part = (part_a, part_b)[side]
        at_side = (at_x, at_z)[side]
        return Ring(
            me, at_side(1), at_side(3),
            lambda k, half: part.at[p, k, pl.ds(2 * half, 2)],
            lambda d: far_ab.at[p, side, d],
            lambda d: near_join.at[p, 0, side, d],
            lambda d: near_join.at[p, 1, side, d],
            sent.at[5], ring_rs.at[p, 0], ring_rs.at[p, 1],
        )

    def second_ring(p, side):
        me = (z, x)[side]
        at_side = (at_z, at_x)[side]
        return Ring(
            me, at_side(1), at_side(3),
            lambda k, half: second_ab.at[p, side, k, half * SEGMENT : (half + 1) * SEGMENT],
            lambda d: far2_ab.at[p, side, d],
            lambda d: near_join2.at[p, 0, side, d],
            lambda d: near_join2.at[p, 1, side, d],
            sent.at[6], second_rs.at[p, 0], second_rs.at[p, 1],
        )

    y_ring = Ring(
        y, up, down,
        lambda k, half: term_own.at[k, half * (LENGTH // 2) : (half + 1) * (LENGTH // 2)],
        lambda d: far_y.at[d],
        lambda d: near_join_y.at[0, d],
        lambda d: near_join_y.at[1, d],
        sent.at[7], y_rs.at[0], y_rs.at[1],
    )

    halves = (slice(0, LENGTH // 2), slice(LENGTH // 2, LENGTH))

    def term(y_index, core_index, rows):
        start = pl.multiple_of((y_index * 2 + core_index) * FEATURES, FEATURES)
        return dot(grads[rows, :], weight[pl.ds(start, FEATURES), :], 1, 1)

    def send_term(k, rows, sem):
        with jax.named_scope("term_send"):
            term_send[k, rows] = term(at(y, AHEAD[k]), 1 - core, rows).astype(BF16)
        pltpu.make_async_remote_copy(
            src_ref=term_send.at[k, rows],
            dst_ref=term_recv.at[k, rows],
            send_sem=sent.at[8],
            recv_sem=term_rs.at[sem],
            device_id=partner,
            device_id_type=MESH,
        ).start()

    def own_term(k, rows, sem):
        with jax.named_scope("term_own"):
            y_index = at(y, AHEAD[k])
            made = term(y_index, core, rows)
            await_bytes(term_recv.at[k, rows], term_rs.at[sem])
            term_own[y_index, rows] = (made + term_recv[k, rows].astype(F32)).astype(BF16)

    def bias_send(buffer, me, targets, which):
        view = buffer.at[me]
        for target in targets:
            pltpu.make_async_remote_copy(
                src_ref=view, dst_ref=view, send_sem=sent.at[9], recv_sem=bias_rs.at[which], device_id=target, device_id_type=MESH
            ).start()

    def bias_sums():
        bias_x[x] = jnp.zeros((8, TILE), F32)
        for h in range(HEADS):
            wide = jnp.concatenate([dsum[h], jnp.zeros((SPAN, ROUND - TILE), F32)], axis=1)
            rows = SPAN
            while rows > 24:
                rows //= 2
                wide = wide[:rows] + pltpu.roll(wide[rows:], ROUND - rows, 1)
            wide = wide[0:8] + pltpu.roll(wide[8:16], ROUND - 8, 1) + pltpu.roll(wide[16:24], ROUND - 16, 1)
            sums = wide[0:1]
            for r in range(1, 8):
                sums = sums + pltpu.roll(wide[r : r + 1], ROUND - r, 1)
            first = lax.broadcasted_iota(jnp.int32, (1, ROUND), 1)
            clipped = jnp.sum(jnp.where(first < TILE, sums, 0.0), axis=1, keepdims=True)
            placed = pltpu.roll(sums, TABLE - 1, 1)
            sums = jnp.where(first == TABLE - 1, clipped, placed)
            for piece in range(3):
                bias_x[x, 3 * h + piece : 3 * h + piece + 1, :] = sums[:, piece * TILE : (piece + 1) * TILE]

    def finish():
        with jax.named_scope("back_wait"):
            await_bytes(back_recv, halo_recv.at[1])
            dkv[LENGTH:, :] = dkv[LENGTH:, :] + back_recv[...].astype(F32)

        def finish_chunk(chunk, carry):
            start = pl.multiple_of(chunk * TILE, TILE)
            grads[pl.ds(start, TILE), :COLS] = grads_t[:COLS, pl.ds(start, TILE)].T
            total = dkv[pl.ds(pl.multiple_of(start + REACH, TILE), TILE), :]
            total = jnp.concatenate([total[:, :COLS] * FACTOR, total[:, COLS:]], axis=1)
            grads[pl.ds(start, TILE), COLS:] = total.astype(BF16)
            grads_t[COLS:, pl.ds(start, TILE)] = total.T.astype(BF16)
            return carry

        with jax.named_scope("finish"):
            lax.fori_loop(0, CHUNKS, finish_chunk, 0)

    def weight_row(k, z_index):
        features = pl.ds(pl.multiple_of(z_index * RING * COLS, RING * COLS), RING * COLS)
        made = dot(grads_t[k * COLS : (k + 1) * COLS, :], whole[:, features]).astype(BF16)
        for x_index in range(RING):
            cut = slice(x_index * COLS, (x_index + 1) * COLS)
            part_b[k, z_index, x_index] = made[HEAD:, cut]

            @pl.when(x_index != at(x, 2))
            def _():
                part_a[k, x_index, z_index] = made[:HEAD, cut]

    def weight_far(k):
        far_x = at(x, 2)
        with jax.named_scope("weight_far"):
            for z_index in range(RING):
                features = pl.ds(pl.multiple_of(z_index * RING * COLS + far_x * COLS, COLS), COLS)
                left = grads_t[k * COLS : k * COLS + HEAD, :]
                part_a[k, far_x, z_index] = dot(left, whole[:, features]).astype(BF16)
            first_ring(k, 0).start_far()
            weight_row(k, at(z, 2))
            first_ring(k, 1).start_far()

    def weight_rest(k):
        def rows(i, inner):
            weight_row(k, at(z, i))
            return inner

        with jax.named_scope("weight_rest"):
            lax.fori_loop(3, RING + 2, rows, 0)
        for side in range(2):
            for d in range(2):
                first_ring(k, side).start_near(d)

    def first_join(p):
        with jax.named_scope("join_first"):
            await_bytes(far_ab.at[p], ring_rs.at[p, 0])
            for side in range(2):
                first_ring(p, side).join()

    whole_rows = slice(0, LENGTH)
    weight_far(0)
    weight_rest(0)
    finish()
    for half in range(2):
        send_term(0, halves[half], half)
    weight_far(1)
    for half in range(2):
        own_term(0, halves[half], half)
        y_ring.start(0, half)
    weight_rest(1)
    first_join(0)
    send_term(1, whole_rows, 2)
    with jax.named_scope("bias_sums"):
        bias_sums()
    bias_send(bias_x, x, [at_x(by) for by in (1, 2, 3)], 0)
    weight_far(2)
    send_term(2, whole_rows, 3)
    send_term(3, whole_rows, 4)
    own_term(1, whole_rows, 2)
    y_ring.start_near(0)
    own_term(2, whole_rows, 3)
    y_ring.start_near(1)
    weight_rest(2)
    first_join(1)
    with jax.named_scope("join_y"):
        await_bytes(far_y, y_rs.at[0])
        y_ring.join()
    with jax.named_scope("bias_x"):
        await_bytes(bias_x.at[0:3], bias_rs.at[0])
        bias_z[z] = (bias_x[0] + bias_x[1]) + (bias_x[2] + bias_x[3])
    bias_send(bias_z, z, [at_z(by) for by in (1, 2, 3)], 1)
    own_term(3, whole_rows, 4)

    def second_start(p):
        with jax.named_scope(f"second_start_{p}"):
            await_bytes(near_join.at[p], ring_rs.at[p, 1])
            for side in range(2):
                ring = first_ring(p, side)
                for half in range(2):
                    second_ab[p, side, 2 * half : 2 * half + 2] = ring.half(half).astype(BF16)
            rings = [second_ring(p, side) for side in range(2)]
            if p in STRAIGHT:
                rings[0].start_straight(at_z(2))
                rings[1].start_straight(at_x(2))
                return
            for ring in rings:
                ring.start_far()
            for ring in rings:
                for d in range(2):
                    ring.start_near(d)

    def second_join(p):
        with jax.named_scope(f"second_join_{p}"):
            await_bytes(far2_ab.at[p], second_rs.at[p, 0])
            for side in range(2):
                second_ring(p, side).join()

    def second_finish(p):
        with jax.named_scope(f"second_finish_{p}"):
            await_bytes(near_join2.at[p], second_rs.at[p, 1])
            if p in STRAIGHT:
                await_bytes(far2_ab.at[p], second_rs.at[p, 0])
            for side in range(2):
                ring = second_ring(p, side)
                sums = [ring.half(half) for half in range(2)]
                if p in STRAIGHT:
                    sums = [sums[half] + far2_ab[p, side, half].astype(F32) for half in range(2)]
                total = jnp.concatenate(sums, axis=0)
                (wq_out, wk_out, wv_out)[p][:, side * HEAD : (side + 1) * HEAD] = total.T

    first_join(2)
    second_start(0)
    second_start(1)
    second_join(0)
    second_start(2)
    second_join(1)
    second_finish(0)
    with jax.named_scope("bias_z"):
        await_bytes(bias_z.at[0:3], bias_rs.at[1])
        sums = (bias_z[0] + bias_z[1]) + (bias_z[2] + bias_z[3])
        for h in range(HEADS):
            for piece in range(3):
                cut = slice(piece * TILE, min((piece + 1) * TILE, TABLE))
                bias_out[h : h + 1, cut] = sums[3 * h + piece : 3 * h + piece + 1, : cut.stop - cut.start]
    with jax.named_scope("input_sum"):
        await_bytes(near_join_y, y_rs.at[1])
        for d in range(2):
            input_out[d * (LENGTH // 2) : (d + 1) * (LENGTH // 2), :] = y_ring.half(d).astype(BF16)
    second_finish(1)
    second_finish(2)

    with jax.named_scope("drain"):
        await_bytes(whole.at[:, 0 : 2 * FEATURES], sent.at[0])
        await_bytes(whole.at[:, 0:FEATURES], sent.at[1])
        await_bytes(whole.at[:, 0 : 4 * FEATURES], sent.at[2])
        await_bytes(kv.at[0:REACH, :], sent.at[3])
        await_bytes(back_send, sent.at[4])
        await_bytes(far_ab, sent.at[5])
        await_bytes(near_join, sent.at[5])
        await_bytes(far2_ab, sent.at[6])
        await_bytes(near_join2, sent.at[6])
        await_bytes(far_y, sent.at[7])
        await_bytes(near_join_y, sent.at[7])
        await_bytes(term_recv, sent.at[8])
        await_bytes(bias_x.at[0:3], sent.at[9])
        await_bytes(bias_z.at[0:3], sent.at[9])


def store_results(*refs):
    sources, targets, sems = refs[:5], refs[5:10], refs[10]
    copies = [pltpu.make_async_copy(source, target, sems.at[n]) for n, (source, target) in enumerate(zip(sources, targets))]
    for copy in copies:
        copy.start()
    for copy in copies:
        copy.wait()


def shards(tokens, query_weight, key_weight, value_weight, position_bias, out_grad):
    anywhere = pl.BlockSpec(memory_space=pl.ANY)
    near = pl.BlockSpec(memory_space=pltpu.VMEM)
    dma = pltpu.SemaphoreType.DMA
    vmem = pltpu.VMEM
    grad = vmem((COLS, COLS), F32)
    results = pl.pallas_call(
        kernel,
        name="segment_attention_grads",
        out_shape=(
            vmem((LENGTH, FEATURES), BF16), grad, grad, grad,
            vmem((HEADS, TABLE), F32),
        ),
        in_specs=[anywhere] * 6,
        out_specs=(near,) * 5,
        scratch_shapes=[
            vmem((HEADS, TABLE), F32),
            vmem((LENGTH, WIDTH), BF16),
            vmem((WIDTH, 3 * COLS), BF16),
            vmem((2, TILE, 3 * COLS), F32),
            vmem((LENGTH, COLS), BF16),
            vmem((REACH + LENGTH, 2 * COLS), BF16),
            vmem((LENGTH, COLS), BF16),
            vmem((COLS, REACH + LENGTH), BF16),
            vmem((REACH + LENGTH, 2 * COLS), F32),
            vmem((LENGTH, 3 * COLS), BF16),
            vmem((3 * COLS, LENGTH), BF16),
            vmem((REACH, 2 * COLS), BF16),
            vmem((REACH, 2 * COLS), BF16),
            vmem((3, RING, RING, HEAD, COLS), BF16),
            vmem((3, RING, RING, HEAD, COLS), BF16),
            vmem((3, 2, 2, 2, HEAD, COLS), BF16),
            vmem((3, 2, 2, 2, 2, HEAD, COLS), BF16),
            vmem((3, 2, RING, HEAD, COLS), BF16),
            vmem((3, 2, 2, SEGMENT, COLS), BF16),
            vmem((3, 2, 2, 2, SEGMENT, COLS), BF16),
            vmem((RING, LENGTH, FEATURES), BF16),
            vmem((RING, LENGTH, FEATURES), BF16),
            vmem((RING, LENGTH, FEATURES), BF16),
            vmem((2, LENGTH // 2, FEATURES), BF16),
            vmem((2, 2, LENGTH // 2, FEATURES), BF16),
            vmem((HEADS, SPAN, TILE), F32),
            vmem((HEADS, SPAN, TILE), F32),
            vmem((RING, 8, TILE), F32),
            vmem((RING, 8, TILE), F32),
            dma((8,)),
            dma((CHUNKS,)), dma((CHUNKS,)), dma((CHUNKS,)), dma((CHUNKS,)), dma((CHUNKS,)),
            dma((3,)),
            dma((RING + 1,)),
            dma((3, 2)), dma((3, 2)), dma((2,)),
            dma((2,)),
            dma((10,)),
        ],
        compiler_params=pltpu.CompilerParams(
            collective_id=0, has_side_effects=True, vmem_limit_bytes=62_000_000
        ),
    )(tokens, query_weight, key_weight, value_weight, position_bias, out_grad)
    return pl.pallas_call(
        store_results,
        name="store_results",
        out_shape=tuple(jax.ShapeDtypeStruct(result.shape, result.dtype) for result in results),
        in_specs=[near] * 5,
        out_specs=(anywhere,) * 5,
        scratch_shapes=[dma((5,))],
        compiler_params=pltpu.CompilerParams(vmem_limit_bytes=1_000_000),
    )(*results)


def solution(mesh):
    return jax.shard_map(
        shards,
        mesh=mesh,
        in_specs=(P("sp", "tp"), P(None, "tp"), P(None, "tp"), P(None, "tp"), P("tp", None), P("sp", "tp")),
        out_specs=(P("sp", "tp"), P("sp", "tp"), P("sp", "tp"), P("sp", "tp"), P("tp", None)),
        check_vma=False,
    )
```

```python
import functools

import jax
import jax.numpy as jnp
from jax import lax
from jax.experimental import pallas as pl
from jax.experimental.pallas import tpu as pltpu
from jax.sharding import PartitionSpec as P

MESH = pl.DeviceIdType.MESH
BF16, F32 = jnp.bfloat16, jnp.float32
SEGMENT, REACH, CLIP, HEAD = 64, 256, 256, 128
TILE = 128
SPAN = REACH + TILE
LENGTH, WIDTH, FEATURES = 768, 4096, 512
CHUNKS = LENGTH // TILE
HEADS = 2
COLS = HEADS * HEAD
FACTOR = HEAD ** (-0.5)
RING = 4
LOG2_E = 1.4426950408889634
TABLE = 320
ROUND = 512
AHEAD = (2, 1, 3, 0)
STRAIGHT = (2,)


def dot(left, right, left_dim=1, right_dim=0):
    return lax.dot_general(left, right, (((left_dim,), (right_dim,)), ((), ())), preferred_element_type=F32)


class Ring:
    def __init__(self, me, up, down, block, via, direct, joined, sent, far_sem, rest_sem):
        self.near = (lax.rem(me + 1, RING), lax.rem(me + RING - 1, RING))
        self.far = lax.rem(me + 2, RING)
        self.me, self.devices, self.block = me, (up, down), block
        self.landing = (via, direct, joined)
        self.sent, self.arrived = sent, (far_sem, rest_sem, rest_sem)

    def start(self, kind, d):
        source = (self.block(self.far, d), self.block(self.near[d], 1 - d), self.block(self.near[d], d))[kind]
        pltpu.make_async_remote_copy(
            src_ref=source,
            dst_ref=self.landing[kind](d),
            send_sem=self.sent,
            recv_sem=self.arrived[kind],
            device_id=self.devices[d],
            device_id_type=MESH,
        ).start()

    def start_straight(self, opposite):
        for d in range(2):
            pltpu.make_async_remote_copy(
                src_ref=self.block(self.far, d),
                dst_ref=self.landing[0](d),
                send_sem=self.sent,
                recv_sem=self.arrived[0],
                device_id=opposite,
                device_id_type=MESH,
            ).start()
        for kind in (1, 2):
            for d in range(2):
                self.start(kind, d)

    def start_far(self):
        for d in range(2):
            self.start(0, d)

    def start_near(self, d):
        self.start(1, d)

    def join(self):
        for d in range(2):
            ref = self.block(self.near[d], d)
            ref[...] = (ref[...].astype(F32) + self.landing[0](d)[...].astype(F32)).astype(BF16)
            self.start(2, d)

    def half(self, d):
        total = self.block(self.me, d)[...].astype(F32) + self.landing[2](d)[...].astype(F32)
        return total + self.landing[1](1 - d)[...].astype(F32)


def await_bytes(view, sem):
    pltpu.make_async_copy(view, view, sem).wait()


def kernel(
    tokens, wq, wk, wv, position_bias, out_grad,
    input_out, wq_out, wk_out, wv_out, bias_out,
    table, whole, weight, projected, query, kv, upstream, keys_t, dkv, grads, grads_t, back_send, back_recv,
    part_a, part_b, far_ab, near_join, second_ab, far2_ab, near_join2,
    term_own, term_send, term_recv, far_y, near_join_y,
    bias, dsum, bias_x, bias_z,
    load_sem, pass_recv, gather_recv, hop_recv, core_recv, last_recv, halo_recv, term_rs, ring_rs, second_rs, y_rs, bias_rs, sent,
):
    sp, tp = lax.axis_index("sp"), lax.axis_index("tp")
    z, x = sp // RING, lax.rem(sp, RING)
    y, core = tp // 2, lax.rem(tp, 2)

    def at(value, by):
        return lax.rem(value + by, RING)

    def at_x(by):
        return (z * RING + at(x, by), tp)

    def at_z(by):
        return (at(z, by) * RING + x, tp)

    def at_y(by):
        return (sp, at(y, by) * 2 + core)

    def at_sp(by):
        return (lax.rem(sp + by, 16), tp)

    partner = (sp, y * 2 + 1 - core)

    barrier = pltpu.get_barrier_semaphore()
    peers = [partner, at_sp(1), at_sp(15)]
    for by in (1, 3):
        peers.append(at_y(by))
    for by in (1, 2, 3):
        peers += [at_x(by), at_z(by)]
    for peer in peers:
        pl.semaphore_signal(barrier, inc=1, device_id=peer, device_id_type=MESH)

    def feature_cols(y_index, core_index):
        return pl.ds(pl.multiple_of((y_index * 2 + core_index) * FEATURES, FEATURES), FEATURES)

    my_cols = feature_cols(y, core)
    own_loads = []
    for number, (first, last) in enumerate(((4 * TILE, 5 * TILE), (5 * TILE, 6 * TILE), (0, 4 * TILE))):
        own = pltpu.make_async_copy(tokens.at[first:last, :], whole.at[first:last, my_cols], load_sem.at[number])
        own.start()
        own_loads.append(own)
    with jax.named_scope("entry"):
        pl.semaphore_wait(barrier, len(peers))

    def rows_of(step):
        return pl.multiple_of(lax.rem(step + 4, CHUNKS) * TILE, TILE)

    def chunk_copy(rows, cols, target, send, recv):
        view = whole.at[rows, cols]
        return pltpu.make_async_remote_copy(
            src_ref=view, dst_ref=view, send_sem=send, recv_sem=recv, device_id=target, device_id_type=MESH
        )

    up, down = at_y(1), at_y(3)

    def gather_start(step):
        for half in range(2):
            for d in range(2):
                first = pl.multiple_of(rows_of(step) + (half ^ d) * SEGMENT, SEGMENT)
                sem = (pass_recv, gather_recv)[half].at[step]
                chunk_copy(pl.ds(first, SEGMENT), my_cols, (up, down)[d], sent.at[0], sem).start()

    def hop_copy(step, d):
        cols = feature_cols(at(y, (3, 1)[d]), core)
        rows = pl.ds(pl.multiple_of(rows_of(step) + d * SEGMENT, SEGMENT), SEGMENT)
        return chunk_copy(rows, cols, (up, down)[d], sent.at[0], hop_recv.at[step])

    def core_copy(step, which):
        cols = feature_cols(at(y, (0, 3, 1, 2)[which]), core)
        sem = (last_recv if which == 3 else core_recv).at[step]
        return chunk_copy(pl.ds(rows_of(step), TILE), cols, partner, sent.at[0], sem)

    def halo_copy(step):
        return pltpu.make_async_remote_copy(
            src_ref=kv.at[pl.ds(pl.multiple_of(LENGTH + step * TILE, TILE), TILE), :],
            dst_ref=kv.at[pl.ds(pl.multiple_of(step * TILE, TILE), TILE), :],
            send_sem=sent.at[0],
            recv_sem=halo_recv.at[0],
            device_id=at_sp(1),
            device_id_type=MESH,
        )

    def back_start(half):
        rows = slice(half * TILE, (half + 1) * TILE)
        back_send[rows] = dkv[rows, :].astype(BF16)
        pltpu.make_async_remote_copy(
            src_ref=back_send.at[rows],
            dst_ref=back_recv.at[rows],
            send_sem=sent.at[0],
            recv_sem=halo_recv.at[1],
            device_id=at_sp(15),
            device_id_type=MESH,
        ).start()

    edge = jnp.where(sp == 0, REACH, 0)
    row = lax.broadcasted_iota(jnp.int32, (SPAN, TILE), 0)

    def ranges(tile):
        start = tile * TILE if isinstance(tile, int) else pl.multiple_of(tile * TILE, TILE)
        return start, pl.ds(start, SPAN), pl.ds(start, TILE)

    head_cols = [slice(h * HEAD, (h + 1) * HEAD) for h in range(HEADS)]
    value_cols = [slice(COLS + h * HEAD, COLS + (h + 1) * HEAD) for h in range(HEADS)]

    def attend_products(tile):
        _, keys_at, here = ranges(tile)
        return [
            (dot(kv[keys_at, head_cols[h]], query[here, head_cols[h]], 1, 1), dot(kv[keys_at, value_cols[h]], upstream[here, head_cols[h]], 1, 1))
            for h in range(HEADS)
        ]

    def attend_weights(tile, products):
        start, _, _ = ranges(tile)
        lows = []
        for h in range(HEADS):
            raw, prob_grad = products[h]
            scores = raw * (FACTOR * LOG2_E) + bias[h]
            if not isinstance(tile, int):
                scores = jnp.where(row + start < edge, -jnp.inf, scores)
            raised = jnp.exp2(scores - jnp.max(scores, axis=0, keepdims=True))
            weights = raised * (1.0 / jnp.sum(raised, axis=0, keepdims=True))
            delta = jnp.sum(weights * prob_grad, axis=0, keepdims=True)
            score_grad = weights * (prob_grad - delta)
            dsum[h] = dsum[h] + score_grad
            lows.append((weights.astype(BF16), score_grad.astype(BF16)))
        return lows

    def attend_queries(tile, lows):
        _, keys_at, here = ranges(tile)
        for h in range(HEADS):
            grads_t[head_cols[h], here] = (dot(keys_t[head_cols[h], keys_at], lows[h][1]) * FACTOR).astype(BF16)

    def attend_keys(tile, lows):
        _, keys_at, here = ranges(tile)
        for h in range(HEADS):
            weights_low, score_low = lows[h]
            dkv[keys_at, value_cols[h]] = dkv[keys_at, value_cols[h]] + dot(weights_low, upstream[here, head_cols[h]])
            dkv[keys_at, head_cols[h]] = dkv[keys_at, head_cols[h]] + dot(score_low, query[here, head_cols[h]])

    def attend(tile):
        lows = attend_weights(tile, attend_products(tile))
        attend_queries(tile, lows)
        attend_keys(tile, lows)

    for step in range(2):
        own_loads[step].wait()
        gather_start(step)
        core_copy(step, 0).start()
    own_loads[2].wait()

    table_load = pltpu.make_async_copy(position_bias, table, load_sem.at[5])
    table_load.start()
    loads = []
    for number, ref in enumerate((wq, wk, wv)):
        loads.append(pltpu.make_async_copy(ref, weight.at[:, number * COLS : (number + 1) * COLS], load_sem.at[3]))
    loads.append(pltpu.make_async_copy(out_grad, upstream, load_sem.at[4]))
    for load in loads:
        load.start()

    lane = lax.broadcasted_iota(jnp.int32, (8, ROUND), 1)
    column = lax.broadcasted_iota(jnp.int32, (SPAN, TILE), 1)
    low = jnp.where(column >= SEGMENT, SEGMENT, 0)
    seen = (row >= low) & (row < low + REACH + SEGMENT)
    table_load.wait()
    for h in range(HEADS):
        entries = jnp.broadcast_to(table[h : h + 1, :], (8, TABLE))
        padded = jnp.concatenate([entries, jnp.zeros((8, ROUND - TABLE), F32)], axis=1)
        turned = pltpu.roll(padded, ROUND - TABLE + 1, 1)
        last = jnp.broadcast_to(table[h : h + 1, TABLE - 1 : TABLE], (8, ROUND))
        turned = jnp.where(lane < TILE, last, turned)
        skewed = pltpu.roll(jnp.broadcast_to(turned[0:1, :], (SPAN, ROUND)), 0, 1, stride=1, stride_axis=0)
        bias[h] = jnp.where(seen, skewed[:, :TILE] * LOG2_E, -jnp.inf)
        dsum[h] = jnp.zeros((SPAN, TILE), F32)
    dkv[...] = jnp.zeros(dkv.shape, F32)

    await_bytes(weight, load_sem.at[3])
    loads[3].wait()

    def project_from(step, blocks):
        total = None
        for which in blocks:
            for on in (core, 1 - core):
                cols = feature_cols(at(y, (0, 3, 1, 2)[which]), on)
                part = dot(whole[pl.ds(rows_of(step), TILE), cols], weight[cols, :])
                total = part if total is None else total + part
        return total

    def hop_landed(step):
        with jax.named_scope("hop_wait"):
            await_bytes(whole.at[0:TILE, 0:FEATURES], hop_recv.at[step])
            core_copy(step, 3).start()

    def project_most(step):
        with jax.named_scope("core_wait"):
            await_bytes(whole.at[0:TILE, 0 : 3 * FEATURES], core_recv.at[step])
        with jax.named_scope("project"):
            projected[lax.rem(step, 2)] = project_from(step, (0, 1, 2))

    def gather_step(s, carry):
        @pl.when(s < CHUNKS)
        def _():
            with jax.named_scope("pass_wait"):
                await_bytes(whole.at[0:TILE, 0:FEATURES], pass_recv.at[s])
                for d in range(2):
                    hop_copy(s, d).start()

        @pl.when(s < CHUNKS - 2)
        def _():
            gather_start(s + 2)
            core_copy(s + 2, 0).start()

        @pl.when((s >= 1) & (s < CHUNKS))
        def _():
            project_most(s - 1)

        @pl.when(s < CHUNKS)
        def _():
            with jax.named_scope("gather_wait"):
                await_bytes(whole.at[0:TILE, 0:FEATURES], gather_recv.at[s])
                for d in range(2):
                    core_copy(s, 1 + d).start()

        @pl.when(s >= 1)
        def _():
            hop_landed(s - 1)

        @pl.when(s == CHUNKS - 1)
        def _():
            project_most(s)

        @pl.when(s == 4)
        def _():
            with jax.named_scope("halo_wait"):
                await_bytes(kv.at[0:REACH, :], halo_recv.at[0])
                keys_t[:, 0:REACH] = kv[0:REACH, :COLS].T

        @pl.when((s == 4) | (s == 6))
        def _():
            with jax.named_scope("attend"):
                attend(jnp.where(s == 4, 0, 2))

            @pl.when(s == 4)
            def _():
                back_start(0)

        @pl.when(s >= 1)
        def _():
            with jax.named_scope("last_wait"):
                await_bytes(whole.at[0:TILE, 0:FEATURES], last_recv.at[s - 1])
            with jax.named_scope("project_rest"):
                start = rows_of(s - 1)
                low = (projected[lax.rem(s - 1, 2)] + project_from(s - 1, (3,))).astype(BF16)
                query[pl.ds(start, TILE), :] = low[:, :COLS]
                kv[pl.ds(pl.multiple_of(start + REACH, TILE), TILE), :] = low[:, COLS:]
                keys_t[:, pl.ds(pl.multiple_of(start + REACH, TILE), TILE)] = low[:, COLS : 2 * COLS].T

        @pl.when((s >= 1) & (s <= 2))
        def _():
            halo_copy(s - 1).start()

        @pl.when(s == 4)
        def _():
            with jax.named_scope("attend"):
                attend(s - 3)
            back_start(1)

        return carry

    lax.fori_loop(0, CHUNKS + 1, gather_step, 0)
    with jax.named_scope("attend_last"):
        products = {tile: attend_products(tile) for tile in (3, 4)}
        lows = {3: attend_weights(3, products[3])}
        products[5] = attend_products(5)
        attend_queries(3, lows[3])
        for tile in (4, 5):
            lows[tile] = attend_weights(tile, products[tile])
            attend_queries(tile, lows[tile])
            attend_keys(tile - 1, lows[tile - 1])
        attend_keys(5, lows[5])

    def first_ring(p, side):
        me = (x, z)[side]
        part = (part_a, part_b)[side]
        at_side = (at_x, at_z)[side]
        return Ring(
            me, at_side(1), at_side(3),
            lambda k, half: part.at[p, k, pl.ds(2 * half, 2)],
            lambda d: far_ab.at[p, side, d],
            lambda d: near_join.at[p, 0, side, d],
            lambda d: near_join.at[p, 1, side, d],
            sent.at[0], ring_rs.at[p, 0], ring_rs.at[p, 1],
        )

    def second_ring(p, side):
        me = (z, x)[side]
        at_side = (at_z, at_x)[side]
        return Ring(
            me, at_side(1), at_side(3),
            lambda k, half: second_ab.at[p, side, k, half * SEGMENT : (half + 1) * SEGMENT],
            lambda d: far2_ab.at[p, side, d],
            lambda d: near_join2.at[p, 0, side, d],
            lambda d: near_join2.at[p, 1, side, d],
            sent.at[0], second_rs.at[p, 0], second_rs.at[p, 1],
        )

    y_ring = Ring(
        y, up, down,
        lambda k, half: term_own.at[k, half * (LENGTH // 2) : (half + 1) * (LENGTH // 2)],
        lambda d: far_y.at[d],
        lambda d: near_join_y.at[0, d],
        lambda d: near_join_y.at[1, d],
        sent.at[0], y_rs.at[0], y_rs.at[1],
    )

    halves = (slice(0, LENGTH // 2), slice(LENGTH // 2, LENGTH))

    def term(y_index, core_index, rows):
        start = pl.multiple_of((y_index * 2 + core_index) * FEATURES, FEATURES)
        return dot(grads[rows, :], weight[pl.ds(start, FEATURES), :], 1, 1)

    def send_term(k, rows, sem):
        with jax.named_scope("term_send"):
            term_send[k, rows] = term(at(y, AHEAD[k]), 1 - core, rows).astype(BF16)
        pltpu.make_async_remote_copy(
            src_ref=term_send.at[k, rows],
            dst_ref=term_recv.at[k, rows],
            send_sem=sent.at[0],
            recv_sem=term_rs.at[sem],
            device_id=partner,
            device_id_type=MESH,
        ).start()

    def own_term(k, rows, sem):
        with jax.named_scope("term_own"):
            y_index = at(y, AHEAD[k])
            made = term(y_index, core, rows)
            await_bytes(term_recv.at[k, rows], term_rs.at[sem])
            term_own[y_index, rows] = (made + term_recv[k, rows].astype(F32)).astype(BF16)

    def bias_send(buffer, me, targets, which):
        view = buffer.at[me]
        for target in targets:
            pltpu.make_async_remote_copy(
                src_ref=view, dst_ref=view, send_sem=sent.at[0], recv_sem=bias_rs.at[which], device_id=target, device_id_type=MESH
            ).start()

    def bias_sums():
        bias_x[x] = jnp.zeros((8, TILE), F32)
        for h in range(HEADS):
            wide = jnp.concatenate([dsum[h], jnp.zeros((SPAN, ROUND - TILE), F32)], axis=1)
            rows = SPAN
            while rows > 24:
                rows //= 2
                wide = wide[:rows] + pltpu.roll(wide[rows:], ROUND - rows, 1)
            wide = wide[0:8] + pltpu.roll(wide[8:16], ROUND - 8, 1) + pltpu.roll(wide[16:24], ROUND - 16, 1)
            sums = wide[0:1]
            for r in range(1, 8):
                sums = sums + pltpu.roll(wide[r : r + 1], ROUND - r, 1)
            first = lax.broadcasted_iota(jnp.int32, (1, ROUND), 1)
            clipped = jnp.sum(jnp.where(first < TILE, sums, 0.0), axis=1, keepdims=True)
            placed = pltpu.roll(sums, TABLE - 1, 1)
            sums = jnp.where(first == TABLE - 1, clipped, placed)
            for piece in range(3):
                bias_x[x, 3 * h + piece : 3 * h + piece + 1, :] = sums[:, piece * TILE : (piece + 1) * TILE]

    def finish():
        with jax.named_scope("back_wait"):
            await_bytes(back_recv, halo_recv.at[1])
            dkv[LENGTH:, :] = dkv[LENGTH:, :] + back_recv[...].astype(F32)

        def finish_chunk(chunk, carry):
            start = pl.multiple_of(chunk * TILE, TILE)
            grads[pl.ds(start, TILE), :COLS] = grads_t[:COLS, pl.ds(start, TILE)].T
            total = dkv[pl.ds(pl.multiple_of(start + REACH, TILE), TILE), :]
            total = jnp.concatenate([total[:, :COLS] * FACTOR, total[:, COLS:]], axis=1)
            grads[pl.ds(start, TILE), COLS:] = total.astype(BF16)
            grads_t[COLS:, pl.ds(start, TILE)] = total.T.astype(BF16)
            return carry

        with jax.named_scope("finish"):
            lax.fori_loop(0, CHUNKS, finish_chunk, 0)

    def weight_row(k, z_index):
        features = pl.ds(pl.multiple_of(z_index * RING * COLS, RING * COLS), RING * COLS)
        made = dot(grads_t[k * COLS : (k + 1) * COLS, :], whole[:, features]).astype(BF16)
        for x_index in range(RING):
            cut = slice(x_index * COLS, (x_index + 1) * COLS)
            part_b[k, z_index, x_index] = made[HEAD:, cut]
            part_a[k, jnp.where(x_index == at(x, 2), RING, x_index), z_index] = made[:HEAD, cut]

    def weight_far(k):
        far_x = at(x, 2)
        with jax.named_scope("weight_far"):
            for z_index in range(RING):
                features = pl.ds(pl.multiple_of(z_index * RING * COLS + far_x * COLS, COLS), COLS)
                left = grads_t[k * COLS : k * COLS + HEAD, :]
                part_a[k, far_x, z_index] = dot(left, whole[:, features]).astype(BF16)
            first_ring(k, 0).start_far()
            weight_row(k, at(z, 2))
            first_ring(k, 1).start_far()

    def weight_rest(k):
        def rows(i, inner):
            weight_row(k, at(z, i))
            return inner

        with jax.named_scope("weight_rest"):
            lax.fori_loop(3, RING + 2, rows, 0)
        for side in range(2):
            for d in range(2):
                first_ring(k, side).start_near(d)

    def first_join(p):
        with jax.named_scope("join_first"):
            await_bytes(far_ab.at[p], ring_rs.at[p, 0])
            for side in range(2):
                first_ring(p, side).join()

    whole_rows = slice(0, LENGTH)
    weight_far(0)
    weight_rest(0)
    finish()
    for half in range(2):
        send_term(0, halves[half], half)
    weight_far(1)
    for half in range(2):
        own_term(0, halves[half], half)
        y_ring.start(0, half)
    weight_rest(1)
    first_join(0)
    send_term(1, whole_rows, 2)
    with jax.named_scope("bias_sums"):
        bias_sums()
    bias_send(bias_x, x, [at_x(by) for by in (1, 2, 3)], 0)
    weight_far(2)
    send_term(2, whole_rows, 3)
    send_term(3, whole_rows, 4)
    own_term(1, whole_rows, 2)
    y_ring.start_near(0)
    own_term(2, whole_rows, 3)
    y_ring.start_near(1)
    weight_rest(2)
    first_join(1)
    with jax.named_scope("join_y"):
        await_bytes(far_y, y_rs.at[0])
        y_ring.join()
    with jax.named_scope("bias_x"):
        await_bytes(bias_x.at[0:3], bias_rs.at[0])
        bias_z[z] = (bias_x[0] + bias_x[1]) + (bias_x[2] + bias_x[3])
    bias_send(bias_z, z, [at_z(by) for by in (1, 2, 3)], 1)
    own_term(3, whole_rows, 4)

    def second_start(p):
        with jax.named_scope(f"second_start_{p}"):
            await_bytes(near_join.at[p], ring_rs.at[p, 1])
            for side in range(2):
                ring = first_ring(p, side)
                for half in range(2):
                    second_ab[p, side, 2 * half : 2 * half + 2] = ring.half(half).astype(BF16)
            rings = [second_ring(p, side) for side in range(2)]
            if p in STRAIGHT:
                rings[0].start_straight(at_z(2))
                rings[1].start_straight(at_x(2))
                return
            for ring in rings:
                ring.start_far()
            for ring in rings:
                for d in range(2):
                    ring.start_near(d)

    def second_join(p):
        with jax.named_scope(f"second_join_{p}"):
            await_bytes(far2_ab.at[p], second_rs.at[p, 0])
            for side in range(2):
                second_ring(p, side).join()

    def second_finish(p):
        with jax.named_scope(f"second_finish_{p}"):
            await_bytes(near_join2.at[p], second_rs.at[p, 1])
            if p in STRAIGHT:
                await_bytes(far2_ab.at[p], second_rs.at[p, 0])
            for side in range(2):
                ring = second_ring(p, side)
                sums = [ring.half(half) for half in range(2)]
                if p in STRAIGHT:
                    sums = [sums[half] + far2_ab[p, side, half].astype(F32) for half in range(2)]
                total = jnp.concatenate(sums, axis=0)
                (wq_out, wk_out, wv_out)[p][:, side * HEAD : (side + 1) * HEAD] = total.T

    first_join(2)
    second_start(0)
    second_start(1)
    second_join(0)
    second_start(2)
    second_join(1)
    second_finish(0)
    with jax.named_scope("bias_z"):
        await_bytes(bias_z.at[0:3], bias_rs.at[1])
        sums = (bias_z[0] + bias_z[1]) + (bias_z[2] + bias_z[3])
        for h in range(HEADS):
            for piece in range(3):
                cut = slice(piece * TILE, min((piece + 1) * TILE, TABLE))
                bias_out[h : h + 1, cut] = sums[3 * h + piece : 3 * h + piece + 1, : cut.stop - cut.start]
    with jax.named_scope("input_sum"):
        await_bytes(near_join_y, y_rs.at[1])
        for d in range(2):
            input_out[d * (LENGTH // 2) : (d + 1) * (LENGTH // 2), :] = y_ring.half(d).astype(BF16)
    second_finish(1)
    second_finish(2)

    with jax.named_scope("drain"):
        await_bytes(whole.at[:, 0 : 2 * FEATURES], sent.at[0])
        await_bytes(whole.at[:, 0:FEATURES], sent.at[0])
        await_bytes(whole.at[:, 0 : 4 * FEATURES], sent.at[0])
        await_bytes(kv.at[0:REACH, :], sent.at[0])
        await_bytes(back_send, sent.at[0])
        await_bytes(far_ab, sent.at[0])
        await_bytes(near_join, sent.at[0])
        await_bytes(far2_ab, sent.at[0])
        await_bytes(near_join2, sent.at[0])
        await_bytes(far_y, sent.at[0])
        await_bytes(near_join_y, sent.at[0])
        await_bytes(term_recv, sent.at[0])
        await_bytes(bias_x.at[0:3], sent.at[0])
        await_bytes(bias_z.at[0:3], sent.at[0])


def store_results(*refs):
    sources, targets, sems = refs[:5], refs[5:10], refs[10]
    copies = [pltpu.make_async_copy(source, target, sems.at[n]) for n, (source, target) in enumerate(zip(sources, targets))]
    for copy in copies:
        copy.start()
    for copy in copies:
        copy.wait()


def shards(tokens, query_weight, key_weight, value_weight, position_bias, out_grad):
    anywhere = pl.BlockSpec(memory_space=pl.ANY)
    near = pl.BlockSpec(memory_space=pltpu.VMEM)
    dma = pltpu.SemaphoreType.DMA
    vmem = pltpu.VMEM
    grad = vmem((COLS, COLS), F32)
    results = pl.pallas_call(
        kernel,
        name="segment_attention_grads",
        out_shape=(
            vmem((LENGTH, FEATURES), BF16), grad, grad, grad,
            vmem((HEADS, TABLE), F32),
        ),
        in_specs=[anywhere] * 6,
        out_specs=(near,) * 5,
        scratch_shapes=[
            vmem((HEADS, TABLE), F32),
            vmem((LENGTH, WIDTH), BF16),
            vmem((WIDTH, 3 * COLS), BF16),
            vmem((2, TILE, 3 * COLS), F32),
            vmem((LENGTH, COLS), BF16),
            vmem((REACH + LENGTH, 2 * COLS), BF16),
            vmem((LENGTH, COLS), BF16),
            vmem((COLS, REACH + LENGTH), BF16),
            vmem((REACH + LENGTH, 2 * COLS), F32),
            vmem((LENGTH, 3 * COLS), BF16),
            vmem((3 * COLS, LENGTH), BF16),
            vmem((REACH, 2 * COLS), BF16),
            vmem((REACH, 2 * COLS), BF16),
            vmem((3, RING + 1, RING, HEAD, COLS), BF16),
            vmem((3, RING, RING, HEAD, COLS), BF16),
            vmem((3, 2, 2, 2, HEAD, COLS), BF16),
            vmem((3, 2, 2, 2, 2, HEAD, COLS), BF16),
            vmem((3, 2, RING, HEAD, COLS), BF16),
            vmem((3, 2, 2, SEGMENT, COLS), BF16),
            vmem((3, 2, 2, 2, SEGMENT, COLS), BF16),
            vmem((RING, LENGTH, FEATURES), BF16),
            vmem((RING, LENGTH, FEATURES), BF16),
            vmem((RING, LENGTH, FEATURES), BF16),
            vmem((2, LENGTH // 2, FEATURES), BF16),
            vmem((2, 2, LENGTH // 2, FEATURES), BF16),
            vmem((HEADS, SPAN, TILE), F32),
            vmem((HEADS, SPAN, TILE), F32),
            vmem((RING, 8, TILE), F32),
            vmem((RING, 8, TILE), F32),
            dma((6,)),
            dma((CHUNKS,)), dma((CHUNKS,)), dma((CHUNKS,)), dma((CHUNKS,)), dma((CHUNKS,)),
            dma((3,)),
            dma((RING + 1,)),
            dma((3, 2)), dma((3, 2)), dma((2,)),
            dma((2,)),
            dma((1,)),
        ],
        compiler_params=pltpu.CompilerParams(
            collective_id=0, has_side_effects=True, vmem_limit_bytes=62_000_000
        ),
    )(tokens, query_weight, key_weight, value_weight, position_bias, out_grad)
    return pl.pallas_call(
        store_results,
        name="store_results",
        out_shape=tuple(jax.ShapeDtypeStruct(result.shape, result.dtype) for result in results),
        in_specs=[near] * 5,
        out_specs=(anywhere,) * 5,
        scratch_shapes=[dma((5,))],
        compiler_params=pltpu.CompilerParams(vmem_limit_bytes=1_000_000),
    )(*results)


def solution(mesh):
    return jax.shard_map(
        shards,
        mesh=mesh,
        in_specs=(P("sp", "tp"), P(None, "tp"), P(None, "tp"), P(None, "tp"), P("tp", None), P("sp", "tp")),
        out_specs=(P("sp", "tp"), P("sp", "tp"), P("sp", "tp"), P("sp", "tp"), P("tp", None)),
        check_vma=False,
    )
```

```python
import functools

import jax
import jax.numpy as jnp
from jax import lax
from jax.experimental import pallas as pl
from jax.experimental.pallas import tpu as pltpu
from jax.sharding import PartitionSpec as P

MESH = pl.DeviceIdType.MESH
BF16, F32 = jnp.bfloat16, jnp.float32
SEGMENT, REACH, CLIP, HEAD = 64, 256, 256, 128
TILE = 128
SPAN = REACH + TILE
LENGTH, WIDTH, FEATURES = 768, 4096, 512
CHUNKS = LENGTH // TILE
HEADS = 2
COLS = HEADS * HEAD
FACTOR = HEAD ** (-0.5)
RING = 4
LOG2_E = 1.4426950408889634
TABLE = 320
ROUND = 512
AHEAD = (2, 1, 3, 0)
STRAIGHT = (2,)


def dot(left, right, left_dim=1, right_dim=0):
    return lax.dot_general(left, right, (((left_dim,), (right_dim,)), ((), ())), preferred_element_type=F32)


class Ring:
    def __init__(self, me, up, down, block, via, direct, joined, sent, far_sem, rest_sem):
        self.near = (lax.rem(me + 1, RING), lax.rem(me + RING - 1, RING))
        self.far = lax.rem(me + 2, RING)
        self.me, self.devices, self.block = me, (up, down), block
        self.landing = (via, direct, joined)
        self.sent, self.arrived = sent, (far_sem, rest_sem, rest_sem)

    def start(self, kind, d):
        source = (self.block(self.far, d), self.block(self.near[d], 1 - d), self.block(self.near[d], d))[kind]
        pltpu.make_async_remote_copy(
            src_ref=source,
            dst_ref=self.landing[kind](d),
            send_sem=self.sent,
            recv_sem=self.arrived[kind],
            device_id=self.devices[d],
            device_id_type=MESH,
        ).start()

    def start_straight(self, opposite):
        for d in range(2):
            pltpu.make_async_remote_copy(
                src_ref=self.block(self.far, d),
                dst_ref=self.landing[0](d),
                send_sem=self.sent,
                recv_sem=self.arrived[0],
                device_id=opposite,
                device_id_type=MESH,
            ).start()
        for kind in (1, 2):
            for d in range(2):
                self.start(kind, d)

    def start_far(self):
        for d in range(2):
            self.start(0, d)

    def start_near(self, d):
        self.start(1, d)

    def join(self):
        for d in range(2):
            ref = self.block(self.near[d], d)
            ref[...] = (ref[...].astype(F32) + self.landing[0](d)[...].astype(F32)).astype(BF16)
            self.start(2, d)

    def half(self, d):
        total = self.block(self.me, d)[...].astype(F32) + self.landing[2](d)[...].astype(F32)
        return total + self.landing[1](1 - d)[...].astype(F32)


def await_bytes(view, sem):
    pltpu.make_async_copy(view, view, sem).wait()


def kernel(
    tokens, wq, wk, wv, position_bias, out_grad,
    input_out, wq_out, wk_out, wv_out, bias_out,
    table, whole, weight, projected, query, kv, upstream, keys_t, dkv, grads, grads_t, back_send, back_recv,
    part_a, part_b, far_ab, near_join, second_ab, far2_ab, near_join2,
    term_own, term_send, term_recv, far_y, near_join_y,
    bias, dsum, bias_x, bias_z,
    load_sem, pass_recv, gather_recv, hop_recv, core_recv, last_recv, halo_recv, term_rs, ring_rs, second_rs, y_rs, bias_rs, sent,
):
    sp, tp = lax.axis_index("sp"), lax.axis_index("tp")
    z, x = sp // RING, lax.rem(sp, RING)
    y, core = tp // 2, lax.rem(tp, 2)

    def at(value, by):
        return lax.rem(value + by, RING)

    def at_x(by):
        return (z * RING + at(x, by), tp)

    def at_z(by):
        return (at(z, by) * RING + x, tp)

    def at_y(by):
        return (sp, at(y, by) * 2 + core)

    def at_sp(by):
        return (lax.rem(sp + by, 16), tp)

    partner = (sp, y * 2 + 1 - core)

    barrier = pltpu.get_barrier_semaphore()
    peers = [partner, at_sp(1), at_sp(15)]
    for by in (1, 3):
        peers.append(at_y(by))
    for by in (1, 2, 3):
        peers += [at_x(by), at_z(by)]
    for peer in peers:
        pl.semaphore_signal(barrier, inc=1, device_id=peer, device_id_type=MESH)

    def feature_cols(y_index, core_index):
        return pl.ds(pl.multiple_of((y_index * 2 + core_index) * FEATURES, FEATURES), FEATURES)

    my_cols = feature_cols(y, core)
    own_loads = []
    for number, (first, last) in enumerate(((4 * TILE, 5 * TILE), (5 * TILE, 6 * TILE), (0, 4 * TILE))):
        own = pltpu.make_async_copy(tokens.at[first:last, :], whole.at[first:last, my_cols], load_sem.at[number])
        own.start()
        own_loads.append(own)
    with jax.named_scope("entry"):
        pl.semaphore_wait(barrier, len(peers))

    def rows_of(step):
        return pl.multiple_of(lax.rem(step + 4, CHUNKS) * TILE, TILE)

    def chunk_copy(rows, cols, target, send, recv):
        view = whole.at[rows, cols]
        return pltpu.make_async_remote_copy(
            src_ref=view, dst_ref=view, send_sem=send, recv_sem=recv, device_id=target, device_id_type=MESH
        )

    up, down = at_y(1), at_y(3)

    def gather_start(step):
        for half in range(2):
            for d in range(2):
                first = pl.multiple_of(rows_of(step) + (half ^ d) * SEGMENT, SEGMENT)
                sem = (pass_recv, gather_recv)[half].at[step]
                chunk_copy(pl.ds(first, SEGMENT), my_cols, (up, down)[d], sent.at[0], sem).start()

    def hop_copy(step, d):
        cols = feature_cols(at(y, (3, 1)[d]), core)
        rows = pl.ds(pl.multiple_of(rows_of(step) + d * SEGMENT, SEGMENT), SEGMENT)
        return chunk_copy(rows, cols, (up, down)[d], sent.at[0], hop_recv.at[step])

    def core_copy(step, which):
        cols = feature_cols(at(y, (0, 3, 1, 2)[which]), core)
        sem = (last_recv if which == 3 else core_recv).at[step]
        return chunk_copy(pl.ds(rows_of(step), TILE), cols, partner, sent.at[0], sem)

    def halo_copy(step):
        return pltpu.make_async_remote_copy(
            src_ref=kv.at[pl.ds(pl.multiple_of(LENGTH + step * TILE, TILE), TILE), :],
            dst_ref=kv.at[pl.ds(pl.multiple_of(step * TILE, TILE), TILE), :],
            send_sem=sent.at[0],
            recv_sem=halo_recv.at[0],
            device_id=at_sp(1),
            device_id_type=MESH,
        )

    def back_start(half):
        rows = slice(half * TILE, (half + 1) * TILE)
        back_send[rows] = dkv[rows, :].astype(BF16)
        pltpu.make_async_remote_copy(
            src_ref=back_send.at[rows],
            dst_ref=back_recv.at[rows],
            send_sem=sent.at[0],
            recv_sem=halo_recv.at[1],
            device_id=at_sp(15),
            device_id_type=MESH,
        ).start()

    edge = jnp.where(sp == 0, REACH, 0)
    row = lax.broadcasted_iota(jnp.int32, (SPAN, TILE), 0)

    def ranges(tile):
        start = tile * TILE if isinstance(tile, int) else pl.multiple_of(tile * TILE, TILE)
        return start, pl.ds(start, SPAN), pl.ds(start, TILE)

    head_cols = [slice(h * HEAD, (h + 1) * HEAD) for h in range(HEADS)]
    value_cols = [slice(COLS + h * HEAD, COLS + (h + 1) * HEAD) for h in range(HEADS)]

    def attend_products(tile):
        _, keys_at, here = ranges(tile)
        return [
            (dot(kv[keys_at, head_cols[h]], query[here, head_cols[h]], 1, 1), dot(kv[keys_at, value_cols[h]], upstream[here, head_cols[h]], 1, 1))
            for h in range(HEADS)
        ]

    def attend_weights(tile, products):
        start, _, _ = ranges(tile)
        lows = []
        for h in range(HEADS):
            raw, prob_grad = products[h]
            scores = raw * (FACTOR * LOG2_E) + bias[h]
            if not isinstance(tile, int):
                scores = jnp.where(row + start < edge, -jnp.inf, scores)
            raised = jnp.exp2(scores - jnp.max(scores, axis=0, keepdims=True))
            weights = raised * (1.0 / jnp.sum(raised, axis=0, keepdims=True))
            delta = jnp.sum(weights * prob_grad, axis=0, keepdims=True)
            score_grad = weights * (prob_grad - delta)
            dsum[h] = dsum[h] + score_grad
            lows.append((weights.astype(BF16), score_grad.astype(BF16)))
        return lows

    def attend_queries(tile, lows):
        _, keys_at, here = ranges(tile)
        for h in range(HEADS):
            grads_t[head_cols[h], here] = (dot(keys_t[head_cols[h], keys_at], lows[h][1]) * FACTOR).astype(BF16)

    def attend_keys(tile, lows):
        _, keys_at, here = ranges(tile)
        for h in range(HEADS):
            weights_low, score_low = lows[h]
            dkv[keys_at, value_cols[h]] = dkv[keys_at, value_cols[h]] + dot(weights_low, upstream[here, head_cols[h]])
            dkv[keys_at, head_cols[h]] = dkv[keys_at, head_cols[h]] + dot(score_low, query[here, head_cols[h]])

    def attend(tile):
        lows = attend_weights(tile, attend_products(tile))
        attend_queries(tile, lows)
        attend_keys(tile, lows)

    for step in range(2):
        own_loads[step].wait()
        gather_start(step)
        core_copy(step, 0).start()
    own_loads[2].wait()

    table_load = pltpu.make_async_copy(position_bias, table, load_sem.at[5])
    table_load.start()
    loads = []
    for number, ref in enumerate((wq, wk, wv)):
        loads.append(pltpu.make_async_copy(ref, weight.at[:, number * COLS : (number + 1) * COLS], load_sem.at[3]))
    loads.append(pltpu.make_async_copy(out_grad, upstream, load_sem.at[4]))
    for load in loads:
        load.start()

    lane = lax.broadcasted_iota(jnp.int32, (8, ROUND), 1)
    column = lax.broadcasted_iota(jnp.int32, (SPAN, TILE), 1)
    low = jnp.where(column >= SEGMENT, SEGMENT, 0)
    seen = (row >= low) & (row < low + REACH + SEGMENT)
    table_load.wait()
    for h in range(HEADS):
        entries = jnp.broadcast_to(table[h : h + 1, :], (8, TABLE))
        padded = jnp.concatenate([entries, jnp.zeros((8, ROUND - TABLE), F32)], axis=1)
        turned = pltpu.roll(padded, ROUND - TABLE + 1, 1)
        last = jnp.broadcast_to(table[h : h + 1, TABLE - 1 : TABLE], (8, ROUND))
        turned = jnp.where(lane < TILE, last, turned)
        skewed = pltpu.roll(jnp.broadcast_to(turned[0:1, :], (SPAN, ROUND)), 0, 1, stride=1, stride_axis=0)
        bias[h] = jnp.where(seen, skewed[:, :TILE] * LOG2_E, -jnp.inf)
        dsum[h] = jnp.zeros((SPAN, TILE), F32)
    dkv[...] = jnp.zeros(dkv.shape, F32)

    await_bytes(weight, load_sem.at[3])
    loads[3].wait()

    def project_from(step, blocks):
        total = None
        for which in blocks:
            for on in (core, 1 - core):
                cols = feature_cols(at(y, (0, 3, 1, 2)[which]), on)
                part = dot(whole[pl.ds(rows_of(step), TILE), cols], weight[cols, :])
                total = part if total is None else total + part
        return total

    def hop_landed(step):
        with jax.named_scope("hop_wait"):
            await_bytes(whole.at[0:TILE, 0:FEATURES], hop_recv.at[step])
            core_copy(step, 3).start()

    def project_most(step):
        with jax.named_scope("core_wait"):
            await_bytes(whole.at[0:TILE, 0 : 3 * FEATURES], core_recv.at[step])
        with jax.named_scope("project"):
            projected[lax.rem(step, 2)] = project_from(step, (0, 1, 2))

    def gather_step(s, carry):
        @pl.when(s < CHUNKS)
        def _():
            with jax.named_scope("pass_wait"):
                await_bytes(whole.at[0:TILE, 0:FEATURES], pass_recv.at[s])
                for d in range(2):
                    hop_copy(s, d).start()

        @pl.when(s < CHUNKS - 2)
        def _():
            gather_start(s + 2)
            core_copy(s + 2, 0).start()

        @pl.when((s >= 1) & (s < CHUNKS))
        def _():
            project_most(s - 1)

        @pl.when(s < CHUNKS)
        def _():
            with jax.named_scope("gather_wait"):
                await_bytes(whole.at[0:TILE, 0:FEATURES], gather_recv.at[s])
                for d in range(2):
                    core_copy(s, 1 + d).start()

        @pl.when(s >= 1)
        def _():
            hop_landed(s - 1)

        @pl.when(s == CHUNKS - 1)
        def _():
            project_most(s)

        @pl.when(s == 4)
        def _():
            with jax.named_scope("halo_wait"):
                await_bytes(kv.at[0:REACH, :], halo_recv.at[0])
                keys_t[:, 0:REACH] = kv[0:REACH, :COLS].T

        @pl.when((s == 4) | (s == 6))
        def _():
            with jax.named_scope("attend"):
                attend(jnp.where(s == 4, 0, 2))

            @pl.when(s == 4)
            def _():
                back_start(0)

        @pl.when(s >= 1)
        def _():
            with jax.named_scope("last_wait"):
                await_bytes(whole.at[0:TILE, 0:FEATURES], last_recv.at[s - 1])
            with jax.named_scope("project_rest"):
                start = rows_of(s - 1)
                low = (projected[lax.rem(s - 1, 2)] + project_from(s - 1, (3,))).astype(BF16)
                query[pl.ds(start, TILE), :] = low[:, :COLS]
                kv[pl.ds(pl.multiple_of(start + REACH, TILE), TILE), :] = low[:, COLS:]
                keys_t[:, pl.ds(pl.multiple_of(start + REACH, TILE), TILE)] = low[:, COLS : 2 * COLS].T

        @pl.when((s >= 1) & (s <= 2))
        def _():
            halo_copy(s - 1).start()

        @pl.when(s == 4)
        def _():
            with jax.named_scope("attend"):
                attend(s - 3)
            back_start(1)

        return carry

    lax.fori_loop(0, CHUNKS + 1, gather_step, 0)
    with jax.named_scope("attend_last"):
        products = {tile: attend_products(tile) for tile in (3, 4)}
        lows = {3: attend_weights(3, products[3])}
        products[5] = attend_products(5)
        attend_queries(3, lows[3])
        for tile in (4, 5):
            lows[tile] = attend_weights(tile, products[tile])
            attend_queries(tile, lows[tile])

    def first_ring(p, side):
        me = (x, z)[side]
        part = (part_a, part_b)[side]
        at_side = (at_x, at_z)[side]
        return Ring(
            me, at_side(1), at_side(3),
            lambda k, half: part.at[p, k, pl.ds(2 * half, 2)],
            lambda d: far_ab.at[p, side, d],
            lambda d: near_join.at[p, 0, side, d],
            lambda d: near_join.at[p, 1, side, d],
            sent.at[0], ring_rs.at[p, 0], ring_rs.at[p, 1],
        )

    def second_ring(p, side):
        me = (z, x)[side]
        at_side = (at_z, at_x)[side]
        return Ring(
            me, at_side(1), at_side(3),
            lambda k, half: second_ab.at[p, side, k, half * SEGMENT : (half + 1) * SEGMENT],
            lambda d: far2_ab.at[p, side, d],
            lambda d: near_join2.at[p, 0, side, d],
            lambda d: near_join2.at[p, 1, side, d],
            sent.at[0], second_rs.at[p, 0], second_rs.at[p, 1],
        )

    y_ring = Ring(
        y, up, down,
        lambda k, half: term_own.at[k, half * (LENGTH // 2) : (half + 1) * (LENGTH // 2)],
        lambda d: far_y.at[d],
        lambda d: near_join_y.at[0, d],
        lambda d: near_join_y.at[1, d],
        sent.at[0], y_rs.at[0], y_rs.at[1],
    )

    halves = (slice(0, LENGTH // 2), slice(LENGTH // 2, LENGTH))

    def term(y_index, core_index, rows):
        start = pl.multiple_of((y_index * 2 + core_index) * FEATURES, FEATURES)
        return dot(grads[rows, :], weight[pl.ds(start, FEATURES), :], 1, 1)

    def send_term(k, rows, sem):
        with jax.named_scope("term_send"):
            term_send[k, rows] = term(at(y, AHEAD[k]), 1 - core, rows).astype(BF16)
        pltpu.make_async_remote_copy(
            src_ref=term_send.at[k, rows],
            dst_ref=term_recv.at[k, rows],
            send_sem=sent.at[0],
            recv_sem=term_rs.at[sem],
            device_id=partner,
            device_id_type=MESH,
        ).start()

    def own_term(k, rows, sem):
        with jax.named_scope("term_own"):
            y_index = at(y, AHEAD[k])
            made = term(y_index, core, rows)
            await_bytes(term_recv.at[k, rows], term_rs.at[sem])
            term_own[y_index, rows] = (made + term_recv[k, rows].astype(F32)).astype(BF16)

    def bias_send(buffer, me, targets, which):
        view = buffer.at[me]
        for target in targets:
            pltpu.make_async_remote_copy(
                src_ref=view, dst_ref=view, send_sem=sent.at[0], recv_sem=bias_rs.at[which], device_id=target, device_id_type=MESH
            ).start()

    def bias_sums():
        bias_x[x] = jnp.zeros((8, TILE), F32)
        for h in range(HEADS):
            wide = jnp.concatenate([dsum[h], jnp.zeros((SPAN, ROUND - TILE), F32)], axis=1)
            rows = SPAN
            while rows > 24:
                rows //= 2
                wide = wide[:rows] + pltpu.roll(wide[rows:], ROUND - rows, 1)
            wide = wide[0:8] + pltpu.roll(wide[8:16], ROUND - 8, 1) + pltpu.roll(wide[16:24], ROUND - 16, 1)
            sums = wide[0:1]
            for r in range(1, 8):
                sums = sums + pltpu.roll(wide[r : r + 1], ROUND - r, 1)
            first = lax.broadcasted_iota(jnp.int32, (1, ROUND), 1)
            clipped = jnp.sum(jnp.where(first < TILE, sums, 0.0), axis=1, keepdims=True)
            placed = pltpu.roll(sums, TABLE - 1, 1)
            sums = jnp.where(first == TABLE - 1, clipped, placed)
            for piece in range(3):
                bias_x[x, 3 * h + piece : 3 * h + piece + 1, :] = sums[:, piece * TILE : (piece + 1) * TILE]

    def finish():
        with jax.named_scope("back_wait"):
            await_bytes(back_recv, halo_recv.at[1])
            dkv[LENGTH:, :] = dkv[LENGTH:, :] + back_recv[...].astype(F32)

        def finish_chunk(chunk, carry):
            start = pl.multiple_of(chunk * TILE, TILE)
            grads[pl.ds(start, TILE), :COLS] = grads_t[:COLS, pl.ds(start, TILE)].T
            total = dkv[pl.ds(pl.multiple_of(start + REACH, TILE), TILE), :]
            total = jnp.concatenate([total[:, :COLS] * FACTOR, total[:, COLS:]], axis=1)
            grads[pl.ds(start, TILE), COLS:] = total.astype(BF16)
            grads_t[COLS:, pl.ds(start, TILE)] = total.T.astype(BF16)
            return carry

        with jax.named_scope("finish"):
            lax.fori_loop(0, CHUNKS, finish_chunk, 0, unroll=True)

    def weight_row(k, z_index):
        features = pl.ds(pl.multiple_of(z_index * RING * COLS, RING * COLS), RING * COLS)
        made = dot(grads_t[k * COLS : (k + 1) * COLS, :], whole[:, features]).astype(BF16)
        for x_index in range(RING):
            cut = slice(x_index * COLS, (x_index + 1) * COLS)
            part_b[k, z_index, x_index] = made[HEAD:, cut]
            part_a[k, jnp.where(x_index == at(x, 2), RING, x_index), z_index] = made[:HEAD, cut]

    def weight_far(k):
        far_x = at(x, 2)
        with jax.named_scope("weight_far"):
            for z_index in range(RING):
                features = pl.ds(pl.multiple_of(z_index * RING * COLS + far_x * COLS, COLS), COLS)
                left = grads_t[k * COLS : k * COLS + HEAD, :]
                part_a[k, far_x, z_index] = dot(left, whole[:, features]).astype(BF16)
            first_ring(k, 0).start_far()
            weight_row(k, at(z, 2))
            first_ring(k, 1).start_far()

    def weight_rest(k):
        def rows(i, inner):
            weight_row(k, at(z, i))
            return inner

        with jax.named_scope("weight_rest"):
            lax.fori_loop(3, RING + 2, rows, 0, unroll=True)
        for side in range(2):
            for d in range(2):
                first_ring(k, side).start_near(d)

    def first_join(p):
        with jax.named_scope("join_first"):
            await_bytes(far_ab.at[p], ring_rs.at[p, 0])
            for side in range(2):
                first_ring(p, side).join()

    whole_rows = slice(0, LENGTH)
    weight_far(0)
    with jax.named_scope("attend_keys"):
        for tile in (3, 4, 5):
            attend_keys(tile, lows[tile])
    weight_rest(0)
    finish()
    for half in range(2):
        send_term(0, halves[half], half)
    weight_far(1)
    for half in range(2):
        own_term(0, halves[half], half)
        y_ring.start(0, half)
    weight_rest(1)
    first_join(0)
    send_term(1, whole_rows, 2)
    with jax.named_scope("bias_sums"):
        bias_sums()
    bias_send(bias_x, x, [at_x(by) for by in (1, 2, 3)], 0)
    weight_far(2)
    send_term(2, whole_rows, 3)
    send_term(3, whole_rows, 4)
    own_term(1, whole_rows, 2)
    y_ring.start_near(0)
    own_term(2, whole_rows, 3)
    y_ring.start_near(1)
    weight_rest(2)
    first_join(1)
    with jax.named_scope("join_y"):
        await_bytes(far_y, y_rs.at[0])
        y_ring.join()
    with jax.named_scope("bias_x"):
        await_bytes(bias_x.at[0:3], bias_rs.at[0])
        bias_z[z] = (bias_x[0] + bias_x[1]) + (bias_x[2] + bias_x[3])
    bias_send(bias_z, z, [at_z(by) for by in (1, 2, 3)], 1)
    own_term(3, whole_rows, 4)

    def second_start(p):
        with jax.named_scope(f"second_start_{p}"):
            await_bytes(near_join.at[p], ring_rs.at[p, 1])
            for side in range(2):
                ring = first_ring(p, side)
                for half in range(2):
                    second_ab[p, side, 2 * half : 2 * half + 2] = ring.half(half).astype(BF16)
            rings = [second_ring(p, side) for side in range(2)]
            if p in STRAIGHT:
                rings[0].start_straight(at_z(2))
                rings[1].start_straight(at_x(2))
                return
            for ring in rings:
                ring.start_far()
            for ring in rings:
                for d in range(2):
                    ring.start_near(d)

    def second_join(p):
        with jax.named_scope(f"second_join_{p}"):
            await_bytes(far2_ab.at[p], second_rs.at[p, 0])
            for side in range(2):
                second_ring(p, side).join()

    def second_finish(p):
        with jax.named_scope(f"second_finish_{p}"):
            await_bytes(near_join2.at[p], second_rs.at[p, 1])
            if p in STRAIGHT:
                await_bytes(far2_ab.at[p], second_rs.at[p, 0])
            for side in range(2):
                ring = second_ring(p, side)
                sums = [ring.half(half) for half in range(2)]
                if p in STRAIGHT:
                    sums = [sums[half] + far2_ab[p, side, half].astype(F32) for half in range(2)]
                total = jnp.concatenate(sums, axis=0)
                (wq_out, wk_out, wv_out)[p][:, side * HEAD : (side + 1) * HEAD] = total.T

    first_join(2)
    second_start(0)
    second_start(1)
    second_join(0)
    second_start(2)
    second_join(1)
    second_finish(0)
    with jax.named_scope("bias_z"):
        await_bytes(bias_z.at[0:3], bias_rs.at[1])
        sums = (bias_z[0] + bias_z[1]) + (bias_z[2] + bias_z[3])
        for h in range(HEADS):
            for piece in range(3):
                cut = slice(piece * TILE, min((piece + 1) * TILE, TABLE))
                bias_out[h : h + 1, cut] = sums[3 * h + piece : 3 * h + piece + 1, : cut.stop - cut.start]
    with jax.named_scope("input_sum"):
        await_bytes(near_join_y, y_rs.at[1])
        for d in range(2):
            input_out[d * (LENGTH // 2) : (d + 1) * (LENGTH // 2), :] = y_ring.half(d).astype(BF16)
    second_finish(1)
    second_finish(2)

    with jax.named_scope("drain"):
        await_bytes(whole.at[:, 0 : 2 * FEATURES], sent.at[0])
        await_bytes(whole.at[:, 0:FEATURES], sent.at[0])
        await_bytes(whole.at[:, 0 : 4 * FEATURES], sent.at[0])
        await_bytes(kv.at[0:REACH, :], sent.at[0])
        await_bytes(back_send, sent.at[0])
        await_bytes(far_ab, sent.at[0])
        await_bytes(near_join, sent.at[0])
        await_bytes(far2_ab, sent.at[0])
        await_bytes(near_join2, sent.at[0])
        await_bytes(far_y, sent.at[0])
        await_bytes(near_join_y, sent.at[0])
        await_bytes(term_recv, sent.at[0])
        await_bytes(bias_x.at[0:3], sent.at[0])
        await_bytes(bias_z.at[0:3], sent.at[0])


def store_results(*refs):
    sources, targets, sems = refs[:5], refs[5:10], refs[10]
    copies = [pltpu.make_async_copy(source, target, sems.at[n]) for n, (source, target) in enumerate(zip(sources, targets))]
    for copy in copies:
        copy.start()
    for copy in copies:
        copy.wait()


def shards(tokens, query_weight, key_weight, value_weight, position_bias, out_grad):
    anywhere = pl.BlockSpec(memory_space=pl.ANY)
    near = pl.BlockSpec(memory_space=pltpu.VMEM)
    dma = pltpu.SemaphoreType.DMA
    vmem = pltpu.VMEM
    grad = vmem((COLS, COLS), F32)
    results = pl.pallas_call(
        kernel,
        name="segment_attention_grads",
        out_shape=(
            vmem((LENGTH, FEATURES), BF16), grad, grad, grad,
            vmem((HEADS, TABLE), F32),
        ),
        in_specs=[anywhere] * 6,
        out_specs=(near,) * 5,
        scratch_shapes=[
            vmem((HEADS, TABLE), F32),
            vmem((LENGTH, WIDTH), BF16),
            vmem((WIDTH, 3 * COLS), BF16),
            vmem((2, TILE, 3 * COLS), F32),
            vmem((LENGTH, COLS), BF16),
            vmem((REACH + LENGTH, 2 * COLS), BF16),
            vmem((LENGTH, COLS), BF16),
            vmem((COLS, REACH + LENGTH), BF16),
            vmem((REACH + LENGTH, 2 * COLS), F32),
            vmem((LENGTH, 3 * COLS), BF16),
            vmem((3 * COLS, LENGTH), BF16),
            vmem((REACH, 2 * COLS), BF16),
            vmem((REACH, 2 * COLS), BF16),
            vmem((3, RING + 1, RING, HEAD, COLS), BF16),
            vmem((3, RING, RING, HEAD, COLS), BF16),
            vmem((3, 2, 2, 2, HEAD, COLS), BF16),
            vmem((3, 2, 2, 2, 2, HEAD, COLS), BF16),
            vmem((3, 2, RING, HEAD, COLS), BF16),
            vmem((3, 2, 2, SEGMENT, COLS), BF16),
            vmem((3, 2, 2, 2, SEGMENT, COLS), BF16),
            vmem((RING, LENGTH, FEATURES), BF16),
            vmem((RING, LENGTH, FEATURES), BF16),
            vmem((RING, LENGTH, FEATURES), BF16),
            vmem((2, LENGTH // 2, FEATURES), BF16),
            vmem((2, 2, LENGTH // 2, FEATURES), BF16),
            vmem((HEADS, SPAN, TILE), F32),
            vmem((HEADS, SPAN, TILE), F32),
            vmem((RING, 8, TILE), F32),
            vmem((RING, 8, TILE), F32),
            dma((6,)),
            dma((CHUNKS,)), dma((CHUNKS,)), dma((CHUNKS,)), dma((CHUNKS,)), dma((CHUNKS,)),
            dma((3,)),
            dma((RING + 1,)),
            dma((3, 2)), dma((3, 2)), dma((2,)),
            dma((2,)),
            dma((1,)),
        ],
        compiler_params=pltpu.CompilerParams(
            collective_id=0, has_side_effects=True, vmem_limit_bytes=62_000_000
        ),
    )(tokens, query_weight, key_weight, value_weight, position_bias, out_grad)
    return pl.pallas_call(
        store_results,
        name="store_results",
        out_shape=tuple(jax.ShapeDtypeStruct(result.shape, result.dtype) for result in results),
        in_specs=[near] * 5,
        out_specs=(anywhere,) * 5,
        scratch_shapes=[dma((5,))],
        compiler_params=pltpu.CompilerParams(vmem_limit_bytes=1_000_000),
    )(*results)


def solution(mesh):
    return jax.shard_map(
        shards,
        mesh=mesh,
        in_specs=(P("sp", "tp"), P(None, "tp"), P(None, "tp"), P(None, "tp"), P("tp", None), P("sp", "tp")),
        out_specs=(P("sp", "tp"), P("sp", "tp"), P("sp", "tp"), P("sp", "tp"), P("tp", None)),
        check_vma=False,
    )
```

```python
import functools

import jax
import jax.numpy as jnp
from jax import lax
from jax.experimental import pallas as pl
from jax.experimental.pallas import tpu as pltpu
from jax.sharding import PartitionSpec as P

MESH = pl.DeviceIdType.MESH
BF16, F32 = jnp.bfloat16, jnp.float32
SEGMENT, REACH, CLIP, HEAD = 64, 256, 256, 128
TILE = 128
SPAN = REACH + TILE
LENGTH, WIDTH, FEATURES = 768, 4096, 512
CHUNKS = LENGTH // TILE
HEADS = 2
COLS = HEADS * HEAD
FACTOR = HEAD ** (-0.5)
RING = 4
LOG2_E = 1.4426950408889634
TABLE = 320
ROUND = 512
AHEAD = (2, 1, 3, 0)
STRAIGHT = (2,)


def dot(left, right, left_dim=1, right_dim=0):
    return lax.dot_general(left, right, (((left_dim,), (right_dim,)), ((), ())), preferred_element_type=F32)


class Ring:
    def __init__(self, me, up, down, block, via, direct, joined, sent, far_sem, rest_sem):
        self.near = (lax.rem(me + 1, RING), lax.rem(me + RING - 1, RING))
        self.far = lax.rem(me + 2, RING)
        self.me, self.devices, self.block = me, (up, down), block
        self.landing = (via, direct, joined)
        self.sent, self.arrived = sent, (far_sem, rest_sem, rest_sem)

    def start(self, kind, d):
        source = (self.block(self.far, d), self.block(self.near[d], 1 - d), self.block(self.near[d], d))[kind]
        pltpu.make_async_remote_copy(
            src_ref=source,
            dst_ref=self.landing[kind](d),
            send_sem=self.sent,
            recv_sem=self.arrived[kind],
            device_id=self.devices[d],
            device_id_type=MESH,
        ).start()

    def start_straight(self, opposite):
        for d in range(2):
            pltpu.make_async_remote_copy(
                src_ref=self.block(self.far, d),
                dst_ref=self.landing[0](d),
                send_sem=self.sent,
                recv_sem=self.arrived[0],
                device_id=opposite,
                device_id_type=MESH,
            ).start()
        for kind in (1, 2):
            for d in range(2):
                self.start(kind, d)

    def start_far(self):
        for d in range(2):
            self.start(0, d)

    def start_near(self, d):
        self.start(1, d)

    def join(self):
        for d in range(2):
            ref = self.block(self.near[d], d)
            ref[...] = (ref[...].astype(F32) + self.landing[0](d)[...].astype(F32)).astype(BF16)
            self.start(2, d)

    def half(self, d):
        total = self.block(self.me, d)[...].astype(F32) + self.landing[2](d)[...].astype(F32)
        return total + self.landing[1](1 - d)[...].astype(F32)


def await_bytes(view, sem):
    pltpu.make_async_copy(view, view, sem).wait()


def kernel(
    tokens, wq, wk, wv, position_bias, out_grad,
    input_out, wq_out, wk_out, wv_out, bias_out,
    table, whole, weight, projected, query, kv, upstream, keys_t, dkv, grads, grads_t, back_send, back_recv,
    part_a, part_b, far_ab, near_join, second_ab, far2_ab, near_join2,
    term_own, term_send, term_recv, far_y, near_join_y,
    bias, dsum, bias_x, bias_z,
    load_sem, pass_recv, gather_recv, hop_recv, core_recv, last_recv, halo_recv, term_rs, ring_rs, second_rs, y_rs, bias_rs, sent,
):
    sp, tp = lax.axis_index("sp"), lax.axis_index("tp")
    z, x = sp // RING, lax.rem(sp, RING)
    y, core = tp // 2, lax.rem(tp, 2)

    def at(value, by):
        return lax.rem(value + by, RING)

    def at_x(by):
        return (z * RING + at(x, by), tp)

    def at_z(by):
        return (at(z, by) * RING + x, tp)

    def at_y(by):
        return (sp, at(y, by) * 2 + core)

    def at_sp(by):
        return (lax.rem(sp + by, 16), tp)

    partner = (sp, y * 2 + 1 - core)

    barrier = pltpu.get_barrier_semaphore()
    peers = [partner, at_sp(1), at_sp(15)]
    for by in (1, 3):
        peers.append(at_y(by))
    for by in (1, 2, 3):
        peers += [at_x(by), at_z(by)]
    for peer in peers:
        pl.semaphore_signal(barrier, inc=1, device_id=peer, device_id_type=MESH)

    def feature_cols(y_index, core_index):
        return pl.ds(pl.multiple_of((y_index * 2 + core_index) * FEATURES, FEATURES), FEATURES)

    my_cols = feature_cols(y, core)
    own_loads = []
    for number, (first, last) in enumerate(((4 * TILE, 5 * TILE), (5 * TILE, 6 * TILE), (0, 4 * TILE))):
        own = pltpu.make_async_copy(tokens.at[first:last, :], whole.at[first:last, my_cols], load_sem.at[number])
        own.start()
        own_loads.append(own)
    with jax.named_scope("entry"):
        pl.semaphore_wait(barrier, len(peers))

    def rows_of(step):
        return pl.multiple_of(lax.rem(step + 4, CHUNKS) * TILE, TILE)

    def chunk_copy(rows, cols, target, send, recv):
        view = whole.at[rows, cols]
        return pltpu.make_async_remote_copy(
            src_ref=view, dst_ref=view, send_sem=send, recv_sem=recv, device_id=target, device_id_type=MESH
        )

    up, down = at_y(1), at_y(3)

    def gather_start(step):
        for half in range(2):
            for d in range(2):
                first = pl.multiple_of(rows_of(step) + (half ^ d) * SEGMENT, SEGMENT)
                sem = (pass_recv, gather_recv)[half].at[step]
                chunk_copy(pl.ds(first, SEGMENT), my_cols, (up, down)[d], sent.at[0], sem).start()

    def hop_copy(step, d):
        cols = feature_cols(at(y, (3, 1)[d]), core)
        rows = pl.ds(pl.multiple_of(rows_of(step) + d * SEGMENT, SEGMENT), SEGMENT)
        return chunk_copy(rows, cols, (up, down)[d], sent.at[0], hop_recv.at[step])

    def core_copy(step, which):
        cols = feature_cols(at(y, (0, 3, 1, 2)[which]), core)
        sem = (last_recv if which == 3 else core_recv).at[step]
        return chunk_copy(pl.ds(rows_of(step), TILE), cols, partner, sent.at[0], sem)

    def halo_copy(step):
        return pltpu.make_async_remote_copy(
            src_ref=kv.at[pl.ds(pl.multiple_of(LENGTH + step * TILE, TILE), TILE), :],
            dst_ref=kv.at[pl.ds(pl.multiple_of(step * TILE, TILE), TILE), :],
            send_sem=sent.at[0],
            recv_sem=halo_recv.at[0],
            device_id=at_sp(1),
            device_id_type=MESH,
        )

    def back_start(half):
        rows = slice(half * TILE, (half + 1) * TILE)
        back_send[rows] = dkv[rows, :].astype(BF16)
        pltpu.make_async_remote_copy(
            src_ref=back_send.at[rows],
            dst_ref=back_recv.at[rows],
            send_sem=sent.at[0],
            recv_sem=halo_recv.at[1],
            device_id=at_sp(15),
            device_id_type=MESH,
        ).start()

    edge = jnp.where(sp == 0, REACH, 0)
    row = lax.broadcasted_iota(jnp.int32, (SPAN, TILE), 0)

    def ranges(tile):
        start = tile * TILE if isinstance(tile, int) else pl.multiple_of(tile * TILE, TILE)
        return start, pl.ds(start, SPAN), pl.ds(start, TILE)

    head_cols = [slice(h * HEAD, (h + 1) * HEAD) for h in range(HEADS)]
    value_cols = [slice(COLS + h * HEAD, COLS + (h + 1) * HEAD) for h in range(HEADS)]

    def attend_products(tile):
        _, keys_at, here = ranges(tile)
        return [
            (dot(kv[keys_at, head_cols[h]], query[here, head_cols[h]], 1, 1), dot(kv[keys_at, value_cols[h]], upstream[here, head_cols[h]], 1, 1))
            for h in range(HEADS)
        ]

    def attend_weights(tile, products):
        start, _, _ = ranges(tile)
        lows = []
        for h in range(HEADS):
            raw, prob_grad = products[h]
            scores = raw * (FACTOR * LOG2_E) + bias[h]
            if not isinstance(tile, int):
                scores = jnp.where(row + start < edge, -jnp.inf, scores)
            raised = jnp.exp2(scores - jnp.max(scores, axis=0, keepdims=True))
            weights = raised * (1.0 / jnp.sum(raised, axis=0, keepdims=True))
            delta = jnp.sum(weights * prob_grad, axis=0, keepdims=True)
            score_grad = weights * (prob_grad - delta)
            dsum[h] = dsum[h] + score_grad
            lows.append((weights.astype(BF16), score_grad.astype(BF16)))
        return lows

    def attend_queries(tile, lows):
        _, keys_at, here = ranges(tile)
        for h in range(HEADS):
            grads_t[head_cols[h], here] = (dot(keys_t[head_cols[h], keys_at], lows[h][1]) * FACTOR).astype(BF16)

    def attend_keys(tile, lows):
        _, keys_at, here = ranges(tile)
        for h in range(HEADS):
            weights_low, score_low = lows[h]
            dkv[keys_at, value_cols[h]] = dkv[keys_at, value_cols[h]] + dot(weights_low, upstream[here, head_cols[h]])
            dkv[keys_at, head_cols[h]] = dkv[keys_at, head_cols[h]] + dot(score_low, query[here, head_cols[h]])

    def attend(tile):
        lows = attend_weights(tile, attend_products(tile))
        attend_queries(tile, lows)
        attend_keys(tile, lows)

    for step in range(2):
        own_loads[step].wait()
        gather_start(step)
        core_copy(step, 0).start()
    own_loads[2].wait()

    table_load = pltpu.make_async_copy(position_bias, table, load_sem.at[5])
    table_load.start()
    loads = []
    for number, ref in enumerate((wq, wk, wv)):
        loads.append(pltpu.make_async_copy(ref, weight.at[:, number * COLS : (number + 1) * COLS], load_sem.at[3]))
    loads.append(pltpu.make_async_copy(out_grad, upstream, load_sem.at[4]))
    for load in loads:
        load.start()

    lane = lax.broadcasted_iota(jnp.int32, (8, ROUND), 1)
    column = lax.broadcasted_iota(jnp.int32, (SPAN, TILE), 1)
    low = jnp.where(column >= SEGMENT, SEGMENT, 0)
    seen = (row >= low) & (row < low + REACH + SEGMENT)
    table_load.wait()
    for h in range(HEADS):
        entries = jnp.broadcast_to(table[h : h + 1, :], (8, TABLE))
        padded = jnp.concatenate([entries, jnp.zeros((8, ROUND - TABLE), F32)], axis=1)
        turned = pltpu.roll(padded, ROUND - TABLE + 1, 1)
        last = jnp.broadcast_to(table[h : h + 1, TABLE - 1 : TABLE], (8, ROUND))
        turned = jnp.where(lane < TILE, last, turned)
        skewed = pltpu.roll(jnp.broadcast_to(turned[0:1, :], (SPAN, ROUND)), 0, 1, stride=1, stride_axis=0)
        bias[h] = jnp.where(seen, skewed[:, :TILE] * LOG2_E, -jnp.inf)
        dsum[h] = jnp.zeros((SPAN, TILE), F32)
    dkv[...] = jnp.zeros(dkv.shape, F32)

    await_bytes(weight, load_sem.at[3])
    loads[3].wait()

    def project_from(step, blocks):
        total = None
        for which in blocks:
            for on in (core, 1 - core):
                cols = feature_cols(at(y, (0, 3, 1, 2)[which]), on)
                part = dot(whole[pl.ds(rows_of(step), TILE), cols], weight[cols, :])
                total = part if total is None else total + part
        return total

    def hop_landed(step):
        with jax.named_scope("hop_wait"):
            await_bytes(whole.at[0:TILE, 0:FEATURES], hop_recv.at[step])
            core_copy(step, 3).start()

    def project_most(step):
        with jax.named_scope("core_wait"):
            await_bytes(whole.at[0:TILE, 0 : 3 * FEATURES], core_recv.at[step])
        with jax.named_scope("project"):
            projected[lax.rem(step, 2)] = project_from(step, (0, 1, 2))

    def gather_step(s, carry):
        @pl.when(s < CHUNKS)
        def _():
            with jax.named_scope("pass_wait"):
                await_bytes(whole.at[0:TILE, 0:FEATURES], pass_recv.at[s])
                for d in range(2):
                    hop_copy(s, d).start()

        @pl.when(s < CHUNKS - 2)
        def _():
            gather_start(s + 2)
            core_copy(s + 2, 0).start()

        @pl.when((s >= 1) & (s < CHUNKS))
        def _():
            project_most(s - 1)

        @pl.when(s < CHUNKS)
        def _():
            with jax.named_scope("gather_wait"):
                await_bytes(whole.at[0:TILE, 0:FEATURES], gather_recv.at[s])
                for d in range(2):
                    core_copy(s, 1 + d).start()

        @pl.when(s >= 1)
        def _():
            hop_landed(s - 1)

        @pl.when(s == CHUNKS - 1)
        def _():
            project_most(s)

        @pl.when(s == 4)
        def _():
            with jax.named_scope("halo_wait"):
                await_bytes(kv.at[0:REACH, :], halo_recv.at[0])
                keys_t[:, 0:REACH] = kv[0:REACH, :COLS].T

        @pl.when((s == 4) | (s == 6))
        def _():
            with jax.named_scope("attend"):
                attend(jnp.where(s == 4, 0, 2))

            @pl.when(s == 4)
            def _():
                back_start(0)

        @pl.when(s >= 1)
        def _():
            with jax.named_scope("last_wait"):
                await_bytes(whole.at[0:TILE, 0:FEATURES], last_recv.at[s - 1])
            with jax.named_scope("project_rest"):
                start = rows_of(s - 1)
                low = (projected[lax.rem(s - 1, 2)] + project_from(s - 1, (3,))).astype(BF16)
                query[pl.ds(start, TILE), :] = low[:, :COLS]
                kv[pl.ds(pl.multiple_of(start + REACH, TILE), TILE), :] = low[:, COLS:]
                keys_t[:, pl.ds(pl.multiple_of(start + REACH, TILE), TILE)] = low[:, COLS : 2 * COLS].T

        @pl.when((s >= 1) & (s <= 2))
        def _():
            halo_copy(s - 1).start()

        @pl.when(s == 4)
        def _():
            with jax.named_scope("attend"):
                attend(s - 3)
            back_start(1)

        return carry

    lax.fori_loop(0, CHUNKS + 1, gather_step, 0)
    with jax.named_scope("attend_last"):
        products = {tile: attend_products(tile) for tile in (3, 4)}
        lows = {3: attend_weights(3, products[3])}
        products[5] = attend_products(5)
        attend_queries(3, lows[3])
        for tile in (4, 5):
            lows[tile] = attend_weights(tile, products[tile])
            attend_queries(tile, lows[tile])

    def first_ring(p, side):
        me = (x, z)[side]
        part = (part_a, part_b)[side]
        at_side = (at_x, at_z)[side]
        return Ring(
            me, at_side(1), at_side(3),
            lambda k, half: part.at[p, k, pl.ds(2 * half, 2)],
            lambda d: far_ab.at[p, side, d],
            lambda d: near_join.at[p, 0, side, d],
            lambda d: near_join.at[p, 1, side, d],
            sent.at[0], ring_rs.at[p, 0], ring_rs.at[p, 1],
        )

    def second_ring(p, side):
        me = (z, x)[side]
        at_side = (at_z, at_x)[side]
        return Ring(
            me, at_side(1), at_side(3),
            lambda k, half: second_ab.at[p, side, k, half * SEGMENT : (half + 1) * SEGMENT],
            lambda d: far2_ab.at[p, side, d],
            lambda d: near_join2.at[p, 0, side, d],
            lambda d: near_join2.at[p, 1, side, d],
            sent.at[0], second_rs.at[p, 0], second_rs.at[p, 1],
        )

    y_ring = Ring(
        y, up, down,
        lambda k, half: term_own.at[k, half * (LENGTH // 2) : (half + 1) * (LENGTH // 2)],
        lambda d: far_y.at[d],
        lambda d: near_join_y.at[0, d],
        lambda d: near_join_y.at[1, d],
        sent.at[0], y_rs.at[0], y_rs.at[1],
    )

    halves = (slice(0, LENGTH // 2), slice(LENGTH // 2, LENGTH))

    def term(y_index, core_index, rows):
        start = pl.multiple_of((y_index * 2 + core_index) * FEATURES, FEATURES)
        return dot(grads[rows, :], weight[pl.ds(start, FEATURES), :], 1, 1)

    def send_term(k, rows, sem):
        with jax.named_scope("term_send"):
            term_send[k, rows] = term(at(y, AHEAD[k]), 1 - core, rows).astype(BF16)
        pltpu.make_async_remote_copy(
            src_ref=term_send.at[k, rows],
            dst_ref=term_recv.at[k, rows],
            send_sem=sent.at[0],
            recv_sem=term_rs.at[sem],
            device_id=partner,
            device_id_type=MESH,
        ).start()

    def own_term(k, rows, sem):
        with jax.named_scope("term_own"):
            y_index = at(y, AHEAD[k])
            made = term(y_index, core, rows)
            await_bytes(term_recv.at[k, rows], term_rs.at[sem])
            term_own[y_index, rows] = (made + term_recv[k, rows].astype(F32)).astype(BF16)

    def bias_send(buffer, me, targets, which):
        view = buffer.at[me]
        for target in targets:
            pltpu.make_async_remote_copy(
                src_ref=view, dst_ref=view, send_sem=sent.at[0], recv_sem=bias_rs.at[which], device_id=target, device_id_type=MESH
            ).start()

    def bias_sums():
        bias_x[x] = jnp.zeros((8, TILE), F32)
        for h in range(HEADS):
            wide = jnp.concatenate([dsum[h], jnp.zeros((SPAN, ROUND - TILE), F32)], axis=1)
            rows = SPAN
            while rows > 24:
                rows //= 2
                wide = wide[:rows] + pltpu.roll(wide[rows:], ROUND - rows, 1)
            wide = wide[0:8] + pltpu.roll(wide[8:16], ROUND - 8, 1) + pltpu.roll(wide[16:24], ROUND - 16, 1)
            sums = wide[0:1]
            for r in range(1, 8):
                sums = sums + pltpu.roll(wide[r : r + 1], ROUND - r, 1)
            first = lax.broadcasted_iota(jnp.int32, (1, ROUND), 1)
            clipped = jnp.sum(jnp.where(first < TILE, sums, 0.0), axis=1, keepdims=True)
            placed = pltpu.roll(sums, TABLE - 1, 1)
            sums = jnp.where(first == TABLE - 1, clipped, placed)
            for piece in range(3):
                bias_x[x, 3 * h + piece : 3 * h + piece + 1, :] = sums[:, piece * TILE : (piece + 1) * TILE]

    def finish():
        with jax.named_scope("back_wait"):
            await_bytes(back_recv, halo_recv.at[1])
            dkv[LENGTH:, :] = dkv[LENGTH:, :] + back_recv[...].astype(F32)

        def finish_chunk(chunk, carry):
            start = pl.multiple_of(chunk * TILE, TILE)
            grads[pl.ds(start, TILE), :COLS] = grads_t[:COLS, pl.ds(start, TILE)].T
            total = dkv[pl.ds(pl.multiple_of(start + REACH, TILE), TILE), :]
            total = jnp.concatenate([total[:, :COLS] * FACTOR, total[:, COLS:]], axis=1)
            grads[pl.ds(start, TILE), COLS:] = total.astype(BF16)
            grads_t[COLS:, pl.ds(start, TILE)] = total.T.astype(BF16)
            return carry

        with jax.named_scope("finish"):
            lax.fori_loop(0, CHUNKS, finish_chunk, 0, unroll=True)

    def weight_row(k, z_index):
        features = pl.ds(pl.multiple_of(z_index * RING * COLS, RING * COLS), RING * COLS)
        made = dot(grads_t[k * COLS : (k + 1) * COLS, :], whole[:, features]).astype(BF16)
        for x_index in range(RING):
            cut = slice(x_index * COLS, (x_index + 1) * COLS)
            part_b[k, z_index, x_index] = made[HEAD:, cut]
            part_a[k, jnp.where(x_index == at(x, 2), RING, x_index), z_index] = made[:HEAD, cut]

    def weight_far(k):
        far_x = at(x, 2)
        with jax.named_scope("weight_far"):
            for z_index in range(RING):
                features = pl.ds(pl.multiple_of(z_index * RING * COLS + far_x * COLS, COLS), COLS)
                left = grads_t[k * COLS : k * COLS + HEAD, :]
                part_a[k, far_x, z_index] = dot(left, whole[:, features]).astype(BF16)
            first_ring(k, 0).start_far()
            weight_row(k, at(z, 2))
            first_ring(k, 1).start_far()

    def weight_rest(k):
        def rows(i, inner):
            weight_row(k, at(z, i))
            return inner

        with jax.named_scope("weight_rest"):
            lax.fori_loop(3, RING + 2, rows, 0, unroll=True)
        for side in range(2):
            for d in range(2):
                first_ring(k, side).start_near(d)

    def first_join(p):
        with jax.named_scope("join_first"):
            await_bytes(far_ab.at[p], ring_rs.at[p, 0])
            for side in range(2):
                first_ring(p, side).join()

    whole_rows = slice(0, LENGTH)
    weight_far(0)
    with jax.named_scope("attend_keys"):
        for tile in (3, 4, 5):
            attend_keys(tile, lows[tile])
    weight_rest(0)
    finish()
    for half in range(2):
        send_term(0, halves[half], half)
    weight_far(1)
    for half in range(2):
        own_term(0, halves[half], half)
        y_ring.start(0, half)
    weight_rest(1)
    first_join(0)
    send_term(1, whole_rows, 2)
    with jax.named_scope("bias_sums"):
        bias_sums()
    bias_send(bias_x, x, [at_x(by) for by in (1, 2, 3)], 0)
    weight_far(2)
    send_term(2, whole_rows, 3)
    send_term(3, whole_rows, 4)
    own_term(1, whole_rows, 2)
    y_ring.start_near(0)
    own_term(2, whole_rows, 3)
    y_ring.start_near(1)
    weight_rest(2)
    first_join(1)
    with jax.named_scope("join_y"):
        await_bytes(far_y, y_rs.at[0])
        y_ring.join()
    with jax.named_scope("bias_x"):
        await_bytes(bias_x.at[0:3], bias_rs.at[0])
        bias_z[z] = (bias_x[0] + bias_x[1]) + (bias_x[2] + bias_x[3])
    bias_send(bias_z, z, [at_z(by) for by in (1, 2, 3)], 1)
    own_term(3, whole_rows, 4)

    def second_start(p):
        with jax.named_scope(f"second_start_{p}"):
            await_bytes(near_join.at[p], ring_rs.at[p, 1])
            for side in range(2):
                ring = first_ring(p, side)
                for half in range(2):
                    second_ab[p, side, 2 * half : 2 * half + 2] = ring.half(half).astype(BF16)
            rings = [second_ring(p, side) for side in range(2)]
            if p in STRAIGHT:
                rings[0].start_straight(at_z(2))
                rings[1].start_straight(at_x(2))
                return
            for ring in rings:
                ring.start_far()
            for ring in rings:
                for d in range(2):
                    ring.start_near(d)

    def second_join(p):
        with jax.named_scope(f"second_join_{p}"):
            await_bytes(far2_ab.at[p], second_rs.at[p, 0])
            for side in range(2):
                second_ring(p, side).join()

    def second_finish(p):
        with jax.named_scope(f"second_finish_{p}"):
            await_bytes(near_join2.at[p], second_rs.at[p, 1])
            if p in STRAIGHT:
                await_bytes(far2_ab.at[p], second_rs.at[p, 0])
            for side in range(2):
                ring = second_ring(p, side)
                sums = [ring.half(half) for half in range(2)]
                if p in STRAIGHT:
                    sums = [sums[half] + far2_ab[p, side, half].astype(F32) for half in range(2)]
                total = jnp.concatenate(sums, axis=0)
                (wq_out, wk_out, wv_out)[p][:, side * HEAD : (side + 1) * HEAD] = total.T

    first_join(2)
    second_start(0)
    second_start(1)
    second_start(2)
    second_join(0)
    second_join(1)
    second_finish(0)
    with jax.named_scope("bias_z"):
        await_bytes(bias_z.at[0:3], bias_rs.at[1])
        sums = (bias_z[0] + bias_z[1]) + (bias_z[2] + bias_z[3])
        for h in range(HEADS):
            for piece in range(3):
                cut = slice(piece * TILE, min((piece + 1) * TILE, TABLE))
                bias_out[h : h + 1, cut] = sums[3 * h + piece : 3 * h + piece + 1, : cut.stop - cut.start]
    with jax.named_scope("input_sum"):
        await_bytes(near_join_y, y_rs.at[1])
        for d in range(2):
            input_out[d * (LENGTH // 2) : (d + 1) * (LENGTH // 2), :] = y_ring.half(d).astype(BF16)
    second_finish(1)
    second_finish(2)

    with jax.named_scope("drain"):
        await_bytes(whole.at[:, 0 : 2 * FEATURES], sent.at[0])
        await_bytes(whole.at[:, 0:FEATURES], sent.at[0])
        await_bytes(whole.at[:, 0 : 4 * FEATURES], sent.at[0])
        await_bytes(kv.at[0:REACH, :], sent.at[0])
        await_bytes(back_send, sent.at[0])
        await_bytes(far_ab, sent.at[0])
        await_bytes(near_join, sent.at[0])
        await_bytes(far2_ab, sent.at[0])
        await_bytes(near_join2, sent.at[0])
        await_bytes(far_y, sent.at[0])
        await_bytes(near_join_y, sent.at[0])
        await_bytes(term_recv, sent.at[0])
        await_bytes(bias_x.at[0:3], sent.at[0])
        await_bytes(bias_z.at[0:3], sent.at[0])


def store_results(*refs):
    sources, targets, sems = refs[:5], refs[5:10], refs[10]
    copies = [pltpu.make_async_copy(source, target, sems.at[n]) for n, (source, target) in enumerate(zip(sources, targets))]
    for copy in copies:
        copy.start()
    for copy in copies:
        copy.wait()


def shards(tokens, query_weight, key_weight, value_weight, position_bias, out_grad):
    anywhere = pl.BlockSpec(memory_space=pl.ANY)
    near = pl.BlockSpec(memory_space=pltpu.VMEM)
    dma = pltpu.SemaphoreType.DMA
    vmem = pltpu.VMEM
    grad = vmem((COLS, COLS), F32)
    results = pl.pallas_call(
        kernel,
        name="segment_attention_grads",
        out_shape=(
            vmem((LENGTH, FEATURES), BF16), grad, grad, grad,
            vmem((HEADS, TABLE), F32),
        ),
        in_specs=[anywhere] * 6,
        out_specs=(near,) * 5,
        scratch_shapes=[
            vmem((HEADS, TABLE), F32),
            vmem((LENGTH, WIDTH), BF16),
            vmem((WIDTH, 3 * COLS), BF16),
            vmem((2, TILE, 3 * COLS), F32),
            vmem((LENGTH, COLS), BF16),
            vmem((REACH + LENGTH, 2 * COLS), BF16),
            vmem((LENGTH, COLS), BF16),
            vmem((COLS, REACH + LENGTH), BF16),
            vmem((REACH + LENGTH, 2 * COLS), F32),
            vmem((LENGTH, 3 * COLS), BF16),
            vmem((3 * COLS, LENGTH), BF16),
            vmem((REACH, 2 * COLS), BF16),
            vmem((REACH, 2 * COLS), BF16),
            vmem((3, RING + 1, RING, HEAD, COLS), BF16),
            vmem((3, RING, RING, HEAD, COLS), BF16),
            vmem((3, 2, 2, 2, HEAD, COLS), BF16),
            vmem((3, 2, 2, 2, 2, HEAD, COLS), BF16),
            vmem((3, 2, RING, HEAD, COLS), BF16),
            vmem((3, 2, 2, SEGMENT, COLS), BF16),
            vmem((3, 2, 2, 2, SEGMENT, COLS), BF16),
            vmem((RING, LENGTH, FEATURES), BF16),
            vmem((RING, LENGTH, FEATURES), BF16),
            vmem((RING, LENGTH, FEATURES), BF16),
            vmem((2, LENGTH // 2, FEATURES), BF16),
            vmem((2, 2, LENGTH // 2, FEATURES), BF16),
            vmem((HEADS, SPAN, TILE), F32),
            vmem((HEADS, SPAN, TILE), F32),
            vmem((RING, 8, TILE), F32),
            vmem((RING, 8, TILE), F32),
            dma((6,)),
            dma((CHUNKS,)), dma((CHUNKS,)), dma((CHUNKS,)), dma((CHUNKS,)), dma((CHUNKS,)),
            dma((3,)),
            dma((RING + 1,)),
            dma((3, 2)), dma((3, 2)), dma((2,)),
            dma((2,)),
            dma((1,)),
        ],
        compiler_params=pltpu.CompilerParams(
            collective_id=0, has_side_effects=True, vmem_limit_bytes=62_000_000
        ),
    )(tokens, query_weight, key_weight, value_weight, position_bias, out_grad)
    return pl.pallas_call(
        store_results,
        name="store_results",
        out_shape=tuple(jax.ShapeDtypeStruct(result.shape, result.dtype) for result in results),
        in_specs=[near] * 5,
        out_specs=(anywhere,) * 5,
        scratch_shapes=[dma((5,))],
        compiler_params=pltpu.CompilerParams(vmem_limit_bytes=1_000_000),
    )(*results)


def solution(mesh):
    return jax.shard_map(
        shards,
        mesh=mesh,
        in_specs=(P("sp", "tp"), P(None, "tp"), P(None, "tp"), P(None, "tp"), P("tp", None), P("sp", "tp")),
        out_specs=(P("sp", "tp"), P("sp", "tp"), P("sp", "tp"), P("sp", "tp"), P("tp", None)),
        check_vma=False,
    )
```
